32 devices in a mesh: grp: 2 (over y), sp: 4 (over z), tp: 4 (over x, core).
Axes of the slice: x: 2, y: 2, z: 4, core: 2. Of those that a mesh axis runs over, the one named last changes fastest.
Arguments:
- residual: bfloat16 [4096, 2048], P(('grp', 'sp', 'tp')), parts along dimension 0, may hold values from -6 to 6
- state_input: bfloat16 [4096, 1024], P(('grp', 'sp'), 'tp'), parts along dimension 0, may hold values from -6 to 6
- gate_input: bfloat16 [4096, 2048], P(('grp', 'sp'), 'tp'), parts along dimension 0, may hold values from -6 to 6
- decay_real: float32 [64, 64], P('tp'), may hold values from -0.2 to 0, as said below
- frequency: float32 [64, 64], P('tp'), as said below
- log_step: float32 [64], P('tp'), as said below
- drive_real: float32 [64, 64, 16], P('tp'), may hold values from -1 to 1
- drive_imag: float32 [64, 64, 16], P('tp'), may hold values from -1 to 1
- read_real: float32 [64, 16, 64], P('tp'), may hold values from -0.75 to 0.75
- read_imag: float32 [64, 16, 64], P('tp'), may hold values from -0.75 to 0.75
- skip_gain: float32 [1024], P('tp'), may hold values from -4 to 4
- value_weight: bfloat16 [1024, 2048], P(None, 'tp'), may hold values from -0.1875 to 0.1875
- glu_weight: bfloat16 [1024, 2048], P(None, 'tp'), may hold values from -0.1875 to 0.1875
- mix_weight: bfloat16 [2048, 2048], P('tp'), may hold values from -0.125 to 0.125
- norm_gain: float32 [2048], replicated, may hold values from 0.1 to 1.9
- mlp_gate: bfloat16 [2048, 3072], P('sp', 'tp'), may hold values from -0.125 to 0.125
- mlp_up: bfloat16 [2048, 3072], P('sp', 'tp'), may hold values from -0.125 to 0.125
- mlp_down: bfloat16 [3072, 2048], P('tp', 'sp'), may hold values from -0.109375 to 0.109375
Outputs:
- result: bfloat16 [4096, 2048], P(('grp', 'sp', 'tp')), parts along dimension 0
The draws below stay inside these ranges and needn't reach their ends.
There are 2 independent parts, one for each index of `grp`. The reference program is written for one: setup_inputs(seed, part) draws one part's arguments, and reference() takes and returns one part's arrays. A program takes and returns all parts, laid end to end along the dimension named above; an argument that names none is the same for every part. Nothing has to cross between parts.
Inputs may be any that keep to these rules, and one draw needn't show every extreme that they name: `decay_real`: negative in every entry. `frequency`: never zero: its magnitude times exp(log_step) of its group lies between 0.05 and 0.5. Every group's time step exp(log_step) is at most one.
All inputs are finite; a program needn't handle non-finite values.
Results may differ from the reference program's by a relative error of at most 0.012.
Values may be sent and summed in bfloat16 or wider, within the bound.
A program may use at most 128 MiB of HBM per device.

```python
import math
import jax
import jax.numpy as jnp
from jax import lax

D = 2048
D_SSM = 1024
SSM_GROUP = 16
STATE = 64
FF = 3072
TOK_DEV = 512
GROUPS = 64
TOKENS = 2048
N_TP = 4


def spectrum(key):
    fast_key = jax.random.fold_in(key, 101)
    rate_key = jax.random.fold_in(key, 202)
    spread_key = jax.random.fold_in(key, 303)
    turn_key = jax.random.fold_in(key, 404)
    sign_key = jax.random.fold_in(key, 505)
    share = 0.5
    fast = jax.random.uniform(fast_key, (GROUPS,), jnp.float32) < share
    unit = jax.random.uniform(rate_key, (GROUPS,), jnp.float32)
    fast_rate = jnp.exp(math.log(1.0 / 40.0) + unit * math.log(2.0))
    slow_rate = jnp.exp(jnp.log(0.5 / TOKENS) + unit * math.log(4.0))
    rate = jnp.where(fast, fast_rate, slow_rate)
    step = 2.0 * jnp.sqrt(rate)
    spread = jnp.exp(jax.random.uniform(spread_key, (GROUPS, STATE), jnp.float32, math.log(0.7), math.log(1.4)))
    decay = -(rate / step)[:, None] * spread
    turn = jax.random.uniform(turn_key, (GROUPS, STATE), jnp.float32, 0.05, 0.5)
    sign = jnp.where(jax.random.uniform(sign_key, (GROUPS, STATE), jnp.float32) < 0.5, -1.0, 1.0)
    frequency = sign * turn / step[:, None]
    return (decay, frequency, jnp.log(step))


def draw_decay_real(key, part):
    return spectrum(key)[0]


def draw_frequency(key, part):
    return spectrum(key)[1]


def draw_log_step(key, part):
    return spectrum(key)[2]


def block_scale(rng, extent, cuts, smallest, top_value):
    factor_of, own = 1.0, jax.random.fold_in(rng, 6)
    for axis_at, blocks in cuts:
        steps = jnp.exp(jax.random.uniform(jax.random.fold_in(own, axis_at), (blocks,), jnp.float32, smallest / len(cuts), top_value / len(cuts)))
        factor_of = factor_of * jnp.repeat(steps, extent[axis_at] // blocks).reshape([-1 if axis == axis_at else 1 for axis in range(len(extent))])
    return factor_of


def bell_draw(key, dims, scale, bound, split=(), dtype=jnp.bfloat16):
    drawn = scale * jax.random.normal(key, dims, jnp.float32)
    if split:
        drawn = drawn * block_scale(key, dims, split, -0.22, 0.18)
    return jnp.clip(drawn, -bound, bound).astype(dtype)


def setup_inputs(seed: int = 0, part: int = 0) -> dict:
    keys = jax.random.split(jax.random.key(seed), 19)
    part_splits = jax.random.split(jax.random.fold_in(keys[18], part), 19)
    residual = bell_draw(part_splits[0], (TOKENS, D), 1.0, 6.0, ((0, 16),))
    state_input = bell_draw(part_splits[1], (TOKENS, D_SSM), 1.0, 6.0, ((0, 4), (1, 4)))
    gate_input = bell_draw(part_splits[2], (TOKENS, D), 1.5, 6.0, ((0, 4), (1, 4)))
    decay_real = draw_decay_real(jax.random.fold_in(keys[18], 71), part)
    frequency = draw_frequency(jax.random.fold_in(keys[18], 71), part)
    log_step = draw_log_step(jax.random.fold_in(keys[18], 71), part)
    drive_real = bell_draw(keys[6], (GROUPS, STATE, SSM_GROUP), (2 * SSM_GROUP) ** -0.5, 1.0, ((0, 4),), jnp.float32)
    drive_imag = bell_draw(keys[7], (GROUPS, STATE, SSM_GROUP), (2 * SSM_GROUP) ** -0.5, 1.0, ((0, 4),), jnp.float32)
    read_real = bell_draw(keys[8], (GROUPS, SSM_GROUP, STATE), STATE ** -0.5, 0.75, ((0, 4),), jnp.float32)
    read_imag = bell_draw(keys[9], (GROUPS, SSM_GROUP, STATE), STATE ** -0.5, 0.75, ((0, 4),), jnp.float32)
    skip_gain = bell_draw(keys[10], (D_SSM,), 1.0, 4.0, ((0, 4),), jnp.float32)
    value_weight = bell_draw(keys[11], (D_SSM, D), D_SSM ** -0.5, 0.1875, ((1, 4),))
    glu_weight = bell_draw(keys[12], (D_SSM, D), D_SSM ** -0.5, 0.1875, ((1, 4),))
    mix_weight = bell_draw(keys[13], (D, D), D ** -0.5, 0.125, ((0, 4),))
    norm_gain = jnp.clip(1.0 + 0.18 * jax.random.normal(keys[14], (D,), jnp.float32), 0.1, 1.9)
    mlp_gate = bell_draw(keys[15], (D, FF), D ** -0.5, 0.125, ((0, 4), (1, 4)))
    mlp_up = bell_draw(keys[16], (D, FF), D ** -0.5, 0.125, ((0, 4), (1, 4)))
    mlp_down = bell_draw(keys[17], (FF, D), FF ** -0.5, 0.109375, ((0, 4), (1, 4)))
    return {"residual": residual, "state_input": state_input, "gate_input": gate_input, "decay_real": decay_real, "frequency": frequency, "log_step": log_step, "drive_real": drive_real, "drive_imag": drive_imag, "read_real": read_real, "read_imag": read_imag, "skip_gain": skip_gain, "value_weight": value_weight, "glu_weight": glu_weight, "mix_weight": mix_weight, "norm_gain": norm_gain, "mlp_gate": mlp_gate, "mlp_up": mlp_up, "mlp_down": mlp_down}


HIGH = lax.Precision.HIGHEST
EPSILON = 1e-06

def discretize(decay_real, frequency, log_step, drive_real, drive_imag):
    step = jnp.exp(log_step)[:, None]
    magnitude = jnp.exp(decay_real * step)
    turned = frequency * step
    bar_real = magnitude * jnp.cos(turned)
    bar_imag = magnitude * jnp.sin(turned)
    modulus = decay_real * decay_real + frequency * frequency
    ratio_real = ((bar_real - 1.0) * decay_real + bar_imag * frequency) / modulus
    ratio_imag = (bar_imag * decay_real - (bar_real - 1.0) * frequency) / modulus
    in_real = ratio_real[..., None] * drive_real - ratio_imag[..., None] * drive_imag
    in_imag = ratio_real[..., None] * drive_imag + ratio_imag[..., None] * drive_real
    return (bar_real, bar_imag, in_real, in_imag)

def combine(earlier, later):
    real_one, imag_one, state_real_one, state_imag_one = earlier
    real_two, imag_two, state_real_two, state_imag_two = later
    return (real_one * real_two - imag_one * imag_two, real_one * imag_two + imag_one * real_two, real_two * state_real_one - imag_two * state_imag_one + state_real_two, real_two * state_imag_one + imag_two * state_real_one + state_imag_two)

def block_states(inputs, bar_real, bar_imag, in_real, in_imag):
    rows = inputs.shape[0]
    flat = bar_real.shape[0] * bar_real.shape[1]
    push_real = jnp.einsum('lgh,gph->lgp', inputs, in_real, precision=HIGH).reshape(rows, flat)
    push_imag = jnp.einsum('lgh,gph->lgp', inputs, in_imag, precision=HIGH).reshape(rows, flat)
    power_real = jnp.broadcast_to(bar_real.reshape(1, flat), (rows, flat))
    power_imag = jnp.broadcast_to(bar_imag.reshape(1, flat), (rows, flat))
    return lax.associative_scan(combine, (power_real, power_imag, push_real, push_imag), axis=0)

def readout(state_real, state_imag, read_real, read_imag, inputs, skip_gain):
    rows = inputs.shape[0]
    groups, width, states = read_real.shape
    grid_real = state_real.reshape(rows, groups, states)
    grid_imag = state_imag.reshape(rows, groups, states)
    output = jnp.einsum('lgp,ghp->lgh', grid_real, read_real, precision=HIGH)
    output = output - jnp.einsum('lgp,ghp->lgh', grid_imag, read_imag, precision=HIGH)
    output = output.reshape(rows, groups * width) + skip_gain * inputs.reshape(rows, groups * width)
    return jax.nn.gelu(output).astype(jnp.bfloat16)

def normalize(inner, norm_gain):
    scale = lax.rsqrt(lax.optimization_barrier(jnp.mean(inner * inner, axis=-1, keepdims=True)) + EPSILON)
    return (inner * scale * norm_gain).astype(jnp.bfloat16)

def reference(residual, state_input, gate_input, decay_real, frequency, log_step, drive_real, drive_imag, read_real, read_imag, skip_gain, value_weight, glu_weight, mix_weight, norm_gain, mlp_gate, mlp_up, mlp_down):
    bar_real, bar_imag, in_real, in_imag = discretize(decay_real, frequency, log_step, drive_real, drive_imag)
    groups, states = bar_real.shape
    blocks = state_input.astype(jnp.float32).reshape(TOKENS // TOK_DEV, TOK_DEV, groups, SSM_GROUP)

    def advance(carry, inputs):
        carry_real, carry_imag = carry
        power_real, power_imag, local_real, local_imag = block_states(inputs, bar_real, bar_imag, in_real, in_imag)
        state_real = local_real + power_real * carry_real - power_imag * carry_imag
        state_imag = local_imag + power_real * carry_imag + power_imag * carry_real
        acts = readout(state_real, state_imag, read_real, read_imag, inputs, skip_gain)
        return ((state_real[-1], state_imag[-1]), acts)
    zero = jnp.zeros((groups * states,), jnp.float32)
    _, acts = lax.scan(advance, (zero, zero), blocks)
    acts = acts.reshape(TOKENS, D_SSM)
    value = jnp.dot(acts, value_weight, preferred_element_type=jnp.float32)
    gated = jnp.dot(acts, glu_weight, preferred_element_type=jnp.float32)
    mixed = (jax.nn.sigmoid(gate_input.astype(jnp.float32)) * value * jax.nn.sigmoid(gated)).astype(jnp.bfloat16)
    span = D // N_TP
    branch = jnp.zeros((TOKENS, D), jnp.float32)
    for index in range(N_TP):
        product = jnp.dot(mixed[:, index * span:(index + 1) * span], mix_weight[index * span:(index + 1) * span], preferred_element_type=jnp.float32).astype(jnp.bfloat16)
        branch = branch + lax.optimization_barrier(product).astype(jnp.float32)
    inner = residual.astype(jnp.float32) + branch
    normed = normalize(inner, norm_gain)
    hidden_gate = jnp.dot(normed, mlp_gate, preferred_element_type=jnp.float32)
    hidden_up = jnp.dot(normed, mlp_up, preferred_element_type=jnp.float32)
    hidden = (jax.nn.silu(hidden_gate) * hidden_up).astype(jnp.bfloat16)
    width = FF // N_TP
    down = jnp.zeros((TOKENS, D), jnp.float32)
    for index in range(N_TP):
        product = jnp.dot(hidden[:, index * width:(index + 1) * width], mlp_down[index * width:(index + 1) * width], preferred_element_type=jnp.float32).astype(jnp.bfloat16)
        down = down + lax.optimization_barrier(product).astype(jnp.float32)
    return (inner + 0.5 * down).astype(jnp.bfloat16)
```

```python
import functools
import jax
import jax.numpy as jnp
from jax import lax
from jax.experimental import pallas as pl
from jax.experimental.pallas import tpu as pltpu
from jax.sharding import PartitionSpec as P

BF = jnp.bfloat16
F32 = jnp.float32
ROWS8 = 8
PIECES = 2

HIGH = lax.Precision.HIGHEST
EPSILON = 1e-06


def carried_in(value, axis, join, neutral):
    count, mine = (lax.axis_size(axis), lax.axis_index(axis))
    pieces = jax.tree.map(lambda part: lax.all_gather(part, axis), value)
    subtotal = jax.tree.map(
        lambda part, zero: jnp.full_like(part, 0) + jnp.asarray(zero, part.dtype), value, neutral
    )

    def step(position, subtotal):
        longer = join(subtotal, jax.tree.map(lambda part: part[position], pieces))
        return jax.tree.map(lambda new, old: jnp.where(position < mine, new, old), longer, subtotal)

    return lax.fori_loop(0, count - 1, step, subtotal)


def discretize(decay_real, frequency, log_step, drive_real, drive_imag):
    step = jnp.exp(log_step)[:, None]
    magnitude = jnp.exp(decay_real * step)
    turned = frequency * step
    bar_real = magnitude * jnp.cos(turned)
    bar_imag = magnitude * jnp.sin(turned)
    modulus = decay_real * decay_real + frequency * frequency
    ratio_real = ((bar_real - 1.0) * decay_real + bar_imag * frequency) / modulus
    ratio_imag = (bar_imag * decay_real - (bar_real - 1.0) * frequency) / modulus
    in_real = ratio_real[..., None] * drive_real - ratio_imag[..., None] * drive_imag
    in_imag = ratio_real[..., None] * drive_imag + ratio_imag[..., None] * drive_real
    return (bar_real, bar_imag, in_real, in_imag)


def combine(earlier, later):
    real_one, imag_one, state_real_one, state_imag_one = earlier
    real_two, imag_two, state_real_two, state_imag_two = later
    return (
        real_one * real_two - imag_one * imag_two,
        real_one * imag_two + imag_one * real_two,
        real_two * state_real_one - imag_two * state_imag_one + state_real_two,
        real_two * state_imag_one + imag_two * state_real_one + state_imag_two,
    )


def powers(log_rate, angle_rate, count):
    return (
        jnp.exp(log_rate * count) * jnp.cos(angle_rate * count),
        jnp.exp(log_rate * count) * jnp.sin(angle_rate * count),
    )


def block_states(flat_inputs, decay_real, frequency, log_step, in_real, in_imag):
    rows = flat_inputs.shape[0]
    groups, states, width = in_real.shape
    flat = groups * states
    eye = jnp.eye(groups, dtype=jnp.float32)
    wide_real = jnp.einsum("gph,gk->ghkp", in_real, eye).reshape(groups * width, flat)
    wide_imag = jnp.einsum("gph,gk->ghkp", in_imag, eye).reshape(groups * width, flat)
    state_real = jnp.dot(flat_inputs, wide_real, precision=HIGH)
    state_imag = jnp.dot(flat_inputs, wide_imag, precision=HIGH)
    step = jnp.exp(log_step)[:, None]
    log_rate = (decay_real * step).reshape(1, flat)
    angle_rate = (frequency * step).reshape(1, flat)
    reach = 1
    while reach < rows:
        lift_real, lift_imag = powers(log_rate, angle_rate, float(reach))
        blank = jnp.zeros((reach, flat), jnp.float32)
        moved_real = jnp.concatenate([blank, state_real[: rows - reach]], axis=0)
        moved_imag = jnp.concatenate([blank, state_imag[: rows - reach]], axis=0)
        state_real, state_imag = (
            state_real + lift_real * moved_real - lift_imag * moved_imag,
            state_imag + lift_real * moved_imag + lift_imag * moved_real,
        )
        reach = reach * 2
    counts = (lax.iota(jnp.int32, rows) + 1).astype(jnp.float32)[:, None]
    power_real, power_imag = powers(log_rate, angle_rate, counts)
    return (power_real, power_imag, state_real, state_imag)


def readout(state_real, state_imag, read_real, read_imag, flat_inputs, skip_gain):
    groups, width, states = read_real.shape
    eye = jnp.eye(groups, dtype=jnp.float32)
    wide_real = jnp.einsum("ghp,gk->gpkh", read_real, eye).reshape(groups * states, groups * width)
    wide_imag = jnp.einsum("ghp,gk->gpkh", read_imag, eye).reshape(groups * states, groups * width)
    output = jnp.dot(state_real, wide_real, precision=HIGH) - jnp.dot(
        state_imag, wide_imag, precision=HIGH
    )
    output = output + skip_gain * flat_inputs
    return jax.nn.gelu(output).astype(jnp.bfloat16)


def normalize(inner, norm_gain):
    scale = lax.rsqrt(jnp.mean(inner * inner, axis=-1, keepdims=True) + EPSILON)
    return (inner * scale * norm_gain).astype(jnp.bfloat16)


def shards(
    residual,
    state_input,
    gate_input,
    decay_real,
    frequency,
    log_step,
    drive_real,
    drive_imag,
    read_real,
    read_imag,
    skip_gain,
    value_weight,
    glu_weight,
    mix_weight,
    norm_gain,
    mlp_gate,
    mlp_up,
    mlp_down,
):
    bar_real, bar_imag, in_real, in_imag = discretize(
        decay_real, frequency, log_step, drive_real, drive_imag
    )
    flat_inputs = state_input.astype(jnp.float32)
    power_real, power_imag, local_real, local_imag = block_states(
        flat_inputs, decay_real, frequency, log_step, in_real, in_imag
    )
    ends = (power_real[-1], power_imag[-1], local_real[-1], local_imag[-1])
    ones = jnp.ones_like(ends[0])
    zeros = jnp.zeros_like(ends[0])
    incoming = carried_in(
        (ends[0], ends[1], ends[2], ends[3]), "sp", combine, (ones, zeros, zeros, zeros)
    )
    carry_real = incoming[2]
    carry_imag = incoming[3]
    state_real = local_real + power_real * carry_real - power_imag * carry_imag
    state_imag = local_imag + power_real * carry_imag + power_imag * carry_real
    acts = readout(state_real, state_imag, read_real, read_imag, flat_inputs, skip_gain)
    piece = lax.all_gather(acts, "tp", axis=1, tiled=True)
    value = jnp.dot(piece, value_weight, preferred_element_type=jnp.float32)
    gated = jnp.dot(piece, glu_weight, preferred_element_type=jnp.float32)
    mixed = (jax.nn.sigmoid(gate_input.astype(jnp.float32)) * value * jax.nn.sigmoid(gated)).astype(
        jnp.bfloat16
    )
    branch = lax.psum_scatter(
        jnp.dot(mixed, mix_weight, preferred_element_type=jnp.float32).astype(jnp.bfloat16),
        "tp",
        scatter_dimension=0,
        tiled=True,
    ).astype(jnp.float32)
    inner = residual.astype(jnp.float32) + branch
    normed = lax.all_gather(normalize(inner, norm_gain), "tp", axis=0, tiled=True)
    hidden_gate = jnp.dot(
        normed,
        lax.all_gather(mlp_gate, "sp", axis=0, tiled=True),
        preferred_element_type=jnp.float32,
    )
    hidden_up = jnp.dot(
        normed, lax.all_gather(mlp_up, "sp", axis=0, tiled=True), preferred_element_type=jnp.float32
    )
    hidden = (jax.nn.silu(hidden_gate) * hidden_up).astype(jnp.bfloat16)
    down = jnp.dot(
        hidden,
        lax.all_gather(mlp_down, "sp", axis=1, tiled=True),
        preferred_element_type=jnp.float32,
    )
    down_own = lax.psum_scatter(
        down.astype(jnp.bfloat16), "tp", scatter_dimension=0, tiled=True
    ).astype(jnp.float32)
    return (inner + 0.5 * down_own).astype(jnp.bfloat16)


def mm(a, b):
    return jnp.dot(a, b, preferred_element_type=F32)


def mm_t(a, b):
    return lax.dot_general(a, b, (((1,), (1,)), ((), ())), preferred_element_type=F32)


def split(x):
    high = x.astype(BF)
    return high, (x - high.astype(F32)).astype(BF)


def layer_kernel(
    n_sp,
    width,
    states,
    residual,
    u,
    gate_in,
    pow_real,
    pow_imag,
    in_real,
    in_imag,
    rd_real,
    rd_imag,
    skip,
    value_h,
    glu_h,
    mix_h,
    gain,
    gate_h,
    up_h,
    down_h,
    out,
    value_w,
    glu_w,
    mix_w,
    w_gate,
    w_up,
    w_down,
    wide,
    st_real,
    st_imag,
    masked,
    ends,
    acts,
    part,
    rx_pair,
    relay,
    rx_far,
    inner,
    normed,
    hidden,
    c_part,
    c_pair,
    c_relay,
    c_far,
    load_sem,
    end_send,
    end_recv,
    z_send,
    z_recv,
    y_send,
    y_recv,
    ag_send,
    ag_recv,
    rs_send,
    rs_recv,
    c_send,
    c_recv,
):
    g, s, t = lax.axis_index("grp"), lax.axis_index("sp"), lax.axis_index("tp")
    low, high_bit = t % 2, t // 2
    p = t + 1 - 2 * low
    q = t + 2 - 4 * high_bit
    far = 3 - t
    other = 1 - g
    rows, chans = u.shape
    flat = st_real.shape[1]
    own, depth = residual.shape
    k_loc = gate_h.shape[0]
    ff, d_loc = down_h.shape
    k_half, f_half = k_loc // 2, ff // 2

    barrier = pltpu.get_barrier_semaphore()
    pl.semaphore_signal(barrier, inc=1, device_id={"tp": p})
    pl.semaphore_signal(barrier, inc=1, device_id={"tp": q})
    pl.semaphore_signal(barrier, inc=1, device_id={"grp": other})

    @pl.loop(1, n_sp)
    def _(d):
        pl.semaphore_signal(barrier, inc=1, device_id={"sp": (s + d) % n_sp})

    def mine(ref, c, origin, half):
        if c < 2:
            return ref.at[pl.ds(pl.multiple_of(origin * k_loc + half * k_half, k_half), k_half), :]
        return ref.at[origin, pl.ds(pl.multiple_of(half * f_half, f_half), f_half), :]

    bufs = (w_gate, w_up, w_down)
    place = pl.ds(pl.multiple_of(s * k_loc, k_loc), k_loc)
    loads = [
        pltpu.make_async_copy(gate_h, w_gate.at[place, :], load_sem.at[0]),
        pltpu.make_async_copy(up_h, w_up.at[place, :], load_sem.at[1]),
        pltpu.make_async_copy(down_h, w_down.at[s], load_sem.at[2]),
        pltpu.make_async_copy(value_h, value_w, load_sem.at[3]),
        pltpu.make_async_copy(glu_h, glu_w, load_sem.at[4]),
        pltpu.make_async_copy(mix_h, mix_w, load_sem.at[5]),
    ]
    for load in loads:
        load.start()
    pl.semaphore_wait(barrier, 3 + n_sp - 1)

    def z_copy(side, c, k, origin, target):
        piece = mine(bufs[c], c, origin, g)
        return pltpu.make_async_remote_copy(
            src_ref=piece,
            dst_ref=piece,
            send_sem=z_send.at[side, c, k],
            recv_sem=z_recv.at[side, c, k],
            device_id={"sp": target},
        )

    def y_copy(side, c, k, origin, half):
        piece = mine(bufs[c], c, origin, half)
        return pltpu.make_async_remote_copy(
            src_ref=piece,
            dst_ref=piece,
            send_sem=y_send.at[side, c, k],
            recv_sem=y_recv.at[side, c, k],
            device_id={"grp": other},
        )

    right, left = (s + 1) % n_sp, (s + n_sp - 1) % n_sp
    has_right, has_left = s < n_sp - 1, s > 0

    for c in range(3):
        loads[c].wait()

        @pl.when(has_right)
        def _():
            z_copy(0, c, 1, s, right).start()

        @pl.when(has_left)
        def _():
            z_copy(1, c, 1, s, left).start()

    def onward(c, k):
        @pl.when(s >= k)
        def _():
            origin = (s + n_sp - k) % n_sp
            z_copy(0, c, k, origin, right).wait_recv()

            @pl.when(has_right)
            def _():
                z_copy(0, c, k + 1, origin, right).start()

            y_copy(0, c, k, origin, g).start()

        @pl.when(s + k < n_sp)
        def _():
            origin = (s + k) % n_sp
            z_copy(1, c, k, origin, left).wait_recv()

            @pl.when(has_left)
            def _():
                z_copy(1, c, k + 1, origin, left).start()

            y_copy(1, c, k, origin, g).start()

    def arrived(c):
        @pl.loop(1, n_sp)
        def _(k):
            @pl.when(s >= k)
            def _():
                y_copy(0, c, k, (s + n_sp - k) % n_sp, other).wait_recv()

            @pl.when(s + k < n_sp)
            def _():
                y_copy(1, c, k, (s + k) % n_sp, other).wait_recv()

    lanes = in_real.shape[1]
    row_group = lax.broadcasted_iota(jnp.int32, (chans, lanes), 0) // width
    lane = lax.broadcasted_iota(jnp.int32, (chans, lanes), 1)
    for i, ref in enumerate((in_real, in_imag, rd_real, rd_imag)):
        value = ref[...]
        for tile in range(flat // lanes):
            kept = jnp.where(row_group == (lane + tile * lanes) // states, value, 0.0)
            big, small = split(kept)
            at = slice(tile * lanes, (tile + 1) * lanes)
            wide[2 * i, :, at] = big
            wide[2 * i + 1, :, at] = small

    @pl.loop(0, rows // own)
    def _(b):
        at = pl.ds(pl.multiple_of(b * own, own), own)
        x = u[at, :]
        st_real[at, :] = mm(x, wide[0]) + mm(x, wide[1])
        st_imag[at, :] = mm(x, wide[2]) + mm(x, wide[3])

    sub = lax.broadcasted_iota(jnp.int32, (ROWS8, flat), 0)
    for i, reach in enumerate((1, 2, 4)):
        masked[2 * i] = jnp.where(sub >= reach, pow_real[reach - 1 : reach, :], 0.0)
        masked[2 * i + 1] = jnp.where(sub >= reach, pow_imag[reach - 1 : reach, :], 0.0)

    def scan_step(b, carry):
        c_re, c_im = carry
        at = pl.ds(pl.multiple_of(b * ROWS8, ROWS8), ROWS8)
        x_re, x_im = st_real[at, :], st_imag[at, :]
        for i, reach in enumerate((1, 2, 4)):
            m_re, m_im = pltpu.roll(x_re, reach, 0), pltpu.roll(x_im, reach, 0)
            a_re, a_im = masked[2 * i], masked[2 * i + 1]
            x_re, x_im = x_re + a_re * m_re - a_im * m_im, x_im + a_re * m_im + a_im * m_re
        p_re, p_im = pow_real[...], pow_imag[...]
        x_re, x_im = x_re + p_re * c_re - p_im * c_im, x_im + p_re * c_im + p_im * c_re
        st_real[at, :] = x_re
        st_imag[at, :] = x_im
        return x_re[ROWS8 - 1 :, :], x_im[ROWS8 - 1 :, :]

    zero = jnp.zeros((1, flat), F32)
    end_re, end_im = lax.fori_loop(0, rows // ROWS8, scan_step, (zero, zero))
    ends[s, 0:1, :] = end_re
    ends[s, 1:2, :] = end_im

    def end_copy(target, origin):
        return pltpu.make_async_remote_copy(
            src_ref=ends.at[origin],
            dst_ref=ends.at[origin],
            send_sem=end_send.at[target],
            recv_sem=end_recv.at[origin],
            device_id={"sp": target},
        )

    @pl.loop(1, n_sp)
    def _(d):
        end_copy((s + d) % n_sp, s).start()

    onward(0, 1)
    last_re, last_im = pow_real[ROWS8 - 1 :, :], pow_imag[ROWS8 - 1 :, :]
    long_re, long_im = last_re, last_im
    reach = ROWS8
    while reach < rows:
        long_re, long_im = long_re * long_re - long_im * long_im, 2.0 * long_re * long_im
        reach *= 2

    @pl.loop(1, n_sp)
    def _(d):
        end_copy((s + d) % n_sp, (s + d) % n_sp).wait_recv()

    def carry_step(j, carry):
        c_re, c_im = carry
        e_re, e_im = ends[j, 0:1, :], ends[j, 1:2, :]
        n_re = long_re * c_re - long_im * c_im + e_re
        n_im = long_re * c_im + long_im * c_re + e_im
        return jnp.where(j < s, n_re, c_re), jnp.where(j < s, n_im, c_im)

    carry = lax.fori_loop(0, n_sp - 1, carry_step, (zero, zero))

    def lift(b, carry):
        c_re, c_im = carry
        at = pl.ds(pl.multiple_of(b * ROWS8, ROWS8), ROWS8)
        p_re, p_im = pow_real[...], pow_imag[...]
        st_real[at, :] = st_real[at, :] + p_re * c_re - p_im * c_im
        st_imag[at, :] = st_imag[at, :] + p_re * c_im + p_im * c_re
        return last_re * c_re - last_im * c_im, last_re * c_im + last_im * c_re

    lax.fori_loop(0, rows // ROWS8, lift, carry)

    @pl.loop(0, rows // own)
    def _(b):
        at = pl.ds(pl.multiple_of(b * own, own), own)
        high, small = split(st_real[at, :])
        y = mm_t(high, wide[4]) + mm_t(small, wide[4]) + mm_t(high, wide[5])
        high, small = split(st_imag[at, :])
        y = y - (mm_t(high, wide[6]) + mm_t(small, wide[6]) + mm_t(high, wide[7]))
        y = y + skip[...] * u[at, :].astype(F32)
        acts[t, at, :] = jax.nn.gelu(y).astype(BF)

    def gather_tp(buf, lane_no, between):
        def copy(slot, kind, target):
            return pltpu.make_async_remote_copy(
                src_ref=buf.at[slot],
                dst_ref=buf.at[slot],
                send_sem=ag_send.at[lane_no, kind],
                recv_sem=ag_recv.at[lane_no, kind],
                device_id={"tp": target},
            )

        sent = [copy(t, 0, q), copy(t, 1, p)]
        for item in sent:
            item.start()
        between()
        copy(q, 0, q).wait_recv()
        relayed = copy(q, 2, p)
        relayed.start()
        copy(p, 1, p).wait_recv()
        copy(far, 2, p).wait_recv()
        return sent + [relayed]

    def scatter_tp(lane_no, block, middle, between):
        def pair(index):
            return pltpu.make_async_remote_copy(
                src_ref=part.at[lane_no, (far, p)[index]],
                dst_ref=rx_pair.at[lane_no, index],
                send_sem=rs_send.at[lane_no, index],
                recv_sem=rs_recv.at[lane_no, index],
                device_id={"tp": p},
            )

        across = pltpu.make_async_remote_copy(
            src_ref=relay.at[lane_no],
            dst_ref=rx_far.at[lane_no],
            send_sem=rs_send.at[lane_no, 2],
            recv_sem=rs_recv.at[lane_no, 2],
            device_id={"tp": q},
        )
        pairs = [pair(0), pair(1)]
        block(far)
        pairs[0].start()
        block(p)
        pairs[1].start()
        block(q)
        middle()
        pairs[0].wait_recv()
        relay[lane_no] = (part[lane_no, q].astype(F32) + rx_pair[lane_no, 0].astype(F32)).astype(BF)
        across.start()
        block(t)
        between()
        pairs[1].wait_recv()
        across.wait_recv()
        return pairs + [across]

    def total(lane_no):
        near = part[lane_no, t].astype(F32) + rx_pair[lane_no, 1].astype(F32)
        return near + rx_far[lane_no].astype(F32)

    def first_forward():
        onward(1, 1)

    pending = gather_tp(acts, 0, first_forward)
    for load in loads[3:]:
        load.wait()
    n_tp = acts.shape[0]

    def mix_block(r):
        at = pl.ds(pl.multiple_of(r * own, own), own)
        value = jnp.zeros((own, value_w.shape[1]), F32)
        gated = value
        for j in range(n_tp):
            a = acts[j, at, :]
            value = value + mm(a, value_w[j * chans : (j + 1) * chans, :])
            gated = gated + mm(a, glu_w[j * chans : (j + 1) * chans, :])
        mixed = jax.nn.sigmoid(gate_in[at, :].astype(F32)) * value * jax.nn.sigmoid(gated)
        part[0, r] = mm(mixed.astype(BF), mix_w[...]).astype(BF)

    def third_forward():
        if n_sp > 2:
            onward(0, 2)

    pending += scatter_tp(0, mix_block, lambda: onward(2, 1), third_forward)
    inner[...] = residual[...].astype(F32) + total(0)
    x = inner[...]
    scale = lax.rsqrt(jnp.mean(x * x, axis=-1, keepdims=True) + EPSILON)
    normed[t] = (x * scale * gain[...]).astype(BF)

    def second_forward():
        if n_sp > 2:
            onward(1, 2)

    pending += gather_tp(normed, 1, second_forward)
    if n_sp > 2:
        onward(2, 2)

    @pl.loop(3, n_sp)
    def _(k):
        onward(0, k)
        onward(1, k)
        onward(2, k)

    arrived(0)
    arrived(1)

    @pl.loop(0, n_tp)
    def _(r):
        x = normed[r]
        hidden[r] = (jax.nn.silu(mm(x, w_gate[...])) * mm(x, w_up[...])).astype(BF)

    def col_pair(o, index):
        return pltpu.make_async_remote_copy(
            src_ref=c_part.at[o, (far, p)[index]],
            dst_ref=c_pair.at[o, index],
            send_sem=c_send.at[o, index],
            recv_sem=c_recv.at[o, index],
            device_id={"tp": p},
        )

    def col_far(o):
        return pltpu.make_async_remote_copy(
            src_ref=c_relay.at[o],
            dst_ref=c_far.at[o],
            send_sem=c_send.at[o, 2],
            recv_sem=c_recv.at[o, 2],
            device_id={"tp": q},
        )

    def column(o):
        weight = w_down.at[o]
        c_part[o, far] = mm(hidden[far], weight[...]).astype(BF)
        col_pair(o, 0).start()
        c_part[o, q] = mm(hidden[q], weight[...]).astype(BF)
        c_part[o, p] = mm(hidden[p], weight[...]).astype(BF)
        col_pair(o, 1).start()
        col_pair(o, 0).wait_recv()
        c_relay[o] = (c_part[o, q].astype(F32) + c_pair[o, 0].astype(F32)).astype(BF)
        col_far(o).start()
        c_part[o, t] = mm(hidden[t], weight[...]).astype(BF)

    column(s)

    @pl.loop(1, n_sp)
    def _(k):
        @pl.when(s >= k)
        def _():
            origin = (s + n_sp - k) % n_sp
            y_copy(0, 2, k, origin, other).wait_recv()
            column(origin)

        @pl.when(s + k < n_sp)
        def _():
            origin = (s + k) % n_sp
            y_copy(1, 2, k, origin, other).wait_recv()
            column(origin)

    for o in range(n_sp):
        col_pair(o, 1).wait_recv()
        col_far(o).wait_recv()
        near = c_part[o, t].astype(F32) + c_pair[o, 1].astype(F32)
        at = slice(o * d_loc, (o + 1) * d_loc)
        out[:, at] = (inner[:, at] + 0.5 * (near + c_far[o].astype(F32))).astype(BF)

    @pl.loop(0, n_sp)
    def _(o):
        col_pair(o, 0).wait_send()
        col_pair(o, 1).wait_send()
        col_far(o).wait_send()

    for item in pending:
        item.wait_send()

    @pl.loop(1, n_sp)
    def _(d):
        end_copy((s + d) % n_sp, s).wait_send()

    @pl.loop(1, n_sp)
    def _(k):
        for c in range(3):

            @pl.when(jnp.logical_and(has_right, s >= k - 1))
            def _():
                z_copy(0, c, k, (s + n_sp + 1 - k) % n_sp, right).wait_send()

            @pl.when(jnp.logical_and(has_left, s + k - 1 < n_sp))
            def _():
                z_copy(1, c, k, (s + k - 1) % n_sp, left).wait_send()

            @pl.when(s >= k)
            def _():
                y_copy(0, c, k, (s + n_sp - k) % n_sp, g).wait_send()

            @pl.when(s + k < n_sp)
            def _():
                y_copy(1, c, k, (s + k) % n_sp, g).wait_send()


def fused(
    residual,
    state_input,
    gate_input,
    decay_real,
    frequency,
    log_step,
    drive_real,
    drive_imag,
    read_real,
    read_imag,
    skip_gain,
    value_weight,
    glu_weight,
    mix_weight,
    norm_gain,
    mlp_gate,
    mlp_up,
    mlp_down,
):
    n_sp, n_tp = lax.axis_size("sp"), lax.axis_size("tp")
    groups, states, width = drive_real.shape
    flat, chans = groups * states, groups * width
    rows = state_input.shape[0]
    own, depth = residual.shape
    ff, d_loc = mlp_down.shape
    cols = value_weight.shape[1]
    _, _, in_real, in_imag = discretize(decay_real, frequency, log_step, drive_real, drive_imag)
    times = max(1, 128 // states)

    def tiled(x):
        return jnp.concatenate([x.reshape(chans, states)] * times, axis=1)

    step = jnp.exp(log_step)[:, None]
    counts = (lax.iota(jnp.int32, ROWS8) + 1).astype(F32)[:, None]
    pow_real, pow_imag = powers(
        (decay_real * step).reshape(1, flat), (frequency * step).reshape(1, flat), counts
    )
    vmem = pl.BlockSpec(memory_space=pltpu.VMEM)
    hbm = pl.BlockSpec(memory_space=pl.ANY)
    dma = pltpu.SemaphoreType.DMA
    return pl.pallas_call(
        functools.partial(layer_kernel, n_sp, width, states),
        out_shape=jax.ShapeDtypeStruct((own, depth), BF),
        in_specs=[vmem] * 10 + [hbm] * 3 + [vmem] + [hbm] * 3,
        out_specs=vmem,
        scratch_shapes=[
            pltpu.VMEM(value_weight.shape, BF),
            pltpu.VMEM(glu_weight.shape, BF),
            pltpu.VMEM(mix_weight.shape, BF),
            pltpu.VMEM((n_sp * mlp_gate.shape[0], ff), BF),
            pltpu.VMEM((n_sp * mlp_gate.shape[0], ff), BF),
            pltpu.VMEM((n_sp, ff, d_loc), BF),
            pltpu.VMEM((8, chans, flat), BF),
            pltpu.VMEM((rows, flat), F32),
            pltpu.VMEM((rows, flat), F32),
            pltpu.VMEM((6, ROWS8, flat), F32),
            pltpu.VMEM((n_sp, ROWS8, flat), F32),
            pltpu.VMEM((n_tp, rows, chans), BF),
            pltpu.VMEM((1, n_tp, own, depth), BF),
            pltpu.VMEM((1, 2, own, depth), BF),
            pltpu.VMEM((1, own, depth), BF),
            pltpu.VMEM((1, own, depth), BF),
            pltpu.VMEM((own, depth), F32),
            pltpu.VMEM((n_tp, own, depth), BF),
            pltpu.VMEM((n_tp, own, ff), BF),
            pltpu.VMEM((n_sp, n_tp, own, d_loc), BF),
            pltpu.VMEM((n_sp, 2, own, d_loc), BF),
            pltpu.VMEM((n_sp, own, d_loc), BF),
            pltpu.VMEM((n_sp, own, d_loc), BF),
            dma((6,)),
            dma((n_sp,)),
            dma((n_sp,)),
            dma((2, 3, n_sp)),
            dma((2, 3, n_sp)),
            dma((2, 3, n_sp)),
            dma((2, 3, n_sp)),
            dma((2, 3)),
            dma((2, 3)),
            dma((1, 3)),
            dma((1, 3)),
            dma((n_sp, 3)),
            dma((n_sp, 3)),
        ],
        compiler_params=pltpu.CompilerParams(
            collective_id=0, has_side_effects=True, vmem_limit_bytes=60 * 1024 * 1024
        ),
    )(
        residual,
        state_input,
        gate_input,
        pow_real,
        pow_imag,
        tiled(in_real.transpose(0, 2, 1)),
        tiled(in_imag.transpose(0, 2, 1)),
        tiled(read_real),
        tiled(read_imag),
        skip_gain[None, :],
        value_weight,
        glu_weight,
        mix_weight,
        norm_gain[None, :],
        mlp_gate,
        mlp_up,
        mlp_down,
    )


def quick_kernel(
    n_sp,
    width,
    states,
    residual,
    u,
    gate_in,
    pow_real,
    pow_imag,
    in_real,
    in_imag,
    rd_real,
    rd_imag,
    skip,
    value_h,
    glu_h,
    mix_h,
    gain,
    gate_h,
    up_h,
    down_h,
    out,
    value_w,
    glu_w,
    mix_w,
    w_gate,
    w_up,
    w_down,
    wide,
    st_real,
    st_imag,
    masked,
    ends,
    acts,
    part,
    rx_pair,
    relay,
    rx_far,
    inner,
    normed,
    hidden,
    c_part,
    c_pair,
    c_relay,
    c_far,
    load_sem,
    end_send,
    end_recv,
    z_send,
    z_recv,
    y_send,
    y_recv,
    ag_send,
    ag_recv,
    rs_send,
    rs_recv,
    c_send,
    c_recv,
):
    g, s, t = lax.axis_index("grp"), lax.axis_index("sp"), lax.axis_index("tp")
    low, high_bit = t % 2, t // 2
    p = t + 1 - 2 * low
    q = t + 2 - 4 * high_bit
    far = 3 - t
    other = 1 - g
    rows, chans = u.shape
    flat = st_real.shape[1]
    own, depth = residual.shape
    k_loc = gate_h.shape[0]
    ff, d_loc = down_h.shape
    k_half, f_half = k_loc // 2, ff // 2

    barrier = pltpu.get_barrier_semaphore()
    pl.semaphore_signal(barrier, inc=1, device_id={"tp": p})
    pl.semaphore_signal(barrier, inc=1, device_id={"tp": q})
    pl.semaphore_signal(barrier, inc=1, device_id={"grp": other})

    @pl.loop(1, n_sp)
    def _(d):
        pl.semaphore_signal(barrier, inc=1, device_id={"sp": (s + d) % n_sp})

    bufs = (w_gate, w_up, w_down)
    place = pl.ds(pl.multiple_of(s * k_loc, k_loc), k_loc)
    loads = [
        pltpu.make_async_copy(gate_h, w_gate.at[place, :], load_sem.at[0]),
        pltpu.make_async_copy(up_h, w_up.at[place, :], load_sem.at[1]),
        pltpu.make_async_copy(down_h, w_down.at[s], load_sem.at[2]),
        pltpu.make_async_copy(value_h, value_w, load_sem.at[3]),
        pltpu.make_async_copy(glu_h, glu_w, load_sem.at[4]),
        pltpu.make_async_copy(mix_h, mix_w, load_sem.at[5]),
    ]
    for load in loads:
        load.start()
    pl.semaphore_wait(barrier, 3 + n_sp - 1)

    k_piece, d_piece = k_half // PIECES, d_loc // PIECES

    def mine(c, i, origin, half):
        if c < 2:
            row = pl.multiple_of(origin * k_loc + half * k_half + i * k_piece, k_piece)
            return bufs[c].at[pl.ds(row, k_piece), :]
        row = pl.multiple_of(half * f_half, f_half)
        return bufs[c].at[origin, pl.ds(row, f_half), pl.ds(i * d_piece, d_piece)]

    def z_copy(side, c, i, k, origin, target):
        piece = mine(c, i, origin, g)
        return pltpu.make_async_remote_copy(
            src_ref=piece,
            dst_ref=piece,
            send_sem=z_send.at[side, c, i, k],
            recv_sem=z_recv.at[side, c, i, k],
            device_id={"sp": target},
        )

    def y_copy(side, c, i, k, origin, half):
        piece = mine(c, i, origin, half)
        return pltpu.make_async_remote_copy(
            src_ref=piece,
            dst_ref=piece,
            send_sem=y_send.at[side, c, i, k],
            recv_sem=y_recv.at[side, c, i, k],
            device_id={"grp": other},
        )

    def spots(behind, side):
        here = behind if side == 0 else n_sp - 1 - behind
        step = 1 if side == 0 else -1
        return here, step, behind < n_sp - 1

    def order(behind):
        early = [(k, c, i) for k in range(1, behind + 1) for c in (0, 1) for i in range(PIECES)]
        late = [(k, 2, i) for k in range(1, behind + 1) for i in range(PIECES)]
        return early, late

    def send_own(side, c, here, step):
        for i in range(PIECES):
            z_copy(side, c, i, 1, s, here + step).start()

    def own_sends(c):
        loads[c].wait()
        for side in range(2):
            for behind in range(n_sp - 1):
                here, step, onward = spots(behind, side)
                if c < 2 or behind == 0:
                    pl.when(s == here)(functools.partial(send_own, side, c, here, step))

    own_sends(0)

    def pass_on(side, behind, number):
        here, step, onward = spots(behind, side)
        early, late = order(behind)
        k, c, i = (early + late)[number]
        origin = here - step * k
        z_copy(side, c, i, k, origin, here).wait_recv()
        if onward:
            z_copy(side, c, i, k + 1, origin, here + step).start()
        y_copy(side, c, i, k, origin, g).start()
        if onward and number == len(early) - 1:
            send_own(side, 2, here, step)

    def advance(*numbers):
        for number in numbers:
            for side in range(2):
                for behind in range(1, n_sp):
                    here = spots(behind, side)[0]
                    if number < 3 * PIECES * behind:
                        pl.when(s == here)(functools.partial(pass_on, side, behind, number))

    def landed(side, behind, kinds, ks):
        here, step, _ = spots(behind, side)
        for k in ks:
            for c in kinds:
                for i in range(PIECES):
                    y_copy(side, c, i, k, here - step * k, other).wait_recv()

    def finish_sends(side, behind):
        here, step, onward = spots(behind, side)
        for c in range(3):
            for i in range(PIECES):
                for k in range(1, behind + 1):
                    y_copy(side, c, i, k, here - step * k, g).wait_send()
                if onward:
                    for k in range(1, behind + 2):
                        z_copy(side, c, i, k, here - step * (k - 1), here + step).wait_send()

    lanes = in_real.shape[1]
    row_group = lax.broadcasted_iota(jnp.int32, (chans, lanes), 0) // width
    lane = lax.broadcasted_iota(jnp.int32, (chans, lanes), 1)
    for i, ref in enumerate((in_real, in_imag, rd_real, rd_imag)):
        value = ref[...]
        for tile in range(flat // lanes):
            kept = jnp.where(row_group == (lane + tile * lanes) // states, value, 0.0)
            big, small = split(kept)
            at = slice(tile * lanes, (tile + 1) * lanes)
            wide[2 * i, :, at] = big
            wide[2 * i + 1, :, at] = small

    @pl.loop(0, rows // own)
    def _(b):
        at = pl.ds(pl.multiple_of(b * own, own), own)
        x = u[at, :]
        st_real[at, :] = mm(x, wide[0]) + mm(x, wide[1])
        st_imag[at, :] = mm(x, wide[2]) + mm(x, wide[3])

    sub = lax.broadcasted_iota(jnp.int32, (ROWS8, flat), 0)
    for i, reach in enumerate((1, 2, 4)):
        masked[2 * i] = jnp.where(sub >= reach, pow_real[reach - 1 : reach, :], 0.0)
        masked[2 * i + 1] = jnp.where(sub >= reach, pow_imag[reach - 1 : reach, :], 0.0)

    def scan_step(b, carry):
        c_re, c_im = carry
        at = pl.ds(pl.multiple_of(b * ROWS8, ROWS8), ROWS8)
        x_re, x_im = st_real[at, :], st_imag[at, :]
        for i, reach in enumerate((1, 2, 4)):
            m_re, m_im = pltpu.roll(x_re, reach, 0), pltpu.roll(x_im, reach, 0)
            a_re, a_im = masked[2 * i], masked[2 * i + 1]
            x_re, x_im = x_re + a_re * m_re - a_im * m_im, x_im + a_re * m_im + a_im * m_re
        p_re, p_im = pow_real[...], pow_imag[...]
        x_re, x_im = x_re + p_re * c_re - p_im * c_im, x_im + p_re * c_im + p_im * c_re
        st_real[at, :] = x_re
        st_imag[at, :] = x_im
        return x_re[ROWS8 - 1 :, :], x_im[ROWS8 - 1 :, :]

    zero = jnp.zeros((1, flat), F32)
    end_re, end_im = lax.fori_loop(0, rows // ROWS8, scan_step, (zero, zero))
    ends[s, :, :flat] = end_re
    ends[s, :, flat:] = end_im

    def end_copy(target, origin):
        return pltpu.make_async_remote_copy(
            src_ref=ends.at[origin],
            dst_ref=ends.at[origin],
            send_sem=end_send.at[target],
            recv_sem=end_recv.at[origin],
            device_id={"sp": target},
        )

    @pl.loop(1, n_sp)
    def _(d):
        end_copy((s + d) % n_sp, s).start()

    own_sends(1)
    own_sends(2)
    advance(0)
    last_re, last_im = pow_real[ROWS8 - 1 :, :], pow_imag[ROWS8 - 1 :, :]
    long_re, long_im = last_re, last_im
    reach = ROWS8
    while reach < rows:
        long_re, long_im = long_re * long_re - long_im * long_im, 2.0 * long_re * long_im
        reach *= 2

    @pl.loop(1, n_sp)
    def _(d):
        end_copy((s + d) % n_sp, (s + d) % n_sp).wait_recv()

    def carry_step(j, carry):
        c_re, c_im = carry
        e_re, e_im = ends[j, :, :flat], ends[j, :, flat:]
        n_re = long_re * c_re - long_im * c_im + e_re
        n_im = long_re * c_im + long_im * c_re + e_im
        return jnp.where(j < s, n_re, c_re), jnp.where(j < s, n_im, c_im)

    carry = lax.fori_loop(0, n_sp - 1, carry_step, (zero, zero))

    def lift(b, carry):
        c_re, c_im = carry
        at = pl.ds(pl.multiple_of(b * ROWS8, ROWS8), ROWS8)
        p_re, p_im = pow_real[...], pow_imag[...]
        st_real[at, :] = st_real[at, :] + p_re * c_re - p_im * c_im
        st_imag[at, :] = st_imag[at, :] + p_re * c_im + p_im * c_re
        return last_re * c_re - last_im * c_im, last_re * c_im + last_im * c_re

    lax.fori_loop(0, rows // ROWS8, lift, carry)
    advance(1)

    @pl.loop(0, rows // own)
    def _(b):
        at = pl.ds(pl.multiple_of(b * own, own), own)
        high, small = split(st_real[at, :])
        y = mm_t(high, wide[4]) + mm_t(small, wide[4]) + mm_t(high, wide[5])
        high, small = split(st_imag[at, :])
        y = y - (mm_t(high, wide[6]) + mm_t(small, wide[6]) + mm_t(high, wide[7]))
        y = y + skip[...] * u[at, :].astype(F32)
        acts[t, at, :] = jax.nn.gelu(y).astype(BF)

    def gather_tp(buf, lane_no, between, later):
        def copy(slot, kind, target):
            return pltpu.make_async_remote_copy(
                src_ref=buf.at[slot],
                dst_ref=buf.at[slot],
                send_sem=ag_send.at[lane_no, kind],
                recv_sem=ag_recv.at[lane_no, kind],
                device_id={"tp": target},
            )

        sent = [copy(t, 0, q), copy(t, 1, p)]
        for item in sent:
            item.start()
        between()
        copy(q, 0, q).wait_recv()
        relayed = copy(q, 2, p)
        relayed.start()
        later()
        copy(p, 1, p).wait_recv()
        copy(far, 2, p).wait_recv()
        return sent + [relayed]

    def scatter_tp(lane_no, block, middle, between):
        def pair(index):
            return pltpu.make_async_remote_copy(
                src_ref=part.at[lane_no, (far, p)[index]],
                dst_ref=rx_pair.at[lane_no, index],
                send_sem=rs_send.at[lane_no, index],
                recv_sem=rs_recv.at[lane_no, index],
                device_id={"tp": p},
            )

        across = pltpu.make_async_remote_copy(
            src_ref=relay.at[lane_no],
            dst_ref=rx_far.at[lane_no],
            send_sem=rs_send.at[lane_no, 2],
            recv_sem=rs_recv.at[lane_no, 2],
            device_id={"tp": q},
        )
        pairs = [pair(0), pair(1)]
        block(far)
        pairs[0].start()
        block(p)
        pairs[1].start()
        block(q)
        middle()
        pairs[0].wait_recv()
        relay[lane_no] = (part[lane_no, q].astype(F32) + rx_pair[lane_no, 0].astype(F32)).astype(BF)
        across.start()
        block(t)
        between()
        pairs[1].wait_recv()
        across.wait_recv()
        return pairs + [across]

    def total(lane_no):
        near = part[lane_no, t].astype(F32) + rx_pair[lane_no, 1].astype(F32)
        return near + rx_far[lane_no].astype(F32)

    pending = gather_tp(acts, 0, lambda: advance(2), lambda: advance(3))
    for load in loads[3:]:
        load.wait()
    n_tp = acts.shape[0]

    def mix_block(r):
        at = pl.ds(pl.multiple_of(r * own, own), own)
        value = jnp.zeros((own, value_w.shape[1]), F32)
        gated = value
        for j in range(n_tp):
            a = acts[j, at, :]
            value = value + mm(a, value_w[j * chans : (j + 1) * chans, :])
            gated = gated + mm(a, glu_w[j * chans : (j + 1) * chans, :])
        mixed = jax.nn.sigmoid(gate_in[at, :].astype(F32)) * value * jax.nn.sigmoid(gated)
        part[0, r] = mm(mixed.astype(BF), mix_w[...]).astype(BF)

    pending += scatter_tp(0, mix_block, lambda: advance(4), lambda: advance(5, 6, 7))
    inner[...] = residual[...].astype(F32) + total(0)
    x = inner[...]
    scale = lax.rsqrt(jnp.mean(x * x, axis=-1, keepdims=True) + EPSILON)
    normed[t] = (x * scale * gain[...]).astype(BF)

    pending += gather_tp(normed, 1, lambda: advance(8, 9), lambda: advance(10))
    advance(11, 12)
    for side in range(2):
        for behind in range(1, n_sp):
            here = spots(behind, side)[0]
            ready = functools.partial(landed, side, behind, (0, 1), range(1, behind + 1))
            pl.when(s == here)(ready)

    @pl.loop(0, n_tp)
    def _(r):
        x = normed[r]
        hidden[r] = (jax.nn.silu(mm(x, w_gate[...])) * mm(x, w_up[...])).astype(BF)

    def col_pair(o, h, index):
        return pltpu.make_async_remote_copy(
            src_ref=c_part.at[o, h, (far, p)[index]],
            dst_ref=c_pair.at[o, h, index],
            send_sem=c_send.at[o, h, index],
            recv_sem=c_recv.at[o, h, index],
            device_id={"tp": p},
        )

    def col_far(o, h):
        return pltpu.make_async_remote_copy(
            src_ref=c_relay.at[o, h],
            dst_ref=c_far.at[o, h],
            send_sem=c_send.at[o, h, 2],
            recv_sem=c_recv.at[o, h, 2],
            device_id={"tp": q},
        )

    def column(o):
        for h in range(PIECES):
            weight = w_down.at[o, :, h * d_piece : (h + 1) * d_piece]
            for r, index in ((far, 0), (p, 1), (q, None), (t, None)):
                c_part[o, h, r] = mm(hidden[r], weight[...]).astype(BF)
                if index is not None:
                    col_pair(o, h, index).start()
        for h in range(PIECES):
            col_pair(o, h, 0).wait_recv()
            both = c_part[o, h, q].astype(F32) + c_pair[o, h, 0].astype(F32)
            c_relay[o, h] = both.astype(BF)
            col_far(o, h).start()

    def settle(o):
        for h in range(PIECES):
            col_pair(o, h, 1).wait_recv()
            col_far(o, h).wait_recv()
            near = c_part[o, h, t].astype(F32) + c_pair[o, h, 1].astype(F32)
            at = pl.ds(pl.multiple_of(o * d_loc + h * d_piece, d_piece), d_piece)
            out[:, at] = (inner[:, at] + 0.5 * (near + c_far[o, h].astype(F32))).astype(BF)

    def both_sides(k, work):
        for side in range(2):
            for behind in range(k, n_sp):
                here, step, _ = spots(behind, side)
                pl.when(s == here)(functools.partial(work, side, behind, k, here - step * k))

    def next_column(side, behind, k, origin):
        landed(side, behind, (2,), (k,))
        column(origin)

    def next_settle(side, behind, k, origin):
        settle(origin)

    column(s)
    advance(13)
    for k in range(1, n_sp):
        upto = range(12 + 2 * k, min(12 + 2 * k + 2, 3 * PIECES * (n_sp - 1)))
        advance(*upto)
        both_sides(k, next_column)
        if k == 1:
            settle(s)
        else:
            both_sides(k - 1, next_settle)
    both_sides(n_sp - 1, next_settle)

    @pl.loop(0, n_sp)
    def _(o):
        for h in range(PIECES):
            col_pair(o, h, 0).wait_send()
            col_pair(o, h, 1).wait_send()
            col_far(o, h).wait_send()

    for item in pending:
        item.wait_send()

    @pl.loop(1, n_sp)
    def _(d):
        end_copy((s + d) % n_sp, s).wait_send()

    for side in range(2):
        for behind in range(n_sp):
            here = spots(behind, side)[0]
            pl.when(s == here)(functools.partial(finish_sends, side, behind))


def quick(
    residual,
    state_input,
    gate_input,
    decay_real,
    frequency,
    log_step,
    drive_real,
    drive_imag,
    read_real,
    read_imag,
    skip_gain,
    value_weight,
    glu_weight,
    mix_weight,
    norm_gain,
    mlp_gate,
    mlp_up,
    mlp_down,
):
    n_sp, n_tp = lax.axis_size("sp"), lax.axis_size("tp")
    groups, states, width = drive_real.shape
    flat, chans = groups * states, groups * width
    rows = state_input.shape[0]
    own, depth = residual.shape
    ff, d_loc = mlp_down.shape
    cols = value_weight.shape[1]
    _, _, in_real, in_imag = discretize(decay_real, frequency, log_step, drive_real, drive_imag)
    times = max(1, 128 // states)

    def tiled(x):
        return jnp.concatenate([x.reshape(chans, states)] * times, axis=1)

    step = jnp.exp(log_step)[:, None]
    counts = (lax.iota(jnp.int32, ROWS8) + 1).astype(F32)[:, None]
    pow_real, pow_imag = powers(
        (decay_real * step).reshape(1, flat), (frequency * step).reshape(1, flat), counts
    )
    vmem = pl.BlockSpec(memory_space=pltpu.VMEM)
    hbm = pl.BlockSpec(memory_space=pl.ANY)
    dma = pltpu.SemaphoreType.DMA
    return pl.pallas_call(
        functools.partial(quick_kernel, n_sp, width, states),
        out_shape=jax.ShapeDtypeStruct((own, depth), BF),
        in_specs=[vmem] * 10 + [hbm] * 3 + [vmem] + [hbm] * 3,
        out_specs=vmem,
        scratch_shapes=[
            pltpu.VMEM(value_weight.shape, BF),
            pltpu.VMEM(glu_weight.shape, BF),
            pltpu.VMEM(mix_weight.shape, BF),
            pltpu.VMEM((n_sp * mlp_gate.shape[0], ff), BF),
            pltpu.VMEM((n_sp * mlp_gate.shape[0], ff), BF),
            pltpu.VMEM((n_sp, ff, d_loc), BF),
            pltpu.VMEM((8, chans, flat), BF),
            pltpu.VMEM((rows, flat), F32),
            pltpu.VMEM((rows, flat), F32),
            pltpu.VMEM((6, ROWS8, flat), F32),
            pltpu.VMEM((n_sp, 1, 2 * flat), F32),
            pltpu.VMEM((n_tp, rows, chans), BF),
            pltpu.VMEM((1, n_tp, own, depth), BF),
            pltpu.VMEM((1, 2, own, depth), BF),
            pltpu.VMEM((1, own, depth), BF),
            pltpu.VMEM((1, own, depth), BF),
            pltpu.VMEM((own, depth), F32),
            pltpu.VMEM((n_tp, own, depth), BF),
            pltpu.VMEM((n_tp, own, ff), BF),
            pltpu.VMEM((n_sp, PIECES, n_tp, own, d_loc // PIECES), BF),
            pltpu.VMEM((n_sp, PIECES, 2, own, d_loc // PIECES), BF),
            pltpu.VMEM((n_sp, PIECES, own, d_loc // PIECES), BF),
            pltpu.VMEM((n_sp, PIECES, own, d_loc // PIECES), BF),
            dma((6,)),
            dma((n_sp,)),
            dma((n_sp,)),
            dma((2, 3, PIECES, n_sp)),
            dma((2, 3, PIECES, n_sp)),
            dma((2, 3, PIECES, n_sp)),
            dma((2, 3, PIECES, n_sp)),
            dma((2, 3)),
            dma((2, 3)),
            dma((1, 3)),
            dma((1, 3)),
            dma((n_sp, PIECES, 3)),
            dma((n_sp, PIECES, 3)),
        ],
        compiler_params=pltpu.CompilerParams(
            collective_id=0, has_side_effects=True, vmem_limit_bytes=60 * 1024 * 1024
        ),
    )(
        residual,
        state_input,
        gate_input,
        pow_real,
        pow_imag,
        tiled(in_real.transpose(0, 2, 1)),
        tiled(in_imag.transpose(0, 2, 1)),
        tiled(read_real),
        tiled(read_imag),
        skip_gain[None, :],
        value_weight,
        glu_weight,
        mix_weight,
        norm_gain[None, :],
        mlp_gate,
        mlp_up,
        mlp_down,
    )


def solution(mesh):
    placed = (
        P(("grp", "sp", "tp"), None),
        P(("grp", "sp"), "tp"),
        P(("grp", "sp"), "tp"),
        P("tp", None),
        P("tp", None),
        P("tp"),
        P("tp", None, None),
        P("tp", None, None),
        P("tp", None, None),
        P("tp", None, None),
        P("tp"),
        P(None, "tp"),
        P(None, "tp"),
        P("tp", None),
        P(),
        P("sp", "tp"),
        P("sp", "tp"),
        P("tp", "sp"),
    )
    body = shards
    if (mesh.shape["tp"], mesh.shape["grp"]) == (4, 2):
        body = quick if mesh.shape["sp"] == 4 else fused
    return jax.shard_map(
        body, mesh=mesh, in_specs=placed, out_specs=P(("grp", "sp", "tp"), None), check_vma=False
    )
```

```python
import functools
import jax
import jax.numpy as jnp
from jax import lax
from jax.experimental import pallas as pl
from jax.experimental.pallas import tpu as pltpu
from jax.sharding import PartitionSpec as P

BF = jnp.bfloat16
F32 = jnp.float32
ROWS8 = 8
PIECES = 4
HALVES = 2

HIGH = lax.Precision.HIGHEST
EPSILON = 1e-06


def carried_in(value, axis, join, neutral):
    count, mine = (lax.axis_size(axis), lax.axis_index(axis))
    pieces = jax.tree.map(lambda part: lax.all_gather(part, axis), value)
    subtotal = jax.tree.map(
        lambda part, zero: jnp.full_like(part, 0) + jnp.asarray(zero, part.dtype), value, neutral
    )

    def step(position, subtotal):
        longer = join(subtotal, jax.tree.map(lambda part: part[position], pieces))
        return jax.tree.map(lambda new, old: jnp.where(position < mine, new, old), longer, subtotal)

    return lax.fori_loop(0, count - 1, step, subtotal)


def discretize(decay_real, frequency, log_step, drive_real, drive_imag):
    step = jnp.exp(log_step)[:, None]
    magnitude = jnp.exp(decay_real * step)
    turned = frequency * step
    bar_real = magnitude * jnp.cos(turned)
    bar_imag = magnitude * jnp.sin(turned)
    modulus = decay_real * decay_real + frequency * frequency
    ratio_real = ((bar_real - 1.0) * decay_real + bar_imag * frequency) / modulus
    ratio_imag = (bar_imag * decay_real - (bar_real - 1.0) * frequency) / modulus
    in_real = ratio_real[..., None] * drive_real - ratio_imag[..., None] * drive_imag
    in_imag = ratio_real[..., None] * drive_imag + ratio_imag[..., None] * drive_real
    return (bar_real, bar_imag, in_real, in_imag)


def combine(earlier, later):
    real_one, imag_one, state_real_one, state_imag_one = earlier
    real_two, imag_two, state_real_two, state_imag_two = later
    return (
        real_one * real_two - imag_one * imag_two,
        real_one * imag_two + imag_one * real_two,
        real_two * state_real_one - imag_two * state_imag_one + state_real_two,
        real_two * state_imag_one + imag_two * state_real_one + state_imag_two,
    )


def powers(log_rate, angle_rate, count):
    return (
        jnp.exp(log_rate * count) * jnp.cos(angle_rate * count),
        jnp.exp(log_rate * count) * jnp.sin(angle_rate * count),
    )


def block_states(flat_inputs, decay_real, frequency, log_step, in_real, in_imag):
    rows = flat_inputs.shape[0]
    groups, states, width = in_real.shape
    flat = groups * states
    eye = jnp.eye(groups, dtype=jnp.float32)
    wide_real = jnp.einsum("gph,gk->ghkp", in_real, eye).reshape(groups * width, flat)
    wide_imag = jnp.einsum("gph,gk->ghkp", in_imag, eye).reshape(groups * width, flat)
    state_real = jnp.dot(flat_inputs, wide_real, precision=HIGH)
    state_imag = jnp.dot(flat_inputs, wide_imag, precision=HIGH)
    step = jnp.exp(log_step)[:, None]
    log_rate = (decay_real * step).reshape(1, flat)
    angle_rate = (frequency * step).reshape(1, flat)
    reach = 1
    while reach < rows:
        lift_real, lift_imag = powers(log_rate, angle_rate, float(reach))
        blank = jnp.zeros((reach, flat), jnp.float32)
        moved_real = jnp.concatenate([blank, state_real[: rows - reach]], axis=0)
        moved_imag = jnp.concatenate([blank, state_imag[: rows - reach]], axis=0)
        state_real, state_imag = (
            state_real + lift_real * moved_real - lift_imag * moved_imag,
            state_imag + lift_real * moved_imag + lift_imag * moved_real,
        )
        reach = reach * 2
    counts = (lax.iota(jnp.int32, rows) + 1).astype(jnp.float32)[:, None]
    power_real, power_imag = powers(log_rate, angle_rate, counts)
    return (power_real, power_imag, state_real, state_imag)


def readout(state_real, state_imag, read_real, read_imag, flat_inputs, skip_gain):
    groups, width, states = read_real.shape
    eye = jnp.eye(groups, dtype=jnp.float32)
    wide_real = jnp.einsum("ghp,gk->gpkh", read_real, eye).reshape(groups * states, groups * width)
    wide_imag = jnp.einsum("ghp,gk->gpkh", read_imag, eye).reshape(groups * states, groups * width)
    output = jnp.dot(state_real, wide_real, precision=HIGH) - jnp.dot(
        state_imag, wide_imag, precision=HIGH
    )
    output = output + skip_gain * flat_inputs
    return jax.nn.gelu(output).astype(jnp.bfloat16)


def normalize(inner, norm_gain):
    scale = lax.rsqrt(jnp.mean(inner * inner, axis=-1, keepdims=True) + EPSILON)
    return (inner * scale * norm_gain).astype(jnp.bfloat16)


def shards(
    residual,
    state_input,
    gate_input,
    decay_real,
    frequency,
    log_step,
    drive_real,
    drive_imag,
    read_real,
    read_imag,
    skip_gain,
    value_weight,
    glu_weight,
    mix_weight,
    norm_gain,
    mlp_gate,
    mlp_up,
    mlp_down,
):
    bar_real, bar_imag, in_real, in_imag = discretize(
        decay_real, frequency, log_step, drive_real, drive_imag
    )
    flat_inputs = state_input.astype(jnp.float32)
    power_real, power_imag, local_real, local_imag = block_states(
        flat_inputs, decay_real, frequency, log_step, in_real, in_imag
    )
    ends = (power_real[-1], power_imag[-1], local_real[-1], local_imag[-1])
    ones = jnp.ones_like(ends[0])
    zeros = jnp.zeros_like(ends[0])
    incoming = carried_in(
        (ends[0], ends[1], ends[2], ends[3]), "sp", combine, (ones, zeros, zeros, zeros)
    )
    carry_real = incoming[2]
    carry_imag = incoming[3]
    state_real = local_real + power_real * carry_real - power_imag * carry_imag
    state_imag = local_imag + power_real * carry_imag + power_imag * carry_real
    acts = readout(state_real, state_imag, read_real, read_imag, flat_inputs, skip_gain)
    piece = lax.all_gather(acts, "tp", axis=1, tiled=True)
    value = jnp.dot(piece, value_weight, preferred_element_type=jnp.float32)
    gated = jnp.dot(piece, glu_weight, preferred_element_type=jnp.float32)
    mixed = (jax.nn.sigmoid(gate_input.astype(jnp.float32)) * value * jax.nn.sigmoid(gated)).astype(
        jnp.bfloat16
    )
    branch = lax.psum_scatter(
        jnp.dot(mixed, mix_weight, preferred_element_type=jnp.float32).astype(jnp.bfloat16),
        "tp",
        scatter_dimension=0,
        tiled=True,
    ).astype(jnp.float32)
    inner = residual.astype(jnp.float32) + branch
    normed = lax.all_gather(normalize(inner, norm_gain), "tp", axis=0, tiled=True)
    hidden_gate = jnp.dot(
        normed,
        lax.all_gather(mlp_gate, "sp", axis=0, tiled=True),
        preferred_element_type=jnp.float32,
    )
    hidden_up = jnp.dot(
        normed, lax.all_gather(mlp_up, "sp", axis=0, tiled=True), preferred_element_type=jnp.float32
    )
    hidden = (jax.nn.silu(hidden_gate) * hidden_up).astype(jnp.bfloat16)
    down = jnp.dot(
        hidden,
        lax.all_gather(mlp_down, "sp", axis=1, tiled=True),
        preferred_element_type=jnp.float32,
    )
    down_own = lax.psum_scatter(
        down.astype(jnp.bfloat16), "tp", scatter_dimension=0, tiled=True
    ).astype(jnp.float32)
    return (inner + 0.5 * down_own).astype(jnp.bfloat16)


def mm(a, b):
    return jnp.dot(a, b, preferred_element_type=F32)


def mm_t(a, b):
    return lax.dot_general(a, b, (((1,), (1,)), ((), ())), preferred_element_type=F32)


def split(x):
    high = x.astype(BF)
    return high, (x - high.astype(F32)).astype(BF)


def layer_kernel(
    n_sp,
    width,
    states,
    residual,
    u,
    gate_in,
    pow_real,
    pow_imag,
    in_real,
    in_imag,
    rd_real,
    rd_imag,
    skip,
    value_h,
    glu_h,
    mix_h,
    gain,
    gate_h,
    up_h,
    down_h,
    out,
    value_w,
    glu_w,
    mix_w,
    w_gate,
    w_up,
    w_down,
    wide,
    st_real,
    st_imag,
    masked,
    ends,
    acts,
    part,
    rx_pair,
    relay,
    rx_far,
    inner,
    normed,
    hidden,
    c_part,
    c_pair,
    c_relay,
    c_far,
    load_sem,
    end_send,
    end_recv,
    z_send,
    z_recv,
    y_send,
    y_recv,
    ag_send,
    ag_recv,
    rs_send,
    rs_recv,
    c_send,
    c_recv,
):
    g, s, t = lax.axis_index("grp"), lax.axis_index("sp"), lax.axis_index("tp")
    low, high_bit = t % 2, t // 2
    p = t + 1 - 2 * low
    q = t + 2 - 4 * high_bit
    far = 3 - t
    other = 1 - g
    rows, chans = u.shape
    flat = st_real.shape[1]
    own, depth = residual.shape
    k_loc = gate_h.shape[0]
    ff, d_loc = down_h.shape
    k_half, f_half = k_loc // 2, ff // 2

    barrier = pltpu.get_barrier_semaphore()
    pl.semaphore_signal(barrier, inc=1, device_id={"tp": p})
    pl.semaphore_signal(barrier, inc=1, device_id={"tp": q})
    pl.semaphore_signal(barrier, inc=1, device_id={"grp": other})

    @pl.loop(1, n_sp)
    def _(d):
        pl.semaphore_signal(barrier, inc=1, device_id={"sp": (s + d) % n_sp})

    def mine(ref, c, origin, half):
        if c < 2:
            return ref.at[pl.ds(pl.multiple_of(origin * k_loc + half * k_half, k_half), k_half), :]
        return ref.at[origin, pl.ds(pl.multiple_of(half * f_half, f_half), f_half), :]

    bufs = (w_gate, w_up, w_down)
    place = pl.ds(pl.multiple_of(s * k_loc, k_loc), k_loc)
    loads = [
        pltpu.make_async_copy(gate_h, w_gate.at[place, :], load_sem.at[0]),
        pltpu.make_async_copy(up_h, w_up.at[place, :], load_sem.at[1]),
        pltpu.make_async_copy(down_h, w_down.at[s], load_sem.at[2]),
        pltpu.make_async_copy(value_h, value_w, load_sem.at[3]),
        pltpu.make_async_copy(glu_h, glu_w, load_sem.at[4]),
        pltpu.make_async_copy(mix_h, mix_w, load_sem.at[5]),
    ]
    for load in loads:
        load.start()
    pl.semaphore_wait(barrier, 3 + n_sp - 1)

    def z_copy(side, c, k, origin, target):
        piece = mine(bufs[c], c, origin, g)
        return pltpu.make_async_remote_copy(
            src_ref=piece,
            dst_ref=piece,
            send_sem=z_send.at[side, c, k],
            recv_sem=z_recv.at[side, c, k],
            device_id={"sp": target},
        )

    def y_copy(side, c, k, origin, half):
        piece = mine(bufs[c], c, origin, half)
        return pltpu.make_async_remote_copy(
            src_ref=piece,
            dst_ref=piece,
            send_sem=y_send.at[side, c, k],
            recv_sem=y_recv.at[side, c, k],
            device_id={"grp": other},
        )

    right, left = (s + 1) % n_sp, (s + n_sp - 1) % n_sp
    has_right, has_left = s < n_sp - 1, s > 0

    for c in range(3):
        loads[c].wait()

        @pl.when(has_right)
        def _():
            z_copy(0, c, 1, s, right).start()

        @pl.when(has_left)
        def _():
            z_copy(1, c, 1, s, left).start()

    def onward(c, k):
        @pl.when(s >= k)
        def _():
            origin = (s + n_sp - k) % n_sp
            z_copy(0, c, k, origin, right).wait_recv()

            @pl.when(has_right)
            def _():
                z_copy(0, c, k + 1, origin, right).start()

            y_copy(0, c, k, origin, g).start()

        @pl.when(s + k < n_sp)
        def _():
            origin = (s + k) % n_sp
            z_copy(1, c, k, origin, left).wait_recv()

            @pl.when(has_left)
            def _():
                z_copy(1, c, k + 1, origin, left).start()

            y_copy(1, c, k, origin, g).start()

    def arrived(c):
        @pl.loop(1, n_sp)
        def _(k):
            @pl.when(s >= k)
            def _():
                y_copy(0, c, k, (s + n_sp - k) % n_sp, other).wait_recv()

            @pl.when(s + k < n_sp)
            def _():
                y_copy(1, c, k, (s + k) % n_sp, other).wait_recv()

    lanes = in_real.shape[1]
    row_group = lax.broadcasted_iota(jnp.int32, (chans, lanes), 0) // width
    lane = lax.broadcasted_iota(jnp.int32, (chans, lanes), 1)
    for i, ref in enumerate((in_real, in_imag, rd_real, rd_imag)):
        value = ref[...]
        for tile in range(flat // lanes):
            kept = jnp.where(row_group == (lane + tile * lanes) // states, value, 0.0)
            big, small = split(kept)
            at = slice(tile * lanes, (tile + 1) * lanes)
            wide[2 * i, :, at] = big
            wide[2 * i + 1, :, at] = small

    @pl.loop(0, rows // own)
    def _(b):
        at = pl.ds(pl.multiple_of(b * own, own), own)
        x = u[at, :]
        st_real[at, :] = mm(x, wide[0]) + mm(x, wide[1])
        st_imag[at, :] = mm(x, wide[2]) + mm(x, wide[3])

    sub = lax.broadcasted_iota(jnp.int32, (ROWS8, flat), 0)
    for i, reach in enumerate((1, 2, 4)):
        masked[2 * i] = jnp.where(sub >= reach, pow_real[reach - 1 : reach, :], 0.0)
        masked[2 * i + 1] = jnp.where(sub >= reach, pow_imag[reach - 1 : reach, :], 0.0)

    def scan_step(b, carry):
        c_re, c_im = carry
        at = pl.ds(pl.multiple_of(b * ROWS8, ROWS8), ROWS8)
        x_re, x_im = st_real[at, :], st_imag[at, :]
        for i, reach in enumerate((1, 2, 4)):
            m_re, m_im = pltpu.roll(x_re, reach, 0), pltpu.roll(x_im, reach, 0)
            a_re, a_im = masked[2 * i], masked[2 * i + 1]
            x_re, x_im = x_re + a_re * m_re - a_im * m_im, x_im + a_re * m_im + a_im * m_re
        p_re, p_im = pow_real[...], pow_imag[...]
        x_re, x_im = x_re + p_re * c_re - p_im * c_im, x_im + p_re * c_im + p_im * c_re
        st_real[at, :] = x_re
        st_imag[at, :] = x_im
        return x_re[ROWS8 - 1 :, :], x_im[ROWS8 - 1 :, :]

    zero = jnp.zeros((1, flat), F32)
    end_re, end_im = lax.fori_loop(0, rows // ROWS8, scan_step, (zero, zero))
    ends[s, 0:1, :] = end_re
    ends[s, 1:2, :] = end_im

    def end_copy(target, origin):
        return pltpu.make_async_remote_copy(
            src_ref=ends.at[origin],
            dst_ref=ends.at[origin],
            send_sem=end_send.at[target],
            recv_sem=end_recv.at[origin],
            device_id={"sp": target},
        )

    @pl.loop(1, n_sp)
    def _(d):
        end_copy((s + d) % n_sp, s).start()

    onward(0, 1)
    last_re, last_im = pow_real[ROWS8 - 1 :, :], pow_imag[ROWS8 - 1 :, :]
    long_re, long_im = last_re, last_im
    reach = ROWS8
    while reach < rows:
        long_re, long_im = long_re * long_re - long_im * long_im, 2.0 * long_re * long_im
        reach *= 2

    @pl.loop(1, n_sp)
    def _(d):
        end_copy((s + d) % n_sp, (s + d) % n_sp).wait_recv()

    def carry_step(j, carry):
        c_re, c_im = carry
        e_re, e_im = ends[j, 0:1, :], ends[j, 1:2, :]
        n_re = long_re * c_re - long_im * c_im + e_re
        n_im = long_re * c_im + long_im * c_re + e_im
        return jnp.where(j < s, n_re, c_re), jnp.where(j < s, n_im, c_im)

    carry = lax.fori_loop(0, n_sp - 1, carry_step, (zero, zero))

    def lift(b, carry):
        c_re, c_im = carry
        at = pl.ds(pl.multiple_of(b * ROWS8, ROWS8), ROWS8)
        p_re, p_im = pow_real[...], pow_imag[...]
        st_real[at, :] = st_real[at, :] + p_re * c_re - p_im * c_im
        st_imag[at, :] = st_imag[at, :] + p_re * c_im + p_im * c_re
        return last_re * c_re - last_im * c_im, last_re * c_im + last_im * c_re

    lax.fori_loop(0, rows // ROWS8, lift, carry)

    @pl.loop(0, rows // own)
    def _(b):
        at = pl.ds(pl.multiple_of(b * own, own), own)
        high, small = split(st_real[at, :])
        y = mm_t(high, wide[4]) + mm_t(small, wide[4]) + mm_t(high, wide[5])
        high, small = split(st_imag[at, :])
        y = y - (mm_t(high, wide[6]) + mm_t(small, wide[6]) + mm_t(high, wide[7]))
        y = y + skip[...] * u[at, :].astype(F32)
        acts[t, at, :] = jax.nn.gelu(y).astype(BF)

    def gather_tp(buf, lane_no, between):
        def copy(slot, kind, target):
            return pltpu.make_async_remote_copy(
                src_ref=buf.at[slot],
                dst_ref=buf.at[slot],
                send_sem=ag_send.at[lane_no, kind],
                recv_sem=ag_recv.at[lane_no, kind],
                device_id={"tp": target},
            )

        sent = [copy(t, 0, q), copy(t, 1, p)]
        for item in sent:
            item.start()
        between()
        copy(q, 0, q).wait_recv()
        relayed = copy(q, 2, p)
        relayed.start()
        copy(p, 1, p).wait_recv()
        copy(far, 2, p).wait_recv()
        return sent + [relayed]

    def scatter_tp(lane_no, block, middle, between):
        def pair(index):
            return pltpu.make_async_remote_copy(
                src_ref=part.at[lane_no, (far, p)[index]],
                dst_ref=rx_pair.at[lane_no, index],
                send_sem=rs_send.at[lane_no, index],
                recv_sem=rs_recv.at[lane_no, index],
                device_id={"tp": p},
            )

        across = pltpu.make_async_remote_copy(
            src_ref=relay.at[lane_no],
            dst_ref=rx_far.at[lane_no],
            send_sem=rs_send.at[lane_no, 2],
            recv_sem=rs_recv.at[lane_no, 2],
            device_id={"tp": q},
        )
        pairs = [pair(0), pair(1)]
        block(far)
        pairs[0].start()
        block(p)
        pairs[1].start()
        block(q)
        middle()
        pairs[0].wait_recv()
        relay[lane_no] = (part[lane_no, q].astype(F32) + rx_pair[lane_no, 0].astype(F32)).astype(BF)
        across.start()
        block(t)
        between()
        pairs[1].wait_recv()
        across.wait_recv()
        return pairs + [across]

    def total(lane_no):
        near = part[lane_no, t].astype(F32) + rx_pair[lane_no, 1].astype(F32)
        return near + rx_far[lane_no].astype(F32)

    def first_forward():
        onward(1, 1)

    pending = gather_tp(acts, 0, first_forward)
    for load in loads[3:]:
        load.wait()
    n_tp = acts.shape[0]

    def mix_block(r):
        at = pl.ds(pl.multiple_of(r * own, own), own)
        value = jnp.zeros((own, value_w.shape[1]), F32)
        gated = value
        for j in range(n_tp):
            a = acts[j, at, :]
            value = value + mm(a, value_w[j * chans : (j + 1) * chans, :])
            gated = gated + mm(a, glu_w[j * chans : (j + 1) * chans, :])
        mixed = jax.nn.sigmoid(gate_in[at, :].astype(F32)) * value * jax.nn.sigmoid(gated)
        part[0, r] = mm(mixed.astype(BF), mix_w[...]).astype(BF)

    def third_forward():
        if n_sp > 2:
            onward(0, 2)

    pending += scatter_tp(0, mix_block, lambda: onward(2, 1), third_forward)
    inner[...] = residual[...].astype(F32) + total(0)
    x = inner[...]
    scale = lax.rsqrt(jnp.mean(x * x, axis=-1, keepdims=True) + EPSILON)
    normed[t] = (x * scale * gain[...]).astype(BF)

    def second_forward():
        if n_sp > 2:
            onward(1, 2)

    pending += gather_tp(normed, 1, second_forward)
    if n_sp > 2:
        onward(2, 2)

    @pl.loop(3, n_sp)
    def _(k):
        onward(0, k)
        onward(1, k)
        onward(2, k)

    arrived(0)
    arrived(1)

    @pl.loop(0, n_tp)
    def _(r):
        x = normed[r]
        hidden[r] = (jax.nn.silu(mm(x, w_gate[...])) * mm(x, w_up[...])).astype(BF)

    def col_pair(o, index):
        return pltpu.make_async_remote_copy(
            src_ref=c_part.at[o, (far, p)[index]],
            dst_ref=c_pair.at[o, index],
            send_sem=c_send.at[o, index],
            recv_sem=c_recv.at[o, index],
            device_id={"tp": p},
        )

    def col_far(o):
        return pltpu.make_async_remote_copy(
            src_ref=c_relay.at[o],
            dst_ref=c_far.at[o],
            send_sem=c_send.at[o, 2],
            recv_sem=c_recv.at[o, 2],
            device_id={"tp": q},
        )

    def column(o):
        weight = w_down.at[o]
        c_part[o, far] = mm(hidden[far], weight[...]).astype(BF)
        col_pair(o, 0).start()
        c_part[o, q] = mm(hidden[q], weight[...]).astype(BF)
        c_part[o, p] = mm(hidden[p], weight[...]).astype(BF)
        col_pair(o, 1).start()
        col_pair(o, 0).wait_recv()
        c_relay[o] = (c_part[o, q].astype(F32) + c_pair[o, 0].astype(F32)).astype(BF)
        col_far(o).start()
        c_part[o, t] = mm(hidden[t], weight[...]).astype(BF)

    column(s)

    @pl.loop(1, n_sp)
    def _(k):
        @pl.when(s >= k)
        def _():
            origin = (s + n_sp - k) % n_sp
            y_copy(0, 2, k, origin, other).wait_recv()
            column(origin)

        @pl.when(s + k < n_sp)
        def _():
            origin = (s + k) % n_sp
            y_copy(1, 2, k, origin, other).wait_recv()
            column(origin)

    for o in range(n_sp):
        col_pair(o, 1).wait_recv()
        col_far(o).wait_recv()
        near = c_part[o, t].astype(F32) + c_pair[o, 1].astype(F32)
        at = slice(o * d_loc, (o + 1) * d_loc)
        out[:, at] = (inner[:, at] + 0.5 * (near + c_far[o].astype(F32))).astype(BF)

    @pl.loop(0, n_sp)
    def _(o):
        col_pair(o, 0).wait_send()
        col_pair(o, 1).wait_send()
        col_far(o).wait_send()

    for item in pending:
        item.wait_send()

    @pl.loop(1, n_sp)
    def _(d):
        end_copy((s + d) % n_sp, s).wait_send()

    @pl.loop(1, n_sp)
    def _(k):
        for c in range(3):

            @pl.when(jnp.logical_and(has_right, s >= k - 1))
            def _():
                z_copy(0, c, k, (s + n_sp + 1 - k) % n_sp, right).wait_send()

            @pl.when(jnp.logical_and(has_left, s + k - 1 < n_sp))
            def _():
                z_copy(1, c, k, (s + k - 1) % n_sp, left).wait_send()

            @pl.when(s >= k)
            def _():
                y_copy(0, c, k, (s + n_sp - k) % n_sp, g).wait_send()

            @pl.when(s + k < n_sp)
            def _():
                y_copy(1, c, k, (s + k) % n_sp, g).wait_send()


def fused(
    residual,
    state_input,
    gate_input,
    decay_real,
    frequency,
    log_step,
    drive_real,
    drive_imag,
    read_real,
    read_imag,
    skip_gain,
    value_weight,
    glu_weight,
    mix_weight,
    norm_gain,
    mlp_gate,
    mlp_up,
    mlp_down,
):
    n_sp, n_tp = lax.axis_size("sp"), lax.axis_size("tp")
    groups, states, width = drive_real.shape
    flat, chans = groups * states, groups * width
    rows = state_input.shape[0]
    own, depth = residual.shape
    ff, d_loc = mlp_down.shape
    cols = value_weight.shape[1]
    _, _, in_real, in_imag = discretize(decay_real, frequency, log_step, drive_real, drive_imag)
    times = max(1, 128 // states)

    def tiled(x):
        return jnp.concatenate([x.reshape(chans, states)] * times, axis=1)

    step = jnp.exp(log_step)[:, None]
    counts = (lax.iota(jnp.int32, ROWS8) + 1).astype(F32)[:, None]
    pow_real, pow_imag = powers(
        (decay_real * step).reshape(1, flat), (frequency * step).reshape(1, flat), counts
    )
    vmem = pl.BlockSpec(memory_space=pltpu.VMEM)
    hbm = pl.BlockSpec(memory_space=pl.ANY)
    dma = pltpu.SemaphoreType.DMA
    return pl.pallas_call(
        functools.partial(layer_kernel, n_sp, width, states),
        out_shape=jax.ShapeDtypeStruct((own, depth), BF),
        in_specs=[vmem] * 10 + [hbm] * 3 + [vmem] + [hbm] * 3,
        out_specs=vmem,
        scratch_shapes=[
            pltpu.VMEM(value_weight.shape, BF),
            pltpu.VMEM(glu_weight.shape, BF),
            pltpu.VMEM(mix_weight.shape, BF),
            pltpu.VMEM((n_sp * mlp_gate.shape[0], ff), BF),
            pltpu.VMEM((n_sp * mlp_gate.shape[0], ff), BF),
            pltpu.VMEM((n_sp, ff, d_loc), BF),
            pltpu.VMEM((8, chans, flat), BF),
            pltpu.VMEM((rows, flat), F32),
            pltpu.VMEM((rows, flat), F32),
            pltpu.VMEM((6, ROWS8, flat), F32),
            pltpu.VMEM((n_sp, ROWS8, flat), F32),
            pltpu.VMEM((n_tp, rows, chans), BF),
            pltpu.VMEM((1, n_tp, own, depth), BF),
            pltpu.VMEM((1, 2, own, depth), BF),
            pltpu.VMEM((1, own, depth), BF),
            pltpu.VMEM((1, own, depth), BF),
            pltpu.VMEM((own, depth), F32),
            pltpu.VMEM((n_tp, own, depth), BF),
            pltpu.VMEM((n_tp, own, ff), BF),
            pltpu.VMEM((n_sp, n_tp, own, d_loc), BF),
            pltpu.VMEM((n_sp, 2, own, d_loc), BF),
            pltpu.VMEM((n_sp, own, d_loc), BF),
            pltpu.VMEM((n_sp, own, d_loc), BF),
            dma((6,)),
            dma((n_sp,)),
            dma((n_sp,)),
            dma((2, 3, n_sp)),
            dma((2, 3, n_sp)),
            dma((2, 3, n_sp)),
            dma((2, 3, n_sp)),
            dma((2, 3)),
            dma((2, 3)),
            dma((1, 3)),
            dma((1, 3)),
            dma((n_sp, 3)),
            dma((n_sp, 3)),
        ],
        compiler_params=pltpu.CompilerParams(
            collective_id=0, has_side_effects=True, vmem_limit_bytes=60 * 1024 * 1024
        ),
    )(
        residual,
        state_input,
        gate_input,
        pow_real,
        pow_imag,
        tiled(in_real.transpose(0, 2, 1)),
        tiled(in_imag.transpose(0, 2, 1)),
        tiled(read_real),
        tiled(read_imag),
        skip_gain[None, :],
        value_weight,
        glu_weight,
        mix_weight,
        norm_gain[None, :],
        mlp_gate,
        mlp_up,
        mlp_down,
    )


def quick_kernel(
    n_sp,
    width,
    states,
    residual_h,
    u_h,
    gate_in_h,
    decay_h,
    freq_h,
    step_h,
    drive_re_h,
    drive_im_h,
    read_re_h,
    read_im_h,
    skip_h,
    value_h,
    glu_h,
    mix_h,
    gain_h,
    gate_h,
    up_h,
    down_h,
    out,
    residual,
    u,
    gate_in,
    decay,
    freq,
    log_step,
    drive_re,
    drive_im,
    read_re,
    read_im,
    skip,
    value_w,
    glu_w,
    mix_w,
    gain,
    w_gate,
    w_up,
    w_down,
    wide,
    pow_real,
    pow_imag,
    ratio,
    st_real,
    st_imag,
    masked,
    ends,
    acts,
    part,
    rx_pair,
    relay,
    rx_far,
    inner,
    normed,
    hidden,
    c_part,
    c_in,
    c_relay,
    load_sem,
    end_send,
    end_recv,
    z_send,
    z_recv,
    y_send,
    y_recv,
    y_late,
    z_more,
    ag_send,
    ag_recv,
    rs_send,
    rs_recv,
    c_send,
    c_recv,
):
    g, s, t = lax.axis_index("grp"), lax.axis_index("sp"), lax.axis_index("tp")
    low, high_bit = t % 2, t // 2
    p = t + 1 - 2 * low
    q = t + 2 - 4 * high_bit
    far = 3 - t
    other = 1 - g
    rows, chans = u.shape
    groups, flat = decay.shape[0], st_real.shape[1]
    own, depth = residual.shape
    k_loc, ff = gate_h.shape
    d_loc = down_h.shape[1]
    n_tp = acts.shape[0]
    k_half, f_half = k_loc // 2, ff // 2
    k_piece, d_half = k_half // PIECES, d_loc // HALVES
    f_piece = f_half * HALVES // PIECES

    barrier = pltpu.get_barrier_semaphore()
    pl.semaphore_signal(barrier, inc=1, device_id={"tp": p})
    pl.semaphore_signal(barrier, inc=1, device_id={"tp": q})
    pl.semaphore_signal(barrier, inc=1, device_id={"grp": other})

    @pl.loop(1, n_sp)
    def _(d):
        pl.semaphore_signal(barrier, inc=1, device_id={"sp": (s + d) % n_sp})

    place = pl.ds(pl.multiple_of(s * k_loc, k_loc), k_loc)
    pairs_of = (
        (gate_h, w_gate.at[place, :]),
        (decay_h, decay),
        (freq_h, freq),
        (step_h, log_step),
        (drive_re_h, drive_re),
        (drive_im_h, drive_im),
        (u_h, u),
        (read_re_h, read_re),
        (read_im_h, read_im),
        (skip_h, skip),
        (up_h, w_up.at[place, :]),
        (down_h, w_down.at[s]),
        (value_h, value_w),
        (glu_h, glu_w),
        (gate_in_h, gate_in),
        (mix_h, mix_w),
        (residual_h, residual),
        (gain_h, gain),
    )
    loads = [
        pltpu.make_async_copy(a, b, load_sem.at[i]) for i, (a, b) in enumerate(pairs_of)
    ]
    for load in loads:
        load.start()
    pl.semaphore_wait(barrier, 3 + n_sp - 1)

    bufs = (w_gate, w_up, w_down)
    behind = (s, n_sp - 1 - s)
    n_early, n_late = 2 * PIECES, PIECES

    def mine(c, i, origin, half):
        if c < 2:
            row = pl.multiple_of(origin * k_loc + half * k_half + i * k_piece, k_piece)
            return bufs[c].at[pl.ds(row, k_piece), :]
        per = PIECES // HALVES
        row = pl.multiple_of(half * f_half + (i % per) * f_piece, f_piece)
        return bufs[c].at[origin, pl.ds(row, f_piece), pl.ds((i // per) * d_half, d_half)]

    def z_copy(side, c, i, origin):
        piece = mine(c, i, origin, g)
        return pltpu.make_async_remote_copy(
            src_ref=piece,
            dst_ref=piece,
            send_sem=z_send.at[side, c],
            recv_sem=z_recv.at[c, i, origin],
            device_id={"sp": ahead(side)},
        )

    def y_copy(c, i, origin, half):
        piece = mine(c, i, origin, half)
        return pltpu.make_async_remote_copy(
            src_ref=piece,
            dst_ref=piece,
            send_sem=y_send.at[c // 2],
            recv_sem=y_recv.at[0] if c < 2 else y_late.at[origin, i // (PIECES // HALVES)],
            device_id={"grp": other},
        )

    def more_copy(side, c, i):
        piece = mine(c, i, s, other)
        return pltpu.make_async_remote_copy(
            src_ref=piece,
            dst_ref=piece,
            send_sem=z_send.at[side, c],
            recv_sem=z_more.at[0 if c < 2 else 1 + i // (PIECES // HALVES)],
            device_id={"sp": ahead(side)},
        )

    def ahead(side):
        return (s + 1) % n_sp if side == 0 else (s + n_sp - 1) % n_sp

    def source(side, k):
        return (s + n_sp - k) % n_sp if side == 0 else (s + k) % n_sp

    def own_sends(side, c, pieces):
        for i in pieces:
            z_copy(side, c, i, s).start()

    def end_sends(side):
        for c in range(3):
            if c == 2:
                own_sends(side, 2, range(PIECES))
            for i in range(PIECES):
                more_copy(side, c, i).start()

    def own_early(c, pieces):
        for side in range(2):
            pl.when(behind[side] < n_sp - 1)(functools.partial(own_sends, side, c, pieces))

    def shared(side, k):
        return behind[side] > 1 if k == 1 else behind[side] >= k

    def onward(side, k, c, i, last):
        @pl.when(behind[side] < n_sp - 1)
        def _():
            z_copy(side, c, i, source(side, k)).start()

        if last:

            @pl.when(jnp.logical_and(behind[side] == k, k < n_sp - 1))
            def _():
                own_sends(side, 2, range(PIECES))

    def pass_on(side, k, c, i, last, hold):
        origin = source(side, k)
        z_copy(side, c, i, origin).wait_recv()
        if not hold:
            onward(side, k, c, i, last)

        @pl.when(shared(side, k))
        def _():
            y_copy(c, i, origin, g).start()

    def advance(*slots, hold=False):
        for n in slots:
            for side in range(2):
                if n < n_early * (n_sp - 1):
                    k, c, i = n // n_early + 1, n % n_early // PIECES, n % PIECES
                    last = n % n_early == n_early - 1
                    work = functools.partial(pass_on, side, k, c, i, last, hold)
                    pl.when(behind[side] >= k)(work)
                for b in range(1, n_sp):
                    m = n - n_early * max(b, 2)
                    if 0 <= m < n_late * b:
                        work = functools.partial(
                            pass_on, side, m // n_late + 1, 2, m % n_late, False, False
                        )
                        pl.when(behind[side] == b)(work)

    loads[0].wait()
    own_early(0, range(PIECES))

    for load in loads[1:4]:
        load.wait()
    eye = lax.broadcasted_iota(jnp.int32, (groups, groups), 0) == lax.broadcasted_iota(
        jnp.int32, (groups, groups), 1
    )
    step = jnp.exp(jnp.sum(jnp.where(eye, log_step[...], 0.0), axis=1, keepdims=True))
    rate, turn = decay[...], freq[...]
    magnitude = jnp.exp(rate * step)
    bar_re = magnitude * jnp.cos(turn * step)
    bar_im = magnitude * jnp.sin(turn * step)
    modulus = rate * rate + turn * turn
    ratio_re = ((bar_re - 1.0) * rate + bar_im * turn) / modulus
    ratio_im = (bar_im * rate - (bar_re - 1.0) * turn) / modulus
    tiles = max(1, 128 // states)
    lanes = tiles * states
    part_of = lax.broadcasted_iota(jnp.int32, (1, lanes), 1) // states

    def spread(target, row, value):
        doubled = jnp.concatenate([value] * tiles, axis=1)
        for tile in range(groups // tiles):
            line = doubled[tile * tiles : tile * tiles + 1, :]
            for j in range(1, tiles):
                line = jnp.where(part_of == j, doubled[tile * tiles + j : tile * tiles + j + 1, :], line)
            target[row : row + 1, tile * lanes : (tile + 1) * lanes] = line

    spread(ratio, 0, ratio_re)
    spread(ratio, 1, ratio_im)
    up_re, up_im = bar_re, bar_im
    for n in range(ROWS8):
        spread(pow_real, n, up_re)
        spread(pow_imag, n, up_im)
        up_re, up_im = up_re * bar_re - up_im * bar_im, up_re * bar_im + up_im * bar_re

    for load in loads[4:9]:
        load.wait()
    row_group = lax.broadcasted_iota(jnp.int32, (chans, lanes), 0) // width
    lane = lax.broadcasted_iota(jnp.int32, (chans, lanes), 1)
    for i, ref in enumerate((drive_re, drive_im, read_re, read_im)):
        value = jnp.concatenate([ref[...]] * tiles, axis=1)
        for tile in range(flat // lanes):
            kept = jnp.where(row_group == (lane + tile * lanes) // states, value, 0.0)
            at = slice(tile * lanes, (tile + 1) * lanes)
            for j, piece in enumerate(split(kept)):
                wide[2 * i + j, :, at] = piece

    @pl.loop(0, rows // own)
    def _(b):
        at = pl.ds(pl.multiple_of(b * own, own), own)
        x = u[at, :]
        push_re = mm(x, wide[0]) + mm(x, wide[1])
        push_im = mm(x, wide[2]) + mm(x, wide[3])
        st_real[at, :] = ratio[0:1, :] * push_re - ratio[1:2, :] * push_im
        st_imag[at, :] = ratio[0:1, :] * push_im + ratio[1:2, :] * push_re

    sub = lax.broadcasted_iota(jnp.int32, (ROWS8, flat), 0)
    for i, reach in enumerate((1, 2, 4)):
        masked[2 * i] = jnp.where(sub >= reach, pow_real[reach - 1 : reach, :], 0.0)
        masked[2 * i + 1] = jnp.where(sub >= reach, pow_imag[reach - 1 : reach, :], 0.0)

    def scan_step(b, carry):
        c_re, c_im = carry
        at = pl.ds(pl.multiple_of(b * ROWS8, ROWS8), ROWS8)
        x_re, x_im = st_real[at, :], st_imag[at, :]
        for i, reach in enumerate((1, 2, 4)):
            m_re, m_im = pltpu.roll(x_re, reach, 0), pltpu.roll(x_im, reach, 0)
            a_re, a_im = masked[2 * i], masked[2 * i + 1]
            x_re, x_im = x_re + a_re * m_re - a_im * m_im, x_im + a_re * m_im + a_im * m_re
        p_re, p_im = pow_real[...], pow_imag[...]
        x_re, x_im = x_re + p_re * c_re - p_im * c_im, x_im + p_re * c_im + p_im * c_re
        st_real[at, :] = x_re
        st_imag[at, :] = x_im
        return x_re[ROWS8 - 1 :, :], x_im[ROWS8 - 1 :, :]

    zero = jnp.zeros((1, flat), F32)
    blocks = rows // ROWS8
    tip = lax.fori_loop(0, blocks // 2, scan_step, (zero, zero))
    advance(0, hold=True)
    end_re, end_im = lax.fori_loop(blocks // 2, blocks, scan_step, tip)
    ends[s, :, :flat] = end_re
    ends[s, :, flat:] = end_im

    def end_copy(target, origin):
        return pltpu.make_async_remote_copy(
            src_ref=ends.at[origin],
            dst_ref=ends.at[origin],
            send_sem=end_send.at[target],
            recv_sem=end_recv.at[origin],
            device_id={"sp": target},
        )

    @pl.loop(s + 1, n_sp)
    def _(later):
        end_copy(later, s).start()

    for load in loads[10:12]:
        load.wait()
    own_early(1, range(PIECES))
    for side in range(2):
        pl.when(behind[side] == 0)(functools.partial(end_sends, side))
        pl.when(behind[side] >= 1)(functools.partial(onward, side, 1, 0, 0, False))
    advance(1)
    last_re, last_im = pow_real[ROWS8 - 1 :, :], pow_imag[ROWS8 - 1 :, :]
    long_re, long_im = last_re, last_im
    reach = ROWS8
    while reach < rows:
        long_re, long_im = long_re * long_re - long_im * long_im, 2.0 * long_re * long_im
        reach *= 2

    advance(2, 3, 4)

    @pl.loop(0, s)
    def _(earlier):
        end_copy((s + 1) % n_sp, earlier).wait_recv()

    def carry_step(j, carry):
        c_re, c_im = carry
        e_re, e_im = ends[j, :, :flat], ends[j, :, flat:]
        n_re = long_re * c_re - long_im * c_im + e_re
        n_im = long_re * c_im + long_im * c_re + e_im
        return jnp.where(j < s, n_re, c_re), jnp.where(j < s, n_im, c_im)

    carry = lax.fori_loop(0, n_sp - 1, carry_step, (zero, zero))

    def lift(b, carry):
        c_re, c_im = carry
        at = pl.ds(pl.multiple_of(b * ROWS8, ROWS8), ROWS8)
        p_re, p_im = pow_real[...], pow_imag[...]
        st_real[at, :] = st_real[at, :] + p_re * c_re - p_im * c_im
        st_imag[at, :] = st_imag[at, :] + p_re * c_im + p_im * c_re
        return last_re * c_re - last_im * c_im, last_re * c_im + last_im * c_re

    carry = lax.fori_loop(0, blocks // 2, lift, carry)
    advance(5)
    lax.fori_loop(blocks // 2, blocks, lift, carry)
    loads[9].wait()

    def read_block(b):
        at = pl.ds(pl.multiple_of(b * own, own), own)
        high, small = split(st_real[at, :])
        y = mm_t(high, wide[4]) + mm_t(small, wide[4]) + mm_t(high, wide[5])
        high, small = split(st_imag[at, :])
        y = y - (mm_t(high, wide[6]) + mm_t(small, wide[6]) + mm_t(high, wide[7]))
        y = y + skip[...] * u[at, :].astype(F32)
        acts[t, at, :] = jax.nn.gelu(y).astype(BF)

    half_rows = rows // own // 2
    pl.loop(0, half_rows)(read_block)
    advance(6)
    pl.loop(half_rows, rows // own)(read_block)
    advance(7)

    def gather_tp(buf, lane_no, between, later):
        def copy(slot, kind, target):
            return pltpu.make_async_remote_copy(
                src_ref=buf.at[slot],
                dst_ref=buf.at[slot],
                send_sem=ag_send.at[lane_no, kind],
                recv_sem=ag_recv.at[lane_no, kind],
                device_id={"tp": target},
            )

        sent = [copy(t, 0, q), copy(t, 1, p)]
        for item in sent:
            item.start()
        between()
        copy(q, 0, q).wait_recv()
        relayed = copy(q, 2, p)
        relayed.start()
        later()
        copy(p, 1, p).wait_recv()
        copy(far, 2, p).wait_recv()
        return sent + [relayed]

    def rs_pair(index):
        return pltpu.make_async_remote_copy(
            src_ref=part.at[(far, p)[index]],
            dst_ref=rx_pair.at[index],
            send_sem=rs_send.at[index],
            recv_sem=rs_recv.at[index],
            device_id={"tp": p},
        )

    across = pltpu.make_async_remote_copy(
        src_ref=relay,
        dst_ref=rx_far,
        send_sem=rs_send.at[2],
        recv_sem=rs_recv.at[2],
        device_id={"tp": q},
    )

    pending = gather_tp(acts, 0, lambda: advance(8, 9), lambda: advance(10))
    for load in loads[12:]:
        load.wait()

    def mix_block(r):
        at = pl.ds(pl.multiple_of(r * own, own), own)
        value = jnp.zeros((own, value_w.shape[1]), F32)
        gated = value
        for j in range(n_tp):
            a = acts[j, at, :]
            value = value + mm(a, value_w[j * chans : (j + 1) * chans, :])
            gated = gated + mm(a, glu_w[j * chans : (j + 1) * chans, :])
        mixed = jax.nn.sigmoid(gate_in[at, :].astype(F32)) * value * jax.nn.sigmoid(gated)
        part[r] = mm(mixed.astype(BF), mix_w[...]).astype(BF)

    mix_block(far)
    rs_pair(0).start()
    advance(11)
    mix_block(q)
    rs_pair(0).wait_recv()
    relay[...] = (part[q].astype(F32) + rx_pair[0].astype(F32)).astype(BF)
    across.start()
    advance(12)
    mix_block(p)
    rs_pair(1).start()
    mix_block(t)
    advance(13, 14, 15, 16, 17)
    rs_pair(1).wait_recv()
    across.wait_recv()
    pending += [rs_pair(0), rs_pair(1), across]
    near = part[t].astype(F32) + rx_pair[1].astype(F32)
    x = residual[...].astype(F32) + (near + rx_far[...].astype(F32))
    inner[...] = x
    scale = lax.rsqrt(jnp.mean(x * x, axis=-1, keepdims=True) + EPSILON)
    normed[t] = (x * scale * gain[...]).astype(BF)

    pending += gather_tp(normed, 1, lambda: advance(18, 19, 20, 21, 22, 23), lambda: None)

    advance(24)

    def await_bytes(sem, ref):
        pltpu.make_async_copy(ref, ref, sem).wait()

    advance(25)
    near_end = jnp.logical_or(behind[0] == 1, behind[1] == 1)

    @pl.when(near_end)
    def _():
        await_bytes(z_more.at[0], w_gate.at[:k_loc, :])
        await_bytes(y_recv.at[0], w_gate.at[: (n_sp - 2) * k_loc, :])

    @pl.when(jnp.logical_not(near_end))
    def _():
        await_bytes(y_recv.at[0], w_gate.at[: (n_sp - 1) * k_loc, :])

    advance(26)

    def hidden_block(r):
        x = normed[r]
        hidden[r] = (jax.nn.silu(mm(x, w_gate[...])) * mm(x, w_up[...])).astype(BF)

    pl.loop(0, n_tp // 2)(hidden_block)
    advance(27)
    pl.loop(n_tp // 2, n_tp)(hidden_block)
    advance(28)

    def col_pair(o, h, index):
        return pltpu.make_async_remote_copy(
            src_ref=c_part.at[o, h, (far, p)[index]],
            dst_ref=c_in.at[o, h, index],
            send_sem=c_send.at[0],
            recv_sem=c_recv.at[o, h if index == 0 else HALVES],
            device_id={"tp": p},
        )

    def col_far(o, h):
        return pltpu.make_async_remote_copy(
            src_ref=c_relay.at[o, h],
            dst_ref=c_in.at[o, h, 2],
            send_sem=c_send.at[0],
            recv_sem=c_recv.at[o, HALVES],
            device_id={"tp": q},
        )

    def column(o, h):
        weight = w_down.at[o, :, h * d_half : (h + 1) * d_half]
        for r, index in ((far, 0), (p, 1), (q, None), (t, None)):
            c_part[o, h, r] = mm(hidden[r], weight[...]).astype(BF)
            if index is not None:
                col_pair(o, h, index).start()
        col_pair(o, h, 0).wait_recv()
        both = c_part[o, h, q].astype(F32) + c_in[o, h, 0].astype(F32)
        c_relay[o, h] = both.astype(BF)
        col_far(o, h).start()

    def settle(o):
        await_bytes(c_recv.at[o, HALVES], c_in.at[o, :, 1:3])
        for h in range(HALVES):
            near = c_part[o, h, t].astype(F32) + c_in[o, h, 1].astype(F32)
            at = pl.ds(pl.multiple_of(o * d_loc + h * d_half, d_half), d_half)
            out[:, at] = (inner[:, at] + 0.5 * (near + c_in[o, h, 2].astype(F32))).astype(BF)

    def both_sides(k, work):
        for side in range(2):
            pl.when(behind[side] >= k)(functools.partial(work, side, k))

    def next_column(h, side, k):
        origin = source(side, k)
        row = pl.multiple_of(other * f_half, f_half)
        came = w_down.at[origin, pl.ds(row, f_half), h * d_half : (h + 1) * d_half]

        @pl.when(shared(side, k))
        def _():
            await_bytes(y_late.at[origin, h], came)

        if k == 1:

            @pl.when(behind[side] == 1)
            def _():
                await_bytes(z_more.at[1 + h], came)

        column(origin, h)

    def next_settle(side, k):
        settle(source(side, k))

    column(s, 0)
    column(s, 1)
    advance(29)
    both_sides(1, functools.partial(next_column, 0))
    advance(30)
    both_sides(1, functools.partial(next_column, 1))
    advance(31)
    settle(s)
    advance(32)
    both_sides(2, functools.partial(next_column, 0))
    advance(33, 34)
    both_sides(2, functools.partial(next_column, 1))
    advance(35)
    both_sides(1, next_settle)
    both_sides(3, functools.partial(next_column, 0))
    both_sides(2, next_settle)
    for item in pending:
        item.wait_send()

    @pl.loop(s + 1, n_sp)
    def _(later):
        end_copy(later, s).wait_send()

    def sent(side, b):
        count = max(2, b + 1)
        for c in range(2):
            await_bytes(z_send.at[side, c], w_gate.at[: count * k_half, :])
        await_bytes(z_send.at[side, 2], w_down.at[:count, :f_half, :])

    for side in range(2):
        for b in range(n_sp - 1):
            pl.when(behind[side] == b)(functools.partial(sent, side, b))

    def exchanged(count):
        await_bytes(y_send.at[0], w_gate.at[: count * k_loc, :])
        await_bytes(y_send.at[1], w_down.at[:count, :f_half, :])

    pl.when(near_end)(functools.partial(exchanged, n_sp - 2))
    pl.when(jnp.logical_not(near_end))(functools.partial(exchanged, n_sp - 1))
    both_sides(3, functools.partial(next_column, 1))
    both_sides(3, next_settle)
    await_bytes(c_send.at[0], c_in)


def quick(
    residual,
    state_input,
    gate_input,
    decay_real,
    frequency,
    log_step,
    drive_real,
    drive_imag,
    read_real,
    read_imag,
    skip_gain,
    value_weight,
    glu_weight,
    mix_weight,
    norm_gain,
    mlp_gate,
    mlp_up,
    mlp_down,
):
    n_sp, n_tp = lax.axis_size("sp"), lax.axis_size("tp")
    groups, states, width = drive_real.shape
    flat, chans = groups * states, groups * width
    rows = state_input.shape[0]
    own, depth = residual.shape
    k_loc, ff = mlp_gate.shape
    d_loc = mlp_down.shape[1]
    d_half = d_loc // HALVES
    hbm = pl.BlockSpec(memory_space=pltpu.HBM)
    dma = pltpu.SemaphoreType.DMA
    operands = (
        residual,
        state_input,
        gate_input,
        decay_real,
        frequency,
        log_step[None, :],
        drive_real.transpose(0, 2, 1).reshape(chans, states),
        drive_imag.transpose(0, 2, 1).reshape(chans, states),
        read_real.reshape(chans, states),
        read_imag.reshape(chans, states),
        skip_gain[None, :],
        value_weight,
        glu_weight,
        mix_weight,
        norm_gain[None, :],
        mlp_gate,
        mlp_up,
        mlp_down,
    )
    return pl.pallas_call(
        functools.partial(quick_kernel, n_sp, width, states),
        out_shape=pltpu.VMEM((own, depth), BF),
        in_specs=[hbm] * len(operands),
        out_specs=pl.BlockSpec(memory_space=pltpu.VMEM),
        scratch_shapes=[pltpu.VMEM(x.shape, x.dtype) for x in operands[:15]]
        + [
            pltpu.VMEM((n_sp * k_loc, ff), BF),
            pltpu.VMEM((n_sp * k_loc, ff), BF),
            pltpu.VMEM((n_sp, ff, d_loc), BF),
            pltpu.VMEM((8, chans, flat), BF),
            pltpu.VMEM((ROWS8, flat), F32),
            pltpu.VMEM((ROWS8, flat), F32),
            pltpu.VMEM((2, flat), F32),
            pltpu.VMEM((rows, flat), F32),
            pltpu.VMEM((rows, flat), F32),
            pltpu.VMEM((6, ROWS8, flat), F32),
            pltpu.VMEM((n_sp, 1, 2 * flat), F32),
            pltpu.VMEM((n_tp, rows, chans), BF),
            pltpu.VMEM((n_tp, own, depth), BF),
            pltpu.VMEM((2, own, depth), BF),
            pltpu.VMEM((own, depth), BF),
            pltpu.VMEM((own, depth), BF),
            pltpu.VMEM((own, depth), F32),
            pltpu.VMEM((n_tp, own, depth), BF),
            pltpu.VMEM((n_tp, own, ff), BF),
            pltpu.VMEM((n_sp, HALVES, n_tp, own, d_half), BF),
            pltpu.VMEM((n_sp, HALVES, 3, own, d_half), BF),
            pltpu.VMEM((n_sp, HALVES, own, d_half), BF),
            dma((len(operands),)),
            dma((n_sp,)),
            dma((n_sp,)),
            dma((2, 3)),
            dma((3, PIECES, n_sp)),
            dma((2,)),
            dma((1,)),
            dma((n_sp, HALVES)),
            dma((1 + HALVES,)),
            dma((2, 3)),
            dma((2, 3)),
            dma((3,)),
            dma((3,)),
            dma((1,)),
            dma((n_sp, HALVES + 1)),
        ],
        compiler_params=pltpu.CompilerParams(
            collective_id=0, has_side_effects=True, vmem_limit_bytes=60 * 1024 * 1024
        ),
    )(*operands)


def solution(mesh):
    placed = (
        P(("grp", "sp", "tp"), None),
        P(("grp", "sp"), "tp"),
        P(("grp", "sp"), "tp"),
        P("tp", None),
        P("tp", None),
        P("tp"),
        P("tp", None, None),
        P("tp", None, None),
        P("tp", None, None),
        P("tp", None, None),
        P("tp"),
        P(None, "tp"),
        P(None, "tp"),
        P("tp", None),
        P(),
        P("sp", "tp"),
        P("sp", "tp"),
        P("tp", "sp"),
    )
    body = shards
    if (mesh.shape["tp"], mesh.shape["grp"]) == (4, 2):
        body = quick if mesh.shape["sp"] == 4 else fused
    return jax.shard_map(
        body, mesh=mesh, in_specs=placed, out_specs=P(("grp", "sp", "tp"), None), check_vma=False
    )
```

```python
import functools
import jax
import jax.numpy as jnp
from jax import lax
from jax.experimental import pallas as pl
from jax.experimental.pallas import tpu as pltpu
from jax.sharding import PartitionSpec as P

BF = jnp.bfloat16
F32 = jnp.float32
ROWS8 = 8
PIECES = 4
HALVES = 2
PER = PIECES // HALVES

HIGH = lax.Precision.HIGHEST
EPSILON = 1e-06


def carried_in(value, axis, join, neutral):
    count, mine = (lax.axis_size(axis), lax.axis_index(axis))
    pieces = jax.tree.map(lambda part: lax.all_gather(part, axis), value)
    subtotal = jax.tree.map(
        lambda part, zero: jnp.full_like(part, 0) + jnp.asarray(zero, part.dtype), value, neutral
    )

    def step(position, subtotal):
        longer = join(subtotal, jax.tree.map(lambda part: part[position], pieces))
        return jax.tree.map(lambda new, old: jnp.where(position < mine, new, old), longer, subtotal)

    return lax.fori_loop(0, count - 1, step, subtotal)


def discretize(decay_real, frequency, log_step, drive_real, drive_imag):
    step = jnp.exp(log_step)[:, None]
    magnitude = jnp.exp(decay_real * step)
    turned = frequency * step
    bar_real = magnitude * jnp.cos(turned)
    bar_imag = magnitude * jnp.sin(turned)
    modulus = decay_real * decay_real + frequency * frequency
    ratio_real = ((bar_real - 1.0) * decay_real + bar_imag * frequency) / modulus
    ratio_imag = (bar_imag * decay_real - (bar_real - 1.0) * frequency) / modulus
    in_real = ratio_real[..., None] * drive_real - ratio_imag[..., None] * drive_imag
    in_imag = ratio_real[..., None] * drive_imag + ratio_imag[..., None] * drive_real
    return (bar_real, bar_imag, in_real, in_imag)


def combine(earlier, later):
    real_one, imag_one, state_real_one, state_imag_one = earlier
    real_two, imag_two, state_real_two, state_imag_two = later
    return (
        real_one * real_two - imag_one * imag_two,
        real_one * imag_two + imag_one * real_two,
        real_two * state_real_one - imag_two * state_imag_one + state_real_two,
        real_two * state_imag_one + imag_two * state_real_one + state_imag_two,
    )


def powers(log_rate, angle_rate, count):
    return (
        jnp.exp(log_rate * count) * jnp.cos(angle_rate * count),
        jnp.exp(log_rate * count) * jnp.sin(angle_rate * count),
    )


def block_states(flat_inputs, decay_real, frequency, log_step, in_real, in_imag):
    rows = flat_inputs.shape[0]
    groups, states, width = in_real.shape
    flat = groups * states
    eye = jnp.eye(groups, dtype=jnp.float32)
    wide_real = jnp.einsum("gph,gk->ghkp", in_real, eye).reshape(groups * width, flat)
    wide_imag = jnp.einsum("gph,gk->ghkp", in_imag, eye).reshape(groups * width, flat)
    state_real = jnp.dot(flat_inputs, wide_real, precision=HIGH)
    state_imag = jnp.dot(flat_inputs, wide_imag, precision=HIGH)
    step = jnp.exp(log_step)[:, None]
    log_rate = (decay_real * step).reshape(1, flat)
    angle_rate = (frequency * step).reshape(1, flat)
    reach = 1
    while reach < rows:
        lift_real, lift_imag = powers(log_rate, angle_rate, float(reach))
        blank = jnp.zeros((reach, flat), jnp.float32)
        moved_real = jnp.concatenate([blank, state_real[: rows - reach]], axis=0)
        moved_imag = jnp.concatenate([blank, state_imag[: rows - reach]], axis=0)
        state_real, state_imag = (
            state_real + lift_real * moved_real - lift_imag * moved_imag,
            state_imag + lift_real * moved_imag + lift_imag * moved_real,
        )
        reach = reach * 2
    counts = (lax.iota(jnp.int32, rows) + 1).astype(jnp.float32)[:, None]
    power_real, power_imag = powers(log_rate, angle_rate, counts)
    return (power_real, power_imag, state_real, state_imag)


def readout(state_real, state_imag, read_real, read_imag, flat_inputs, skip_gain):
    groups, width, states = read_real.shape
    eye = jnp.eye(groups, dtype=jnp.float32)
    wide_real = jnp.einsum("ghp,gk->gpkh", read_real, eye).reshape(groups * states, groups * width)
    wide_imag = jnp.einsum("ghp,gk->gpkh", read_imag, eye).reshape(groups * states, groups * width)
    output = jnp.dot(state_real, wide_real, precision=HIGH) - jnp.dot(
        state_imag, wide_imag, precision=HIGH
    )
    output = output + skip_gain * flat_inputs
    return jax.nn.gelu(output).astype(jnp.bfloat16)


def normalize(inner, norm_gain):
    scale = lax.rsqrt(jnp.mean(inner * inner, axis=-1, keepdims=True) + EPSILON)
    return (inner * scale * norm_gain).astype(jnp.bfloat16)


def shards(
    residual,
    state_input,
    gate_input,
    decay_real,
    frequency,
    log_step,
    drive_real,
    drive_imag,
    read_real,
    read_imag,
    skip_gain,
    value_weight,
    glu_weight,
    mix_weight,
    norm_gain,
    mlp_gate,
    mlp_up,
    mlp_down,
):
    bar_real, bar_imag, in_real, in_imag = discretize(
        decay_real, frequency, log_step, drive_real, drive_imag
    )
    flat_inputs = state_input.astype(jnp.float32)
    power_real, power_imag, local_real, local_imag = block_states(
        flat_inputs, decay_real, frequency, log_step, in_real, in_imag
    )
    ends = (power_real[-1], power_imag[-1], local_real[-1], local_imag[-1])
    ones = jnp.ones_like(ends[0])
    zeros = jnp.zeros_like(ends[0])
    incoming = carried_in(
        (ends[0], ends[1], ends[2], ends[3]), "sp", combine, (ones, zeros, zeros, zeros)
    )
    carry_real = incoming[2]
    carry_imag = incoming[3]
    state_real = local_real + power_real * carry_real - power_imag * carry_imag
    state_imag = local_imag + power_real * carry_imag + power_imag * carry_real
    acts = readout(state_real, state_imag, read_real, read_imag, flat_inputs, skip_gain)
    piece = lax.all_gather(acts, "tp", axis=1, tiled=True)
    value = jnp.dot(piece, value_weight, preferred_element_type=jnp.float32)
    gated = jnp.dot(piece, glu_weight, preferred_element_type=jnp.float32)
    mixed = (jax.nn.sigmoid(gate_input.astype(jnp.float32)) * value * jax.nn.sigmoid(gated)).astype(
        jnp.bfloat16
    )
    branch = lax.psum_scatter(
        jnp.dot(mixed, mix_weight, preferred_element_type=jnp.float32).astype(jnp.bfloat16),
        "tp",
        scatter_dimension=0,
        tiled=True,
    ).astype(jnp.float32)
    inner = residual.astype(jnp.float32) + branch
    normed = lax.all_gather(normalize(inner, norm_gain), "tp", axis=0, tiled=True)
    hidden_gate = jnp.dot(
        normed,
        lax.all_gather(mlp_gate, "sp", axis=0, tiled=True),
        preferred_element_type=jnp.float32,
    )
    hidden_up = jnp.dot(
        normed, lax.all_gather(mlp_up, "sp", axis=0, tiled=True), preferred_element_type=jnp.float32
    )
    hidden = (jax.nn.silu(hidden_gate) * hidden_up).astype(jnp.bfloat16)
    down = jnp.dot(
        hidden,
        lax.all_gather(mlp_down, "sp", axis=1, tiled=True),
        preferred_element_type=jnp.float32,
    )
    down_own = lax.psum_scatter(
        down.astype(jnp.bfloat16), "tp", scatter_dimension=0, tiled=True
    ).astype(jnp.float32)
    return (inner + 0.5 * down_own).astype(jnp.bfloat16)


def mm(a, b):
    return jnp.dot(a, b, preferred_element_type=F32)


def mm_t(a, b):
    return lax.dot_general(a, b, (((1,), (1,)), ((), ())), preferred_element_type=F32)


def split(x):
    high = x.astype(BF)
    return high, (x - high.astype(F32)).astype(BF)


def layer_kernel(
    n_sp,
    width,
    states,
    residual,
    u,
    gate_in,
    pow_real,
    pow_imag,
    in_real,
    in_imag,
    rd_real,
    rd_imag,
    skip,
    value_h,
    glu_h,
    mix_h,
    gain,
    gate_h,
    up_h,
    down_h,
    out,
    value_w,
    glu_w,
    mix_w,
    w_gate,
    w_up,
    w_down,
    wide,
    st_real,
    st_imag,
    masked,
    ends,
    acts,
    part,
    rx_pair,
    relay,
    rx_far,
    inner,
    normed,
    hidden,
    c_part,
    c_pair,
    c_relay,
    c_far,
    load_sem,
    end_send,
    end_recv,
    z_send,
    z_recv,
    y_send,
    y_recv,
    ag_send,
    ag_recv,
    rs_send,
    rs_recv,
    c_send,
    c_recv,
):
    g, s, t = lax.axis_index("grp"), lax.axis_index("sp"), lax.axis_index("tp")
    low, high_bit = t % 2, t // 2
    p = t + 1 - 2 * low
    q = t + 2 - 4 * high_bit
    far = 3 - t
    other = 1 - g
    rows, chans = u.shape
    flat = st_real.shape[1]
    own, depth = residual.shape
    k_loc = gate_h.shape[0]
    ff, d_loc = down_h.shape
    k_half, f_half = k_loc // 2, ff // 2

    barrier = pltpu.get_barrier_semaphore()
    pl.semaphore_signal(barrier, inc=1, device_id={"tp": p})
    pl.semaphore_signal(barrier, inc=1, device_id={"tp": q})
    pl.semaphore_signal(barrier, inc=1, device_id={"grp": other})

    @pl.loop(1, n_sp)
    def _(d):
        pl.semaphore_signal(barrier, inc=1, device_id={"sp": (s + d) % n_sp})

    def mine(ref, c, origin, half):
        if c < 2:
            return ref.at[pl.ds(pl.multiple_of(origin * k_loc + half * k_half, k_half), k_half), :]
        return ref.at[origin, pl.ds(pl.multiple_of(half * f_half, f_half), f_half), :]

    bufs = (w_gate, w_up, w_down)
    place = pl.ds(pl.multiple_of(s * k_loc, k_loc), k_loc)
    loads = [
        pltpu.make_async_copy(gate_h, w_gate.at[place, :], load_sem.at[0]),
        pltpu.make_async_copy(up_h, w_up.at[place, :], load_sem.at[1]),
        pltpu.make_async_copy(down_h, w_down.at[s], load_sem.at[2]),
        pltpu.make_async_copy(value_h, value_w, load_sem.at[3]),
        pltpu.make_async_copy(glu_h, glu_w, load_sem.at[4]),
        pltpu.make_async_copy(mix_h, mix_w, load_sem.at[5]),
    ]
    for load in loads:
        load.start()
    pl.semaphore_wait(barrier, 3 + n_sp - 1)

    def z_copy(side, c, k, origin, target):
        piece = mine(bufs[c], c, origin, g)
        return pltpu.make_async_remote_copy(
            src_ref=piece,
            dst_ref=piece,
            send_sem=z_send.at[side, c, k],
            recv_sem=z_recv.at[side, c, k],
            device_id={"sp": target},
        )

    def y_copy(side, c, k, origin, half):
        piece = mine(bufs[c], c, origin, half)
        return pltpu.make_async_remote_copy(
            src_ref=piece,
            dst_ref=piece,
            send_sem=y_send.at[side, c, k],
            recv_sem=y_recv.at[side, c, k],
            device_id={"grp": other},
        )

    right, left = (s + 1) % n_sp, (s + n_sp - 1) % n_sp
    has_right, has_left = s < n_sp - 1, s > 0

    for c in range(3):
        loads[c].wait()

        @pl.when(has_right)
        def _():
            z_copy(0, c, 1, s, right).start()

        @pl.when(has_left)
        def _():
            z_copy(1, c, 1, s, left).start()

    def onward(c, k):
        @pl.when(s >= k)
        def _():
            origin = (s + n_sp - k) % n_sp
            z_copy(0, c, k, origin, right).wait_recv()

            @pl.when(has_right)
            def _():
                z_copy(0, c, k + 1, origin, right).start()

            y_copy(0, c, k, origin, g).start()

        @pl.when(s + k < n_sp)
        def _():
            origin = (s + k) % n_sp
            z_copy(1, c, k, origin, left).wait_recv()

            @pl.when(has_left)
            def _():
                z_copy(1, c, k + 1, origin, left).start()

            y_copy(1, c, k, origin, g).start()

    def arrived(c):
        @pl.loop(1, n_sp)
        def _(k):
            @pl.when(s >= k)
            def _():
                y_copy(0, c, k, (s + n_sp - k) % n_sp, other).wait_recv()

            @pl.when(s + k < n_sp)
            def _():
                y_copy(1, c, k, (s + k) % n_sp, other).wait_recv()

    lanes = in_real.shape[1]
    row_group = lax.broadcasted_iota(jnp.int32, (chans, lanes), 0) // width
    lane = lax.broadcasted_iota(jnp.int32, (chans, lanes), 1)
    for i, ref in enumerate((in_real, in_imag, rd_real, rd_imag)):
        value = ref[...]
        for tile in range(flat // lanes):
            kept = jnp.where(row_group == (lane + tile * lanes) // states, value, 0.0)
            big, small = split(kept)
            at = slice(tile * lanes, (tile + 1) * lanes)
            wide[2 * i, :, at] = big
            wide[2 * i + 1, :, at] = small

    @pl.loop(0, rows // own)
    def _(b):
        at = pl.ds(pl.multiple_of(b * own, own), own)
        x = u[at, :]
        st_real[at, :] = mm(x, wide[0]) + mm(x, wide[1])
        st_imag[at, :] = mm(x, wide[2]) + mm(x, wide[3])

    sub = lax.broadcasted_iota(jnp.int32, (ROWS8, flat), 0)
    for i, reach in enumerate((1, 2, 4)):
        masked[2 * i] = jnp.where(sub >= reach, pow_real[reach - 1 : reach, :], 0.0)
        masked[2 * i + 1] = jnp.where(sub >= reach, pow_imag[reach - 1 : reach, :], 0.0)

    def scan_step(b, carry):
        c_re, c_im = carry
        at = pl.ds(pl.multiple_of(b * ROWS8, ROWS8), ROWS8)
        x_re, x_im = st_real[at, :], st_imag[at, :]
        for i, reach in enumerate((1, 2, 4)):
            m_re, m_im = pltpu.roll(x_re, reach, 0), pltpu.roll(x_im, reach, 0)
            a_re, a_im = masked[2 * i], masked[2 * i + 1]
            x_re, x_im = x_re + a_re * m_re - a_im * m_im, x_im + a_re * m_im + a_im * m_re
        p_re, p_im = pow_real[...], pow_imag[...]
        x_re, x_im = x_re + p_re * c_re - p_im * c_im, x_im + p_re * c_im + p_im * c_re
        st_real[at, :] = x_re
        st_imag[at, :] = x_im
        return x_re[ROWS8 - 1 :, :], x_im[ROWS8 - 1 :, :]

    zero = jnp.zeros((1, flat), F32)
    end_re, end_im = lax.fori_loop(0, rows // ROWS8, scan_step, (zero, zero))
    ends[s, 0:1, :] = end_re
    ends[s, 1:2, :] = end_im

    def end_copy(target, origin):
        return pltpu.make_async_remote_copy(
            src_ref=ends.at[origin],
            dst_ref=ends.at[origin],
            send_sem=end_send.at[target],
            recv_sem=end_recv.at[origin],
            device_id={"sp": target},
        )

    @pl.loop(1, n_sp)
    def _(d):
        end_copy((s + d) % n_sp, s).start()

    onward(0, 1)
    last_re, last_im = pow_real[ROWS8 - 1 :, :], pow_imag[ROWS8 - 1 :, :]
    long_re, long_im = last_re, last_im
    reach = ROWS8
    while reach < rows:
        long_re, long_im = long_re * long_re - long_im * long_im, 2.0 * long_re * long_im
        reach *= 2

    @pl.loop(1, n_sp)
    def _(d):
        end_copy((s + d) % n_sp, (s + d) % n_sp).wait_recv()

    def carry_step(j, carry):
        c_re, c_im = carry
        e_re, e_im = ends[j, 0:1, :], ends[j, 1:2, :]
        n_re = long_re * c_re - long_im * c_im + e_re
        n_im = long_re * c_im + long_im * c_re + e_im
        return jnp.where(j < s, n_re, c_re), jnp.where(j < s, n_im, c_im)

    carry = lax.fori_loop(0, n_sp - 1, carry_step, (zero, zero))

    def lift(b, carry):
        c_re, c_im = carry
        at = pl.ds(pl.multiple_of(b * ROWS8, ROWS8), ROWS8)
        p_re, p_im = pow_real[...], pow_imag[...]
        st_real[at, :] = st_real[at, :] + p_re * c_re - p_im * c_im
        st_imag[at, :] = st_imag[at, :] + p_re * c_im + p_im * c_re
        return last_re * c_re - last_im * c_im, last_re * c_im + last_im * c_re

    lax.fori_loop(0, rows // ROWS8, lift, carry)

    @pl.loop(0, rows // own)
    def _(b):
        at = pl.ds(pl.multiple_of(b * own, own), own)
        high, small = split(st_real[at, :])
        y = mm_t(high, wide[4]) + mm_t(small, wide[4]) + mm_t(high, wide[5])
        high, small = split(st_imag[at, :])
        y = y - (mm_t(high, wide[6]) + mm_t(small, wide[6]) + mm_t(high, wide[7]))
        y = y + skip[...] * u[at, :].astype(F32)
        acts[t, at, :] = jax.nn.gelu(y).astype(BF)

    def gather_tp(buf, lane_no, between):
        def copy(slot, kind, target):
            return pltpu.make_async_remote_copy(
                src_ref=buf.at[slot],
                dst_ref=buf.at[slot],
                send_sem=ag_send.at[lane_no, kind],
                recv_sem=ag_recv.at[lane_no, kind],
                device_id={"tp": target},
            )

        sent = [copy(t, 0, q), copy(t, 1, p)]
        for item in sent:
            item.start()
        between()
        copy(q, 0, q).wait_recv()
        relayed = copy(q, 2, p)
        relayed.start()
        copy(p, 1, p).wait_recv()
        copy(far, 2, p).wait_recv()
        return sent + [relayed]

    def scatter_tp(lane_no, block, middle, between):
        def pair(index):
            return pltpu.make_async_remote_copy(
                src_ref=part.at[lane_no, (far, p)[index]],
                dst_ref=rx_pair.at[lane_no, index],
                send_sem=rs_send.at[lane_no, index],
                recv_sem=rs_recv.at[lane_no, index],
                device_id={"tp": p},
            )

        across = pltpu.make_async_remote_copy(
            src_ref=relay.at[lane_no],
            dst_ref=rx_far.at[lane_no],
            send_sem=rs_send.at[lane_no, 2],
            recv_sem=rs_recv.at[lane_no, 2],
            device_id={"tp": q},
        )
        pairs = [pair(0), pair(1)]
        block(far)
        pairs[0].start()
        block(p)
        pairs[1].start()
        block(q)
        middle()
        pairs[0].wait_recv()
        relay[lane_no] = (part[lane_no, q].astype(F32) + rx_pair[lane_no, 0].astype(F32)).astype(BF)
        across.start()
        block(t)
        between()
        pairs[1].wait_recv()
        across.wait_recv()
        return pairs + [across]

    def total(lane_no):
        near = part[lane_no, t].astype(F32) + rx_pair[lane_no, 1].astype(F32)
        return near + rx_far[lane_no].astype(F32)

    def first_forward():
        onward(1, 1)

    pending = gather_tp(acts, 0, first_forward)
    for load in loads[3:]:
        load.wait()
    n_tp = acts.shape[0]

    def mix_block(r):
        at = pl.ds(pl.multiple_of(r * own, own), own)
        value = jnp.zeros((own, value_w.shape[1]), F32)
        gated = value
        for j in range(n_tp):
            a = acts[j, at, :]
            value = value + mm(a, value_w[j * chans : (j + 1) * chans, :])
            gated = gated + mm(a, glu_w[j * chans : (j + 1) * chans, :])
        mixed = jax.nn.sigmoid(gate_in[at, :].astype(F32)) * value * jax.nn.sigmoid(gated)
        part[0, r] = mm(mixed.astype(BF), mix_w[...]).astype(BF)

    def third_forward():
        if n_sp > 2:
            onward(0, 2)

    pending += scatter_tp(0, mix_block, lambda: onward(2, 1), third_forward)
    inner[...] = residual[...].astype(F32) + total(0)
    x = inner[...]
    scale = lax.rsqrt(jnp.mean(x * x, axis=-1, keepdims=True) + EPSILON)
    normed[t] = (x * scale * gain[...]).astype(BF)

    def second_forward():
        if n_sp > 2:
            onward(1, 2)

    pending += gather_tp(normed, 1, second_forward)
    if n_sp > 2:
        onward(2, 2)

    @pl.loop(3, n_sp)
    def _(k):
        onward(0, k)
        onward(1, k)
        onward(2, k)

    arrived(0)
    arrived(1)

    @pl.loop(0, n_tp)
    def _(r):
        x = normed[r]
        hidden[r] = (jax.nn.silu(mm(x, w_gate[...])) * mm(x, w_up[...])).astype(BF)

    def col_pair(o, index):
        return pltpu.make_async_remote_copy(
            src_ref=c_part.at[o, (far, p)[index]],
            dst_ref=c_pair.at[o, index],
            send_sem=c_send.at[o, index],
            recv_sem=c_recv.at[o, index],
            device_id={"tp": p},
        )

    def col_far(o):
        return pltpu.make_async_remote_copy(
            src_ref=c_relay.at[o],
            dst_ref=c_far.at[o],
            send_sem=c_send.at[o, 2],
            recv_sem=c_recv.at[o, 2],
            device_id={"tp": q},
        )

    def column(o):
        weight = w_down.at[o]
        c_part[o, far] = mm(hidden[far], weight[...]).astype(BF)
        col_pair(o, 0).start()
        c_part[o, q] = mm(hidden[q], weight[...]).astype(BF)
        c_part[o, p] = mm(hidden[p], weight[...]).astype(BF)
        col_pair(o, 1).start()
        col_pair(o, 0).wait_recv()
        c_relay[o] = (c_part[o, q].astype(F32) + c_pair[o, 0].astype(F32)).astype(BF)
        col_far(o).start()
        c_part[o, t] = mm(hidden[t], weight[...]).astype(BF)

    column(s)

    @pl.loop(1, n_sp)
    def _(k):
        @pl.when(s >= k)
        def _():
            origin = (s + n_sp - k) % n_sp
            y_copy(0, 2, k, origin, other).wait_recv()
            column(origin)

        @pl.when(s + k < n_sp)
        def _():
            origin = (s + k) % n_sp
            y_copy(1, 2, k, origin, other).wait_recv()
            column(origin)

    for o in range(n_sp):
        col_pair(o, 1).wait_recv()
        col_far(o).wait_recv()
        near = c_part[o, t].astype(F32) + c_pair[o, 1].astype(F32)
        at = slice(o * d_loc, (o + 1) * d_loc)
        out[:, at] = (inner[:, at] + 0.5 * (near + c_far[o].astype(F32))).astype(BF)

    @pl.loop(0, n_sp)
    def _(o):
        col_pair(o, 0).wait_send()
        col_pair(o, 1).wait_send()
        col_far(o).wait_send()

    for item in pending:
        item.wait_send()

    @pl.loop(1, n_sp)
    def _(d):
        end_copy((s + d) % n_sp, s).wait_send()

    @pl.loop(1, n_sp)
    def _(k):
        for c in range(3):

            @pl.when(jnp.logical_and(has_right, s >= k - 1))
            def _():
                z_copy(0, c, k, (s + n_sp + 1 - k) % n_sp, right).wait_send()

            @pl.when(jnp.logical_and(has_left, s + k - 1 < n_sp))
            def _():
                z_copy(1, c, k, (s + k - 1) % n_sp, left).wait_send()

            @pl.when(s >= k)
            def _():
                y_copy(0, c, k, (s + n_sp - k) % n_sp, g).wait_send()

            @pl.when(s + k < n_sp)
            def _():
                y_copy(1, c, k, (s + k) % n_sp, g).wait_send()


def fused(
    residual,
    state_input,
    gate_input,
    decay_real,
    frequency,
    log_step,
    drive_real,
    drive_imag,
    read_real,
    read_imag,
    skip_gain,
    value_weight,
    glu_weight,
    mix_weight,
    norm_gain,
    mlp_gate,
    mlp_up,
    mlp_down,
):
    n_sp, n_tp = lax.axis_size("sp"), lax.axis_size("tp")
    groups, states, width = drive_real.shape
    flat, chans = groups * states, groups * width
    rows = state_input.shape[0]
    own, depth = residual.shape
    ff, d_loc = mlp_down.shape
    cols = value_weight.shape[1]
    _, _, in_real, in_imag = discretize(decay_real, frequency, log_step, drive_real, drive_imag)
    times = max(1, 128 // states)

    def tiled(x):
        return jnp.concatenate([x.reshape(chans, states)] * times, axis=1)

    step = jnp.exp(log_step)[:, None]
    counts = (lax.iota(jnp.int32, ROWS8) + 1).astype(F32)[:, None]
    pow_real, pow_imag = powers(
        (decay_real * step).reshape(1, flat), (frequency * step).reshape(1, flat), counts
    )
    vmem = pl.BlockSpec(memory_space=pltpu.VMEM)
    hbm = pl.BlockSpec(memory_space=pl.ANY)
    dma = pltpu.SemaphoreType.DMA
    return pl.pallas_call(
        functools.partial(layer_kernel, n_sp, width, states),
        out_shape=jax.ShapeDtypeStruct((own, depth), BF),
        in_specs=[vmem] * 10 + [hbm] * 3 + [vmem] + [hbm] * 3,
        out_specs=vmem,
        scratch_shapes=[
            pltpu.VMEM(value_weight.shape, BF),
            pltpu.VMEM(glu_weight.shape, BF),
            pltpu.VMEM(mix_weight.shape, BF),
            pltpu.VMEM((n_sp * mlp_gate.shape[0], ff), BF),
            pltpu.VMEM((n_sp * mlp_gate.shape[0], ff), BF),
            pltpu.VMEM((n_sp, ff, d_loc), BF),
            pltpu.VMEM((8, chans, flat), BF),
            pltpu.VMEM((rows, flat), F32),
            pltpu.VMEM((rows, flat), F32),
            pltpu.VMEM((6, ROWS8, flat), F32),
            pltpu.VMEM((n_sp, ROWS8, flat), F32),
            pltpu.VMEM((n_tp, rows, chans), BF),
            pltpu.VMEM((1, n_tp, own, depth), BF),
            pltpu.VMEM((1, 2, own, depth), BF),
            pltpu.VMEM((1, own, depth), BF),
            pltpu.VMEM((1, own, depth), BF),
            pltpu.VMEM((own, depth), F32),
            pltpu.VMEM((n_tp, own, depth), BF),
            pltpu.VMEM((n_tp, own, ff), BF),
            pltpu.VMEM((n_sp, n_tp, own, d_loc), BF),
            pltpu.VMEM((n_sp, 2, own, d_loc), BF),
            pltpu.VMEM((n_sp, own, d_loc), BF),
            pltpu.VMEM((n_sp, own, d_loc), BF),
            dma((6,)),
            dma((n_sp,)),
            dma((n_sp,)),
            dma((2, 3, n_sp)),
            dma((2, 3, n_sp)),
            dma((2, 3, n_sp)),
            dma((2, 3, n_sp)),
            dma((2, 3)),
            dma((2, 3)),
            dma((1, 3)),
            dma((1, 3)),
            dma((n_sp, 3)),
            dma((n_sp, 3)),
        ],
        compiler_params=pltpu.CompilerParams(
            collective_id=0, has_side_effects=True, vmem_limit_bytes=60 * 1024 * 1024
        ),
    )(
        residual,
        state_input,
        gate_input,
        pow_real,
        pow_imag,
        tiled(in_real.transpose(0, 2, 1)),
        tiled(in_imag.transpose(0, 2, 1)),
        tiled(read_real),
        tiled(read_imag),
        skip_gain[None, :],
        value_weight,
        glu_weight,
        mix_weight,
        norm_gain[None, :],
        mlp_gate,
        mlp_up,
        mlp_down,
    )


def quick_kernel(
    n_sp,
    width,
    states,
    residual_h,
    u_h,
    gate_in_h,
    decay_h,
    freq_h,
    step_h,
    drive_re_h,
    drive_im_h,
    read_re_h,
    read_im_h,
    skip_h,
    value_h,
    glu_h,
    mix_h,
    gain_h,
    gate_h,
    up_h,
    down_h,
    out,
    residual,
    u,
    gate_in,
    decay,
    freq,
    log_step,
    drive_re,
    drive_im,
    read_re,
    read_im,
    skip,
    value_w,
    glu_w,
    mix_w,
    gain,
    w_gate,
    w_up,
    w_down,
    wide,
    pow_real,
    pow_imag,
    ratio,
    st_real,
    st_imag,
    masked,
    ends,
    acts,
    part,
    rx_pair,
    relay,
    rx_far,
    inner,
    normed,
    hidden,
    c_part,
    c_in,
    c_relay,
    load_sem,
    end_send,
    end_recv,
    z_send,
    z_recv,
    y_send,
    y_recv,
    y_late,
    z_more,
    z_last,
    ag_send,
    ag_recv,
    rs_send,
    rs_recv,
    c_send,
    c_recv,
):
    g, s, t = lax.axis_index("grp"), lax.axis_index("sp"), lax.axis_index("tp")
    low, high_bit = t % 2, t // 2
    p = t + 1 - 2 * low
    q = t + 2 - 4 * high_bit
    far = 3 - t
    other = 1 - g
    rows, chans = u.shape
    groups, flat = decay.shape[0], st_real.shape[1]
    own, depth = residual.shape
    k_loc, ff = gate_h.shape
    d_loc = down_h.shape[1]
    n_tp = acts.shape[0]
    k_half, f_half = k_loc // 2, ff // 2
    k_piece, d_half = k_half // PIECES, d_loc // HALVES
    f_piece = f_half * HALVES // PIECES

    barrier = pltpu.get_barrier_semaphore()
    pl.semaphore_signal(barrier, inc=1, device_id={"tp": p})
    pl.semaphore_signal(barrier, inc=1, device_id={"tp": q})
    pl.semaphore_signal(barrier, inc=1, device_id={"grp": other})

    @pl.loop(1, n_sp)
    def _(d):
        pl.semaphore_signal(barrier, inc=1, device_id={"sp": (s + d) % n_sp})

    place = pl.ds(pl.multiple_of(s * k_loc, k_loc), k_loc)
    pairs_of = (
        (gate_h, w_gate.at[place, :]),
        (decay_h, decay),
        (freq_h, freq),
        (step_h, log_step),
        (drive_re_h, drive_re),
        (drive_im_h, drive_im),
        (u_h, u),
        (read_re_h, read_re),
        (read_im_h, read_im),
        (skip_h, skip),
        (up_h, w_up.at[place, :]),
        (down_h, w_down.at[s]),
        (value_h, value_w),
        (glu_h, glu_w),
        (gate_in_h, gate_in),
        (mix_h, mix_w),
        (residual_h, residual),
        (gain_h, gain),
    )
    loads = [
        pltpu.make_async_copy(a, b, load_sem.at[i]) for i, (a, b) in enumerate(pairs_of)
    ]
    for load in loads:
        load.start()
    pl.semaphore_wait(barrier, 3 + n_sp - 1)

    bufs = (w_gate, w_up, w_down)
    behind = (s, n_sp - 1 - s)
    n_early, n_late = 2 * PIECES, PIECES

    def await_bytes(sem, ref):
        pltpu.make_async_copy(ref, ref, sem).wait()

    def mine(c, i, origin, half):
        if c < 2:
            row = pl.multiple_of(origin * k_loc + half * k_half + i * k_piece, k_piece)
            return bufs[c].at[pl.ds(row, k_piece), :]
        row = pl.multiple_of(half * f_half + (i % PER) * f_piece, f_piece)
        return bufs[c].at[origin, pl.ds(row, f_piece), pl.ds((i // PER) * d_half, d_half)]

    def z_copy(side, c, i, origin):
        piece = mine(c, i, origin, g)
        return pltpu.make_async_remote_copy(
            src_ref=piece,
            dst_ref=piece,
            send_sem=z_send.at[side, c],
            recv_sem=z_recv.at[c, i, origin - side],
            device_id={"sp": ahead(side)},
        )

    def y_copy(c, i, origin, half):
        piece = mine(c, i, origin, half)
        return pltpu.make_async_remote_copy(
            src_ref=piece,
            dst_ref=piece,
            send_sem=y_send.at[c // 2],
            recv_sem=y_recv.at[0] if c < 2 else y_late.at[origin, i // (PER)],
            device_id={"grp": other},
        )

    def more_copy(side, c, i):
        piece = mine(c, i, s, other)
        return pltpu.make_async_remote_copy(
            src_ref=piece,
            dst_ref=piece,
            send_sem=z_send.at[side, c],
            recv_sem=z_more.at[0 if c < 2 else 1 + HALVES * (i == PIECES - 1) + i // PER],
            device_id={"sp": ahead(side)},
        )

    def last_copy(side, k):
        piece = mine(2, PIECES - 1, source(side, k), other)
        return pltpu.make_async_remote_copy(
            src_ref=piece,
            dst_ref=piece,
            send_sem=z_send.at[side, 2],
            recv_sem=z_last.at[0],
            device_id={"sp": ahead(side)},
        )

    def last_on(side, b):
        if b == 1:
            await_bytes(z_more.at[1 + HALVES + (PIECES - 1) // PER], mine(2, 0, s, g))
        else:
            last_copy(side, b).wait_recv()
        if b < n_sp - 1:
            last_copy(side, b).start()

    def last_advance(b):
        for side in range(2):
            pl.when(behind[side] == b)(functools.partial(last_on, side, b))

    def ahead(side):
        return (s + 1) % n_sp if side == 0 else (s + n_sp - 1) % n_sp

    def source(side, k):
        return (s + n_sp - k) % n_sp if side == 0 else (s + k) % n_sp

    def own_sends(side, c, pieces):
        for i in pieces:
            z_copy(side, c, i, s).start()

    def end_sends(side):
        for c in range(3):
            if c == 2:
                own_sends(side, 2, range(PIECES))
            for i in range(PIECES):
                more_copy(side, c, i).start()

    def own_early(c, pieces):
        for side in range(2):
            pl.when(behind[side] < n_sp - 1)(functools.partial(own_sends, side, c, pieces))

    def shared(side, k):
        return behind[side] > 1 if k == 1 else behind[side] >= k

    def onward(side, k, c, i, last):
        @pl.when(behind[side] < n_sp - 1)
        def _():
            z_copy(side, c, i, source(side, k)).start()

        if last:

            @pl.when(jnp.logical_and(behind[side] == k, k < n_sp - 1))
            def _():
                own_sends(side, 2, range(PIECES))

    def pass_on(side, k, c, i, last, hold):
        origin = source(side, k)
        z_copy(side, c, i, origin).wait_recv()
        if not hold:
            onward(side, k, c, i, last)

        only_z = c == 2 and i == PIECES - 1

        @pl.when(behind[side] > k if only_z else shared(side, k))
        def _():
            y_copy(c, i, origin, g).start()

    def advance(*slots, hold=False):
        for n in slots:
            for side in range(2):
                if n < n_early * (n_sp - 1):
                    k, c, i = n // n_early + 1, n % n_early // PIECES, n % PIECES
                    last = n % n_early == n_early - 1
                    work = functools.partial(pass_on, side, k, c, i, last, hold)
                    pl.when(behind[side] >= k)(work)
                for b in range(1, n_sp):
                    m = n - n_early * max(b, 2)
                    if 0 <= m < n_late * b:
                        work = functools.partial(
                            pass_on, side, m // n_late + 1, 2, m % n_late, False, False
                        )
                        pl.when(behind[side] == b)(work)

    loads[0].wait()
    own_early(0, range(PIECES))

    for load in loads[1:4]:
        load.wait()
    eye = lax.broadcasted_iota(jnp.int32, (groups, groups), 0) == lax.broadcasted_iota(
        jnp.int32, (groups, groups), 1
    )
    step = jnp.exp(jnp.sum(jnp.where(eye, log_step[...], 0.0), axis=1, keepdims=True))
    rate, turn = decay[...], freq[...]
    magnitude = jnp.exp(rate * step)
    bar_re = magnitude * jnp.cos(turn * step)
    bar_im = magnitude * jnp.sin(turn * step)
    modulus = rate * rate + turn * turn
    ratio_re = ((bar_re - 1.0) * rate + bar_im * turn) / modulus
    ratio_im = (bar_im * rate - (bar_re - 1.0) * turn) / modulus
    tiles = max(1, 128 // states)
    lanes = tiles * states
    part_of = lax.broadcasted_iota(jnp.int32, (1, lanes), 1) // states

    def spread(target, row, value):
        doubled = jnp.concatenate([value] * tiles, axis=1)
        for tile in range(groups // tiles):
            line = doubled[tile * tiles : tile * tiles + 1, :]
            for j in range(1, tiles):
                line = jnp.where(part_of == j, doubled[tile * tiles + j : tile * tiles + j + 1, :], line)
            target[row : row + 1, tile * lanes : (tile + 1) * lanes] = line

    spread(ratio, 0, ratio_re)
    spread(ratio, 1, ratio_im)
    up_re, up_im = bar_re, bar_im
    for n in range(ROWS8):
        spread(pow_real, n, up_re)
        spread(pow_imag, n, up_im)
        up_re, up_im = up_re * bar_re - up_im * bar_im, up_re * bar_im + up_im * bar_re

    for load in loads[4:9]:
        load.wait()
    row_group = lax.broadcasted_iota(jnp.int32, (chans, lanes), 0) // width
    lane = lax.broadcasted_iota(jnp.int32, (chans, lanes), 1)
    for i, ref in enumerate((drive_re, drive_im, read_re, read_im)):
        value = jnp.concatenate([ref[...]] * tiles, axis=1)
        for tile in range(flat // lanes):
            kept = jnp.where(row_group == (lane + tile * lanes) // states, value, 0.0)
            at = slice(tile * lanes, (tile + 1) * lanes)
            for j, piece in enumerate(split(kept)):
                wide[2 * i + j, :, at] = piece

    @pl.loop(0, rows // own)
    def _(b):
        at = pl.ds(pl.multiple_of(b * own, own), own)
        x = u[at, :]
        push_re = mm(x, wide[0]) + mm(x, wide[1])
        push_im = mm(x, wide[2]) + mm(x, wide[3])
        st_real[at, :] = ratio[0:1, :] * push_re - ratio[1:2, :] * push_im
        st_imag[at, :] = ratio[0:1, :] * push_im + ratio[1:2, :] * push_re

    sub = lax.broadcasted_iota(jnp.int32, (ROWS8, flat), 0)
    for i, reach in enumerate((1, 2, 4)):
        masked[2 * i] = jnp.where(sub >= reach, pow_real[reach - 1 : reach, :], 0.0)
        masked[2 * i + 1] = jnp.where(sub >= reach, pow_imag[reach - 1 : reach, :], 0.0)

    def scan_step(b, carry):
        c_re, c_im = carry
        at = pl.ds(pl.multiple_of(b * ROWS8, ROWS8), ROWS8)
        x_re, x_im = st_real[at, :], st_imag[at, :]
        for i, reach in enumerate((1, 2, 4)):
            m_re, m_im = pltpu.roll(x_re, reach, 0), pltpu.roll(x_im, reach, 0)
            a_re, a_im = masked[2 * i], masked[2 * i + 1]
            x_re, x_im = x_re + a_re * m_re - a_im * m_im, x_im + a_re * m_im + a_im * m_re
        p_re, p_im = pow_real[...], pow_imag[...]
        x_re, x_im = x_re + p_re * c_re - p_im * c_im, x_im + p_re * c_im + p_im * c_re
        st_real[at, :] = x_re
        st_imag[at, :] = x_im
        return x_re[ROWS8 - 1 :, :], x_im[ROWS8 - 1 :, :]

    zero = jnp.zeros((1, flat), F32)
    blocks = rows // ROWS8
    tip = lax.fori_loop(0, blocks // 2, scan_step, (zero, zero))
    advance(0, hold=True)
    end_re, end_im = lax.fori_loop(blocks // 2, blocks, scan_step, tip)
    ends[s, :, :flat] = end_re
    ends[s, :, flat:] = end_im

    def end_copy(target, origin):
        return pltpu.make_async_remote_copy(
            src_ref=ends.at[origin],
            dst_ref=ends.at[origin],
            send_sem=end_send.at[target],
            recv_sem=end_recv.at[origin],
            device_id={"sp": target},
        )

    @pl.loop(s + 1, n_sp)
    def _(later):
        end_copy(later, s).start()

    for load in loads[10:12]:
        load.wait()
    own_early(1, range(PIECES))
    for side in range(2):
        pl.when(behind[side] == 0)(functools.partial(end_sends, side))
        pl.when(behind[side] >= 1)(functools.partial(onward, side, 1, 0, 0, False))
    advance(1)
    last_re, last_im = pow_real[ROWS8 - 1 :, :], pow_imag[ROWS8 - 1 :, :]
    long_re, long_im = last_re, last_im
    reach = ROWS8
    while reach < rows:
        long_re, long_im = long_re * long_re - long_im * long_im, 2.0 * long_re * long_im
        reach *= 2

    advance(2, 3, 4)

    @pl.loop(0, s)
    def _(earlier):
        end_copy((s + 1) % n_sp, earlier).wait_recv()

    def carry_step(j, carry):
        c_re, c_im = carry
        e_re, e_im = ends[j, :, :flat], ends[j, :, flat:]
        n_re = long_re * c_re - long_im * c_im + e_re
        n_im = long_re * c_im + long_im * c_re + e_im
        return jnp.where(j < s, n_re, c_re), jnp.where(j < s, n_im, c_im)

    carry = lax.fori_loop(0, n_sp - 1, carry_step, (zero, zero))

    def lift(b, carry):
        c_re, c_im = carry
        at = pl.ds(pl.multiple_of(b * ROWS8, ROWS8), ROWS8)
        p_re, p_im = pow_real[...], pow_imag[...]
        st_real[at, :] = st_real[at, :] + p_re * c_re - p_im * c_im
        st_imag[at, :] = st_imag[at, :] + p_re * c_im + p_im * c_re
        return last_re * c_re - last_im * c_im, last_re * c_im + last_im * c_re

    carry = lax.fori_loop(0, blocks // 2, lift, carry)
    advance(5)
    lax.fori_loop(blocks // 2, blocks, lift, carry)
    loads[9].wait()

    def read_block(b):
        at = pl.ds(pl.multiple_of(b * own, own), own)
        high, small = split(st_real[at, :])
        y = mm_t(high, wide[4]) + mm_t(small, wide[4]) + mm_t(high, wide[5])
        high, small = split(st_imag[at, :])
        y = y - (mm_t(high, wide[6]) + mm_t(small, wide[6]) + mm_t(high, wide[7]))
        y = y + skip[...] * u[at, :].astype(F32)
        acts[t, at, :] = jax.nn.gelu(y).astype(BF)

    half_rows = rows // own // 2
    pl.loop(0, half_rows)(read_block)
    advance(6)
    pl.loop(half_rows, rows // own)(read_block)
    advance(7)

    def gather_tp(buf, lane_no, between, later):
        def copy(slot, kind, target):
            return pltpu.make_async_remote_copy(
                src_ref=buf.at[slot],
                dst_ref=buf.at[slot],
                send_sem=ag_send.at[lane_no, kind],
                recv_sem=ag_recv.at[lane_no, kind],
                device_id={"tp": target},
            )

        sent = [copy(t, 0, q), copy(t, 1, p)]
        for item in sent:
            item.start()
        between()
        copy(q, 0, q).wait_recv()
        relayed = copy(q, 2, p)
        relayed.start()
        later()
        copy(p, 1, p).wait_recv()
        copy(far, 2, p).wait_recv()
        return sent + [relayed]

    def rs_pair(index):
        return pltpu.make_async_remote_copy(
            src_ref=part.at[(far, p)[index]],
            dst_ref=rx_pair.at[index],
            send_sem=rs_send.at[index],
            recv_sem=rs_recv.at[index],
            device_id={"tp": p},
        )

    across = pltpu.make_async_remote_copy(
        src_ref=relay,
        dst_ref=rx_far,
        send_sem=rs_send.at[2],
        recv_sem=rs_recv.at[2],
        device_id={"tp": q},
    )

    pending = gather_tp(acts, 0, lambda: advance(8, 9), lambda: advance(10))
    for load in loads[12:]:
        load.wait()

    def mix_block(r):
        at = pl.ds(pl.multiple_of(r * own, own), own)
        value = jnp.zeros((own, value_w.shape[1]), F32)
        gated = value
        for j in range(n_tp):
            a = acts[j, at, :]
            value = value + mm(a, value_w[j * chans : (j + 1) * chans, :])
            gated = gated + mm(a, glu_w[j * chans : (j + 1) * chans, :])
        mixed = jax.nn.sigmoid(gate_in[at, :].astype(F32)) * value * jax.nn.sigmoid(gated)
        part[r] = mm(mixed.astype(BF), mix_w[...]).astype(BF)

    mix_block(far)
    rs_pair(0).start()
    advance(11)
    mix_block(q)
    rs_pair(0).wait_recv()
    relay[...] = (part[q].astype(F32) + rx_pair[0].astype(F32)).astype(BF)
    across.start()
    advance(12)
    mix_block(p)
    rs_pair(1).start()
    mix_block(t)
    advance(13, 14, 15, 16, 17)
    rs_pair(1).wait_recv()
    across.wait_recv()
    pending += [rs_pair(0), rs_pair(1), across]
    near = part[t].astype(F32) + rx_pair[1].astype(F32)
    x = residual[...].astype(F32) + (near + rx_far[...].astype(F32))
    inner[...] = x
    scale = lax.rsqrt(jnp.mean(x * x, axis=-1, keepdims=True) + EPSILON)
    normed[t] = (x * scale * gain[...]).astype(BF)

    pending += gather_tp(normed, 1, lambda: advance(18, 19, 20, 21, 22, 23), lambda: None)

    advance(24)
    last_advance(1)

    advance(25)
    near_end = jnp.logical_or(behind[0] == 1, behind[1] == 1)

    @pl.when(near_end)
    def _():
        await_bytes(z_more.at[0], w_gate.at[:k_loc, :])
        await_bytes(y_recv.at[0], w_gate.at[: (n_sp - 2) * k_loc, :])

    @pl.when(jnp.logical_not(near_end))
    def _():
        await_bytes(y_recv.at[0], w_gate.at[: (n_sp - 1) * k_loc, :])

    advance(26)

    def hidden_block(r):
        x = normed[r]
        hidden[r] = (jax.nn.silu(mm(x, w_gate[...])) * mm(x, w_up[...])).astype(BF)

    pl.loop(0, n_tp // 2)(hidden_block)
    advance(27)
    pl.loop(n_tp // 2, n_tp)(hidden_block)
    advance(28)
    last_advance(2)

    def col_pair(o, h, index):
        return pltpu.make_async_remote_copy(
            src_ref=c_part.at[o, h, (far, p)[index]],
            dst_ref=c_in.at[o, h, index],
            send_sem=c_send.at[0],
            recv_sem=c_recv.at[o, h if index == 0 else HALVES],
            device_id={"tp": p},
        )

    def col_far(o, h):
        return pltpu.make_async_remote_copy(
            src_ref=c_relay.at[o, h],
            dst_ref=c_in.at[o, h, 2],
            send_sem=c_send.at[0],
            recv_sem=c_recv.at[o, HALVES],
            device_id={"tp": q},
        )

    def column(o, h):
        weight = w_down.at[o, :, h * d_half : (h + 1) * d_half]
        for r, index in ((far, 0), (p, 1), (q, None), (t, None)):
            c_part[o, h, r] = mm(hidden[r], weight[...]).astype(BF)
            if index is not None:
                col_pair(o, h, index).start()
        col_pair(o, h, 0).wait_recv()
        both = c_part[o, h, q].astype(F32) + c_in[o, h, 0].astype(F32)
        c_relay[o, h] = both.astype(BF)
        col_far(o, h).start()

    def settle(o):
        await_bytes(c_recv.at[o, HALVES], c_in.at[o, :, 1:3])
        for h in range(HALVES):
            near = c_part[o, h, t].astype(F32) + c_in[o, h, 1].astype(F32)
            at = pl.ds(pl.multiple_of(o * d_loc + h * d_half, d_half), d_half)
            out[:, at] = (inner[:, at] + 0.5 * (near + c_in[o, h, 2].astype(F32))).astype(BF)

    def both_sides(k, work):
        for side in range(2):
            pl.when(behind[side] >= k)(functools.partial(work, side, k))

    def next_column(h, side, k):
        origin = source(side, k)
        row = pl.multiple_of(other * f_half, f_half)
        came = w_down.at[origin, pl.ds(row, f_half), h * d_half : (h + 1) * d_half]
        piece = mine(2, h * PER, origin, other)
        pairs = h == HALVES - 1

        @pl.when(behind[side] > k if pairs else shared(side, k))
        def _():
            await_bytes(y_late.at[origin, h], came)

        if pairs and k > 1:

            @pl.when(behind[side] == k)
            def _():
                await_bytes(y_late.at[origin, h], piece)

        if k == 1:

            @pl.when(behind[side] == 1)
            def _():
                await_bytes(z_more.at[1 + h], piece if pairs else came)

        column(origin, h)

    def next_settle(side, k):
        settle(source(side, k))

    column(s, 0)
    column(s, 1)
    advance(29)
    both_sides(1, functools.partial(next_column, 0))
    advance(30)
    both_sides(1, functools.partial(next_column, 1))
    advance(31)
    settle(s)
    advance(32)
    both_sides(2, functools.partial(next_column, 0))
    advance(33, 34)
    both_sides(2, functools.partial(next_column, 1))
    advance(35)
    both_sides(1, next_settle)
    both_sides(3, functools.partial(next_column, 0))
    both_sides(2, next_settle)
    for item in pending:
        item.wait_send()

    @pl.loop(s + 1, n_sp)
    def _(later):
        end_copy(later, s).wait_send()

    def sent(side, b):
        count = max(2, b + 1)
        for c in range(2):
            await_bytes(z_send.at[side, c], w_gate.at[: count * k_half, :])
        count = count * PIECES + (b > 0)
        await_bytes(z_send.at[side, 2], w_gate.at[: count * k_piece, :])

    for side in range(2):
        for b in range(n_sp - 1):
            pl.when(behind[side] == b)(functools.partial(sent, side, b))

    def exchanged(count):
        await_bytes(y_send.at[0], w_gate.at[: count * k_loc, :])
        await_bytes(y_send.at[1], w_gate.at[: (count * PIECES - 1) * k_piece, :])

    pl.when(near_end)(functools.partial(exchanged, n_sp - 2))
    pl.when(jnp.logical_not(near_end))(functools.partial(exchanged, n_sp - 1))
    last_advance(3)
    both_sides(3, functools.partial(next_column, 1))
    both_sides(3, next_settle)
    await_bytes(c_send.at[0], c_in)


def quick(
    residual,
    state_input,
    gate_input,
    decay_real,
    frequency,
    log_step,
    drive_real,
    drive_imag,
    read_real,
    read_imag,
    skip_gain,
    value_weight,
    glu_weight,
    mix_weight,
    norm_gain,
    mlp_gate,
    mlp_up,
    mlp_down,
):
    n_sp, n_tp = lax.axis_size("sp"), lax.axis_size("tp")
    groups, states, width = drive_real.shape
    flat, chans = groups * states, groups * width
    rows = state_input.shape[0]
    own, depth = residual.shape
    k_loc, ff = mlp_gate.shape
    d_loc = mlp_down.shape[1]
    d_half = d_loc // HALVES
    hbm = pl.BlockSpec(memory_space=pltpu.HBM)
    dma = pltpu.SemaphoreType.DMA
    operands = (
        residual,
        state_input,
        gate_input,
        decay_real,
        frequency,
        log_step[None, :],
        drive_real.transpose(0, 2, 1).reshape(chans, states),
        drive_imag.transpose(0, 2, 1).reshape(chans, states),
        read_real.reshape(chans, states),
        read_imag.reshape(chans, states),
        skip_gain[None, :],
        value_weight,
        glu_weight,
        mix_weight,
        norm_gain[None, :],
        mlp_gate,
        mlp_up,
        mlp_down,
    )
    return pl.pallas_call(
        functools.partial(quick_kernel, n_sp, width, states),
        out_shape=pltpu.VMEM((own, depth), BF),
        in_specs=[hbm] * len(operands),
        out_specs=pl.BlockSpec(memory_space=pltpu.VMEM),
        scratch_shapes=[pltpu.VMEM(x.shape, x.dtype) for x in operands[:15]]
        + [
            pltpu.VMEM((n_sp * k_loc, ff), BF),
            pltpu.VMEM((n_sp * k_loc, ff), BF),
            pltpu.VMEM((n_sp, ff, d_loc), BF),
            pltpu.VMEM((8, chans, flat), BF),
            pltpu.VMEM((ROWS8, flat), F32),
            pltpu.VMEM((ROWS8, flat), F32),
            pltpu.VMEM((2, flat), F32),
            pltpu.VMEM((rows, flat), F32),
            pltpu.VMEM((rows, flat), F32),
            pltpu.VMEM((6, ROWS8, flat), F32),
            pltpu.VMEM((n_sp, 1, 2 * flat), F32),
            pltpu.VMEM((n_tp, rows, chans), BF),
            pltpu.VMEM((n_tp, own, depth), BF),
            pltpu.VMEM((2, own, depth), BF),
            pltpu.VMEM((own, depth), BF),
            pltpu.VMEM((own, depth), BF),
            pltpu.VMEM((own, depth), F32),
            pltpu.VMEM((n_tp, own, depth), BF),
            pltpu.VMEM((n_tp, own, ff), BF),
            pltpu.VMEM((n_sp, HALVES, n_tp, own, d_half), BF),
            pltpu.VMEM((n_sp, HALVES, 3, own, d_half), BF),
            pltpu.VMEM((n_sp, HALVES, own, d_half), BF),
            dma((len(operands),)),
            dma((n_sp,)),
            dma((n_sp,)),
            dma((2, 3)),
            dma((3, PIECES, n_sp - 1)),
            dma((2,)),
            dma((1,)),
            dma((n_sp, HALVES)),
            dma((1 + 2 * HALVES,)),
            dma((1,)),
            dma((2, 3)),
            dma((2, 3)),
            dma((3,)),
            dma((3,)),
            dma((1,)),
            dma((n_sp, HALVES + 1)),
        ],
        compiler_params=pltpu.CompilerParams(
            collective_id=0, has_side_effects=True, vmem_limit_bytes=60 * 1024 * 1024
        ),
    )(*operands)


def solution(mesh):
    placed = (
        P(("grp", "sp", "tp"), None),
        P(("grp", "sp"), "tp"),
        P(("grp", "sp"), "tp"),
        P("tp", None),
        P("tp", None),
        P("tp"),
        P("tp", None, None),
        P("tp", None, None),
        P("tp", None, None),
        P("tp", None, None),
        P("tp"),
        P(None, "tp"),
        P(None, "tp"),
        P("tp", None),
        P(),
        P("sp", "tp"),
        P("sp", "tp"),
        P("tp", "sp"),
    )
    body = shards
    if (mesh.shape["tp"], mesh.shape["grp"]) == (4, 2):
        body = quick if mesh.shape["sp"] == 4 else fused
    return jax.shard_map(
        body, mesh=mesh, in_specs=placed, out_specs=P(("grp", "sp", "tp"), None), check_vma=False
    )
```

```python
import functools
import jax
import jax.numpy as jnp
from jax import lax
from jax.experimental import pallas as pl
from jax.experimental.pallas import tpu as pltpu
from jax.sharding import PartitionSpec as P

BF = jnp.bfloat16
F32 = jnp.float32
ROWS8 = 8
PIECES = 4
HALVES = 2
PER = PIECES // HALVES

HIGH = lax.Precision.HIGHEST
EPSILON = 1e-06


def carried_in(value, axis, join, neutral):
    count, mine = (lax.axis_size(axis), lax.axis_index(axis))
    pieces = jax.tree.map(lambda part: lax.all_gather(part, axis), value)
    subtotal = jax.tree.map(
        lambda part, zero: jnp.full_like(part, 0) + jnp.asarray(zero, part.dtype), value, neutral
    )

    def step(position, subtotal):
        longer = join(subtotal, jax.tree.map(lambda part: part[position], pieces))
        return jax.tree.map(lambda new, old: jnp.where(position < mine, new, old), longer, subtotal)

    return lax.fori_loop(0, count - 1, step, subtotal)


def discretize(decay_real, frequency, log_step, drive_real, drive_imag):
    step = jnp.exp(log_step)[:, None]
    magnitude = jnp.exp(decay_real * step)
    turned = frequency * step
    bar_real = magnitude * jnp.cos(turned)
    bar_imag = magnitude * jnp.sin(turned)
    modulus = decay_real * decay_real + frequency * frequency
    ratio_real = ((bar_real - 1.0) * decay_real + bar_imag * frequency) / modulus
    ratio_imag = (bar_imag * decay_real - (bar_real - 1.0) * frequency) / modulus
    in_real = ratio_real[..., None] * drive_real - ratio_imag[..., None] * drive_imag
    in_imag = ratio_real[..., None] * drive_imag + ratio_imag[..., None] * drive_real
    return (bar_real, bar_imag, in_real, in_imag)


def combine(earlier, later):
    real_one, imag_one, state_real_one, state_imag_one = earlier
    real_two, imag_two, state_real_two, state_imag_two = later
    return (
        real_one * real_two - imag_one * imag_two,
        real_one * imag_two + imag_one * real_two,
        real_two * state_real_one - imag_two * state_imag_one + state_real_two,
        real_two * state_imag_one + imag_two * state_real_one + state_imag_two,
    )


def powers(log_rate, angle_rate, count):
    return (
        jnp.exp(log_rate * count) * jnp.cos(angle_rate * count),
        jnp.exp(log_rate * count) * jnp.sin(angle_rate * count),
    )


def block_states(flat_inputs, decay_real, frequency, log_step, in_real, in_imag):
    rows = flat_inputs.shape[0]
    groups, states, width = in_real.shape
    flat = groups * states
    eye = jnp.eye(groups, dtype=jnp.float32)
    wide_real = jnp.einsum("gph,gk->ghkp", in_real, eye).reshape(groups * width, flat)
    wide_imag = jnp.einsum("gph,gk->ghkp", in_imag, eye).reshape(groups * width, flat)
    state_real = jnp.dot(flat_inputs, wide_real, precision=HIGH)
    state_imag = jnp.dot(flat_inputs, wide_imag, precision=HIGH)
    step = jnp.exp(log_step)[:, None]
    log_rate = (decay_real * step).reshape(1, flat)
    angle_rate = (frequency * step).reshape(1, flat)
    reach = 1
    while reach < rows:
        lift_real, lift_imag = powers(log_rate, angle_rate, float(reach))
        blank = jnp.zeros((reach, flat), jnp.float32)
        moved_real = jnp.concatenate([blank, state_real[: rows - reach]], axis=0)
        moved_imag = jnp.concatenate([blank, state_imag[: rows - reach]], axis=0)
        state_real, state_imag = (
            state_real + lift_real * moved_real - lift_imag * moved_imag,
            state_imag + lift_real * moved_imag + lift_imag * moved_real,
        )
        reach = reach * 2
    counts = (lax.iota(jnp.int32, rows) + 1).astype(jnp.float32)[:, None]
    power_real, power_imag = powers(log_rate, angle_rate, counts)
    return (power_real, power_imag, state_real, state_imag)


def readout(state_real, state_imag, read_real, read_imag, flat_inputs, skip_gain):
    groups, width, states = read_real.shape
    eye = jnp.eye(groups, dtype=jnp.float32)
    wide_real = jnp.einsum("ghp,gk->gpkh", read_real, eye).reshape(groups * states, groups * width)
    wide_imag = jnp.einsum("ghp,gk->gpkh", read_imag, eye).reshape(groups * states, groups * width)
    output = jnp.dot(state_real, wide_real, precision=HIGH) - jnp.dot(
        state_imag, wide_imag, precision=HIGH
    )
    output = output + skip_gain * flat_inputs
    return jax.nn.gelu(output).astype(jnp.bfloat16)


def normalize(inner, norm_gain):
    scale = lax.rsqrt(jnp.mean(inner * inner, axis=-1, keepdims=True) + EPSILON)
    return (inner * scale * norm_gain).astype(jnp.bfloat16)


def shards(
    residual,
    state_input,
    gate_input,
    decay_real,
    frequency,
    log_step,
    drive_real,
    drive_imag,
    read_real,
    read_imag,
    skip_gain,
    value_weight,
    glu_weight,
    mix_weight,
    norm_gain,
    mlp_gate,
    mlp_up,
    mlp_down,
):
    bar_real, bar_imag, in_real, in_imag = discretize(
        decay_real, frequency, log_step, drive_real, drive_imag
    )
    flat_inputs = state_input.astype(jnp.float32)
    power_real, power_imag, local_real, local_imag = block_states(
        flat_inputs, decay_real, frequency, log_step, in_real, in_imag
    )
    ends = (power_real[-1], power_imag[-1], local_real[-1], local_imag[-1])
    ones = jnp.ones_like(ends[0])
    zeros = jnp.zeros_like(ends[0])
    incoming = carried_in(
        (ends[0], ends[1], ends[2], ends[3]), "sp", combine, (ones, zeros, zeros, zeros)
    )
    carry_real = incoming[2]
    carry_imag = incoming[3]
    state_real = local_real + power_real * carry_real - power_imag * carry_imag
    state_imag = local_imag + power_real * carry_imag + power_imag * carry_real
    acts = readout(state_real, state_imag, read_real, read_imag, flat_inputs, skip_gain)
    piece = lax.all_gather(acts, "tp", axis=1, tiled=True)
    value = jnp.dot(piece, value_weight, preferred_element_type=jnp.float32)
    gated = jnp.dot(piece, glu_weight, preferred_element_type=jnp.float32)
    mixed = (jax.nn.sigmoid(gate_input.astype(jnp.float32)) * value * jax.nn.sigmoid(gated)).astype(
        jnp.bfloat16
    )
    branch = lax.psum_scatter(
        jnp.dot(mixed, mix_weight, preferred_element_type=jnp.float32).astype(jnp.bfloat16),
        "tp",
        scatter_dimension=0,
        tiled=True,
    ).astype(jnp.float32)
    inner = residual.astype(jnp.float32) + branch
    normed = lax.all_gather(normalize(inner, norm_gain), "tp", axis=0, tiled=True)
    hidden_gate = jnp.dot(
        normed,
        lax.all_gather(mlp_gate, "sp", axis=0, tiled=True),
        preferred_element_type=jnp.float32,
    )
    hidden_up = jnp.dot(
        normed, lax.all_gather(mlp_up, "sp", axis=0, tiled=True), preferred_element_type=jnp.float32
    )
    hidden = (jax.nn.silu(hidden_gate) * hidden_up).astype(jnp.bfloat16)
    down = jnp.dot(
        hidden,
        lax.all_gather(mlp_down, "sp", axis=1, tiled=True),
        preferred_element_type=jnp.float32,
    )
    down_own = lax.psum_scatter(
        down.astype(jnp.bfloat16), "tp", scatter_dimension=0, tiled=True
    ).astype(jnp.float32)
    return (inner + 0.5 * down_own).astype(jnp.bfloat16)


def mm(a, b):
    return jnp.dot(a, b, preferred_element_type=F32)


def mm_t(a, b):
    return lax.dot_general(a, b, (((1,), (1,)), ((), ())), preferred_element_type=F32)


def split(x):
    high = x.astype(BF)
    return high, (x - high.astype(F32)).astype(BF)


def layer_kernel(
    n_sp,
    width,
    states,
    residual,
    u,
    gate_in,
    pow_real,
    pow_imag,
    in_real,
    in_imag,
    rd_real,
    rd_imag,
    skip,
    value_h,
    glu_h,
    mix_h,
    gain,
    gate_h,
    up_h,
    down_h,
    out,
    value_w,
    glu_w,
    mix_w,
    w_gate,
    w_up,
    w_down,
    wide,
    st_real,
    st_imag,
    masked,
    ends,
    acts,
    part,
    rx_pair,
    relay,
    rx_far,
    inner,
    normed,
    hidden,
    c_part,
    c_pair,
    c_relay,
    c_far,
    load_sem,
    end_send,
    end_recv,
    z_send,
    z_recv,
    y_send,
    y_recv,
    ag_send,
    ag_recv,
    rs_send,
    rs_recv,
    c_send,
    c_recv,
):
    g, s, t = lax.axis_index("grp"), lax.axis_index("sp"), lax.axis_index("tp")
    low, high_bit = t % 2, t // 2
    p = t + 1 - 2 * low
    q = t + 2 - 4 * high_bit
    far = 3 - t
    other = 1 - g
    rows, chans = u.shape
    flat = st_real.shape[1]
    own, depth = residual.shape
    k_loc = gate_h.shape[0]
    ff, d_loc = down_h.shape
    k_half, f_half = k_loc // 2, ff // 2

    barrier = pltpu.get_barrier_semaphore()
    pl.semaphore_signal(barrier, inc=1, device_id={"tp": p})
    pl.semaphore_signal(barrier, inc=1, device_id={"tp": q})
    pl.semaphore_signal(barrier, inc=1, device_id={"grp": other})

    @pl.loop(1, n_sp)
    def _(d):
        pl.semaphore_signal(barrier, inc=1, device_id={"sp": (s + d) % n_sp})

    def mine(ref, c, origin, half):
        if c < 2:
            return ref.at[pl.ds(pl.multiple_of(origin * k_loc + half * k_half, k_half), k_half), :]
        return ref.at[origin, pl.ds(pl.multiple_of(half * f_half, f_half), f_half), :]

    bufs = (w_gate, w_up, w_down)
    place = pl.ds(pl.multiple_of(s * k_loc, k_loc), k_loc)
    loads = [
        pltpu.make_async_copy(gate_h, w_gate.at[place, :], load_sem.at[0]),
        pltpu.make_async_copy(up_h, w_up.at[place, :], load_sem.at[1]),
        pltpu.make_async_copy(down_h, w_down.at[s], load_sem.at[2]),
        pltpu.make_async_copy(value_h, value_w, load_sem.at[3]),
        pltpu.make_async_copy(glu_h, glu_w, load_sem.at[4]),
        pltpu.make_async_copy(mix_h, mix_w, load_sem.at[5]),
    ]
    for load in loads:
        load.start()
    pl.semaphore_wait(barrier, 3 + n_sp - 1)

    def z_copy(side, c, k, origin, target):
        piece = mine(bufs[c], c, origin, g)
        return pltpu.make_async_remote_copy(
            src_ref=piece,
            dst_ref=piece,
            send_sem=z_send.at[side, c, k],
            recv_sem=z_recv.at[side, c, k],
            device_id={"sp": target},
        )

    def y_copy(side, c, k, origin, half):
        piece = mine(bufs[c], c, origin, half)
        return pltpu.make_async_remote_copy(
            src_ref=piece,
            dst_ref=piece,
            send_sem=y_send.at[side, c, k],
            recv_sem=y_recv.at[side, c, k],
            device_id={"grp": other},
        )

    right, left = (s + 1) % n_sp, (s + n_sp - 1) % n_sp
    has_right, has_left = s < n_sp - 1, s > 0

    for c in range(3):
        loads[c].wait()

        @pl.when(has_right)
        def _():
            z_copy(0, c, 1, s, right).start()

        @pl.when(has_left)
        def _():
            z_copy(1, c, 1, s, left).start()

    def onward(c, k):
        @pl.when(s >= k)
        def _():
            origin = (s + n_sp - k) % n_sp
            z_copy(0, c, k, origin, right).wait_recv()

            @pl.when(has_right)
            def _():
                z_copy(0, c, k + 1, origin, right).start()

            y_copy(0, c, k, origin, g).start()

        @pl.when(s + k < n_sp)
        def _():
            origin = (s + k) % n_sp
            z_copy(1, c, k, origin, left).wait_recv()

            @pl.when(has_left)
            def _():
                z_copy(1, c, k + 1, origin, left).start()

            y_copy(1, c, k, origin, g).start()

    def arrived(c):
        @pl.loop(1, n_sp)
        def _(k):
            @pl.when(s >= k)
            def _():
                y_copy(0, c, k, (s + n_sp - k) % n_sp, other).wait_recv()

            @pl.when(s + k < n_sp)
            def _():
                y_copy(1, c, k, (s + k) % n_sp, other).wait_recv()

    lanes = in_real.shape[1]
    row_group = lax.broadcasted_iota(jnp.int32, (chans, lanes), 0) // width
    lane = lax.broadcasted_iota(jnp.int32, (chans, lanes), 1)
    for i, ref in enumerate((in_real, in_imag, rd_real, rd_imag)):
        value = ref[...]
        for tile in range(flat // lanes):
            kept = jnp.where(row_group == (lane + tile * lanes) // states, value, 0.0)
            big, small = split(kept)
            at = slice(tile * lanes, (tile + 1) * lanes)
            wide[2 * i, :, at] = big
            wide[2 * i + 1, :, at] = small

    @pl.loop(0, rows // own)
    def _(b):
        at = pl.ds(pl.multiple_of(b * own, own), own)
        x = u[at, :]
        st_real[at, :] = mm(x, wide[0]) + mm(x, wide[1])
        st_imag[at, :] = mm(x, wide[2]) + mm(x, wide[3])

    sub = lax.broadcasted_iota(jnp.int32, (ROWS8, flat), 0)
    for i, reach in enumerate((1, 2, 4)):
        masked[2 * i] = jnp.where(sub >= reach, pow_real[reach - 1 : reach, :], 0.0)
        masked[2 * i + 1] = jnp.where(sub >= reach, pow_imag[reach - 1 : reach, :], 0.0)

    def scan_step(b, carry):
        c_re, c_im = carry
        at = pl.ds(pl.multiple_of(b * ROWS8, ROWS8), ROWS8)
        x_re, x_im = st_real[at, :], st_imag[at, :]
        for i, reach in enumerate((1, 2, 4)):
            m_re, m_im = pltpu.roll(x_re, reach, 0), pltpu.roll(x_im, reach, 0)
            a_re, a_im = masked[2 * i], masked[2 * i + 1]
            x_re, x_im = x_re + a_re * m_re - a_im * m_im, x_im + a_re * m_im + a_im * m_re
        p_re, p_im = pow_real[...], pow_imag[...]
        x_re, x_im = x_re + p_re * c_re - p_im * c_im, x_im + p_re * c_im + p_im * c_re
        st_real[at, :] = x_re
        st_imag[at, :] = x_im
        return x_re[ROWS8 - 1 :, :], x_im[ROWS8 - 1 :, :]

    zero = jnp.zeros((1, flat), F32)
    end_re, end_im = lax.fori_loop(0, rows // ROWS8, scan_step, (zero, zero))
    ends[s, 0:1, :] = end_re
    ends[s, 1:2, :] = end_im

    def end_copy(target, origin):
        return pltpu.make_async_remote_copy(
            src_ref=ends.at[origin],
            dst_ref=ends.at[origin],
            send_sem=end_send.at[target],
            recv_sem=end_recv.at[origin],
            device_id={"sp": target},
        )

    @pl.loop(1, n_sp)
    def _(d):
        end_copy((s + d) % n_sp, s).start()

    onward(0, 1)
    last_re, last_im = pow_real[ROWS8 - 1 :, :], pow_imag[ROWS8 - 1 :, :]
    long_re, long_im = last_re, last_im
    reach = ROWS8
    while reach < rows:
        long_re, long_im = long_re * long_re - long_im * long_im, 2.0 * long_re * long_im
        reach *= 2

    @pl.loop(1, n_sp)
    def _(d):
        end_copy((s + d) % n_sp, (s + d) % n_sp).wait_recv()

    def carry_step(j, carry):
        c_re, c_im = carry
        e_re, e_im = ends[j, 0:1, :], ends[j, 1:2, :]
        n_re = long_re * c_re - long_im * c_im + e_re
        n_im = long_re * c_im + long_im * c_re + e_im
        return jnp.where(j < s, n_re, c_re), jnp.where(j < s, n_im, c_im)

    carry = lax.fori_loop(0, n_sp - 1, carry_step, (zero, zero))

    def lift(b, carry):
        c_re, c_im = carry
        at = pl.ds(pl.multiple_of(b * ROWS8, ROWS8), ROWS8)
        p_re, p_im = pow_real[...], pow_imag[...]
        st_real[at, :] = st_real[at, :] + p_re * c_re - p_im * c_im
        st_imag[at, :] = st_imag[at, :] + p_re * c_im + p_im * c_re
        return last_re * c_re - last_im * c_im, last_re * c_im + last_im * c_re

    lax.fori_loop(0, rows // ROWS8, lift, carry)

    @pl.loop(0, rows // own)
    def _(b):
        at = pl.ds(pl.multiple_of(b * own, own), own)
        high, small = split(st_real[at, :])
        y = mm_t(high, wide[4]) + mm_t(small, wide[4]) + mm_t(high, wide[5])
        high, small = split(st_imag[at, :])
        y = y - (mm_t(high, wide[6]) + mm_t(small, wide[6]) + mm_t(high, wide[7]))
        y = y + skip[...] * u[at, :].astype(F32)
        acts[t, at, :] = jax.nn.gelu(y).astype(BF)

    def gather_tp(buf, lane_no, between):
        def copy(slot, kind, target):
            return pltpu.make_async_remote_copy(
                src_ref=buf.at[slot],
                dst_ref=buf.at[slot],
                send_sem=ag_send.at[lane_no, kind],
                recv_sem=ag_recv.at[lane_no, kind],
                device_id={"tp": target},
            )

        sent = [copy(t, 0, q), copy(t, 1, p)]
        for item in sent:
            item.start()
        between()
        copy(q, 0, q).wait_recv()
        relayed = copy(q, 2, p)
        relayed.start()
        copy(p, 1, p).wait_recv()
        copy(far, 2, p).wait_recv()
        return sent + [relayed]

    def scatter_tp(lane_no, block, middle, between):
        def pair(index):
            return pltpu.make_async_remote_copy(
                src_ref=part.at[lane_no, (far, p)[index]],
                dst_ref=rx_pair.at[lane_no, index],
                send_sem=rs_send.at[lane_no, index],
                recv_sem=rs_recv.at[lane_no, index],
                device_id={"tp": p},
            )

        across = pltpu.make_async_remote_copy(
            src_ref=relay.at[lane_no],
            dst_ref=rx_far.at[lane_no],
            send_sem=rs_send.at[lane_no, 2],
            recv_sem=rs_recv.at[lane_no, 2],
            device_id={"tp": q},
        )
        pairs = [pair(0), pair(1)]
        block(far)
        pairs[0].start()
        block(p)
        pairs[1].start()
        block(q)
        middle()
        pairs[0].wait_recv()
        relay[lane_no] = (part[lane_no, q].astype(F32) + rx_pair[lane_no, 0].astype(F32)).astype(BF)
        across.start()
        block(t)
        between()
        pairs[1].wait_recv()
        across.wait_recv()
        return pairs + [across]

    def total(lane_no):
        near = part[lane_no, t].astype(F32) + rx_pair[lane_no, 1].astype(F32)
        return near + rx_far[lane_no].astype(F32)

    def first_forward():
        onward(1, 1)

    pending = gather_tp(acts, 0, first_forward)
    for load in loads[3:]:
        load.wait()
    n_tp = acts.shape[0]

    def mix_block(r):
        at = pl.ds(pl.multiple_of(r * own, own), own)
        value = jnp.zeros((own, value_w.shape[1]), F32)
        gated = value
        for j in range(n_tp):
            a = acts[j, at, :]
            value = value + mm(a, value_w[j * chans : (j + 1) * chans, :])
            gated = gated + mm(a, glu_w[j * chans : (j + 1) * chans, :])
        mixed = jax.nn.sigmoid(gate_in[at, :].astype(F32)) * value * jax.nn.sigmoid(gated)
        part[0, r] = mm(mixed.astype(BF), mix_w[...]).astype(BF)

    def third_forward():
        if n_sp > 2:
            onward(0, 2)

    pending += scatter_tp(0, mix_block, lambda: onward(2, 1), third_forward)
    inner[...] = residual[...].astype(F32) + total(0)
    x = inner[...]
    scale = lax.rsqrt(jnp.mean(x * x, axis=-1, keepdims=True) + EPSILON)
    normed[t] = (x * scale * gain[...]).astype(BF)

    def second_forward():
        if n_sp > 2:
            onward(1, 2)

    pending += gather_tp(normed, 1, second_forward)
    if n_sp > 2:
        onward(2, 2)

    @pl.loop(3, n_sp)
    def _(k):
        onward(0, k)
        onward(1, k)
        onward(2, k)

    arrived(0)
    arrived(1)

    @pl.loop(0, n_tp)
    def _(r):
        x = normed[r]
        hidden[r] = (jax.nn.silu(mm(x, w_gate[...])) * mm(x, w_up[...])).astype(BF)

    def col_pair(o, index):
        return pltpu.make_async_remote_copy(
            src_ref=c_part.at[o, (far, p)[index]],
            dst_ref=c_pair.at[o, index],
            send_sem=c_send.at[o, index],
            recv_sem=c_recv.at[o, index],
            device_id={"tp": p},
        )

    def col_far(o):
        return pltpu.make_async_remote_copy(
            src_ref=c_relay.at[o],
            dst_ref=c_far.at[o],
            send_sem=c_send.at[o, 2],
            recv_sem=c_recv.at[o, 2],
            device_id={"tp": q},
        )

    def column(o):
        weight = w_down.at[o]
        c_part[o, far] = mm(hidden[far], weight[...]).astype(BF)
        col_pair(o, 0).start()
        c_part[o, q] = mm(hidden[q], weight[...]).astype(BF)
        c_part[o, p] = mm(hidden[p], weight[...]).astype(BF)
        col_pair(o, 1).start()
        col_pair(o, 0).wait_recv()
        c_relay[o] = (c_part[o, q].astype(F32) + c_pair[o, 0].astype(F32)).astype(BF)
        col_far(o).start()
        c_part[o, t] = mm(hidden[t], weight[...]).astype(BF)

    column(s)

    @pl.loop(1, n_sp)
    def _(k):
        @pl.when(s >= k)
        def _():
            origin = (s + n_sp - k) % n_sp
            y_copy(0, 2, k, origin, other).wait_recv()
            column(origin)

        @pl.when(s + k < n_sp)
        def _():
            origin = (s + k) % n_sp
            y_copy(1, 2, k, origin, other).wait_recv()
            column(origin)

    for o in range(n_sp):
        col_pair(o, 1).wait_recv()
        col_far(o).wait_recv()
        near = c_part[o, t].astype(F32) + c_pair[o, 1].astype(F32)
        at = slice(o * d_loc, (o + 1) * d_loc)
        out[:, at] = (inner[:, at] + 0.5 * (near + c_far[o].astype(F32))).astype(BF)

    @pl.loop(0, n_sp)
    def _(o):
        col_pair(o, 0).wait_send()
        col_pair(o, 1).wait_send()
        col_far(o).wait_send()

    for item in pending:
        item.wait_send()

    @pl.loop(1, n_sp)
    def _(d):
        end_copy((s + d) % n_sp, s).wait_send()

    @pl.loop(1, n_sp)
    def _(k):
        for c in range(3):

            @pl.when(jnp.logical_and(has_right, s >= k - 1))
            def _():
                z_copy(0, c, k, (s + n_sp + 1 - k) % n_sp, right).wait_send()

            @pl.when(jnp.logical_and(has_left, s + k - 1 < n_sp))
            def _():
                z_copy(1, c, k, (s + k - 1) % n_sp, left).wait_send()

            @pl.when(s >= k)
            def _():
                y_copy(0, c, k, (s + n_sp - k) % n_sp, g).wait_send()

            @pl.when(s + k < n_sp)
            def _():
                y_copy(1, c, k, (s + k) % n_sp, g).wait_send()


def fused(
    residual,
    state_input,
    gate_input,
    decay_real,
    frequency,
    log_step,
    drive_real,
    drive_imag,
    read_real,
    read_imag,
    skip_gain,
    value_weight,
    glu_weight,
    mix_weight,
    norm_gain,
    mlp_gate,
    mlp_up,
    mlp_down,
):
    n_sp, n_tp = lax.axis_size("sp"), lax.axis_size("tp")
    groups, states, width = drive_real.shape
    flat, chans = groups * states, groups * width
    rows = state_input.shape[0]
    own, depth = residual.shape
    ff, d_loc = mlp_down.shape
    cols = value_weight.shape[1]
    _, _, in_real, in_imag = discretize(decay_real, frequency, log_step, drive_real, drive_imag)
    times = max(1, 128 // states)

    def tiled(x):
        return jnp.concatenate([x.reshape(chans, states)] * times, axis=1)

    step = jnp.exp(log_step)[:, None]
    counts = (lax.iota(jnp.int32, ROWS8) + 1).astype(F32)[:, None]
    pow_real, pow_imag = powers(
        (decay_real * step).reshape(1, flat), (frequency * step).reshape(1, flat), counts
    )
    vmem = pl.BlockSpec(memory_space=pltpu.VMEM)
    hbm = pl.BlockSpec(memory_space=pl.ANY)
    dma = pltpu.SemaphoreType.DMA
    return pl.pallas_call(
        functools.partial(layer_kernel, n_sp, width, states),
        out_shape=jax.ShapeDtypeStruct((own, depth), BF),
        in_specs=[vmem] * 10 + [hbm] * 3 + [vmem] + [hbm] * 3,
        out_specs=vmem,
        scratch_shapes=[
            pltpu.VMEM(value_weight.shape, BF),
            pltpu.VMEM(glu_weight.shape, BF),
            pltpu.VMEM(mix_weight.shape, BF),
            pltpu.VMEM((n_sp * mlp_gate.shape[0], ff), BF),
            pltpu.VMEM((n_sp * mlp_gate.shape[0], ff), BF),
            pltpu.VMEM((n_sp, ff, d_loc), BF),
            pltpu.VMEM((8, chans, flat), BF),
            pltpu.VMEM((rows, flat), F32),
            pltpu.VMEM((rows, flat), F32),
            pltpu.VMEM((6, ROWS8, flat), F32),
            pltpu.VMEM((n_sp, ROWS8, flat), F32),
            pltpu.VMEM((n_tp, rows, chans), BF),
            pltpu.VMEM((1, n_tp, own, depth), BF),
            pltpu.VMEM((1, 2, own, depth), BF),
            pltpu.VMEM((1, own, depth), BF),
            pltpu.VMEM((1, own, depth), BF),
            pltpu.VMEM((own, depth), F32),
            pltpu.VMEM((n_tp, own, depth), BF),
            pltpu.VMEM((n_tp, own, ff), BF),
            pltpu.VMEM((n_sp, n_tp, own, d_loc), BF),
            pltpu.VMEM((n_sp, 2, own, d_loc), BF),
            pltpu.VMEM((n_sp, own, d_loc), BF),
            pltpu.VMEM((n_sp, own, d_loc), BF),
            dma((6,)),
            dma((n_sp,)),
            dma((n_sp,)),
            dma((2, 3, n_sp)),
            dma((2, 3, n_sp)),
            dma((2, 3, n_sp)),
            dma((2, 3, n_sp)),
            dma((2, 3)),
            dma((2, 3)),
            dma((1, 3)),
            dma((1, 3)),
            dma((n_sp, 3)),
            dma((n_sp, 3)),
        ],
        compiler_params=pltpu.CompilerParams(
            collective_id=0, has_side_effects=True, vmem_limit_bytes=60 * 1024 * 1024
        ),
    )(
        residual,
        state_input,
        gate_input,
        pow_real,
        pow_imag,
        tiled(in_real.transpose(0, 2, 1)),
        tiled(in_imag.transpose(0, 2, 1)),
        tiled(read_real),
        tiled(read_imag),
        skip_gain[None, :],
        value_weight,
        glu_weight,
        mix_weight,
        norm_gain[None, :],
        mlp_gate,
        mlp_up,
        mlp_down,
    )


def quick_kernel(
    n_sp,
    width,
    states,
    residual_h,
    u_h,
    gate_in_h,
    decay_h,
    freq_h,
    step_h,
    drive_re_h,
    drive_im_h,
    read_re_h,
    read_im_h,
    skip_h,
    value_h,
    glu_h,
    mix_h,
    gain_h,
    gate_h,
    up_h,
    down_h,
    out,
    residual,
    u,
    gate_in,
    decay,
    freq,
    log_step,
    drive_re,
    drive_im,
    read_re,
    read_im,
    skip,
    value_w,
    glu_w,
    mix_w,
    gain,
    w_gate,
    w_up,
    w_down,
    wide,
    pow_real,
    pow_imag,
    ratio,
    st_real,
    st_imag,
    masked,
    ends,
    acts,
    part,
    rx_pair,
    relay,
    rx_far,
    inner,
    normed,
    hidden,
    c_part,
    c_in,
    c_relay,
    guest,
    g_hidden,
    g_out,
    g_in,
    load_sem,
    end_send,
    end_recv,
    z_send,
    z_recv,
    y_send,
    y_recv,
    y_late,
    z_more,
    g_send,
    g_recv,
    b_send,
    b_recv,
    ag_send,
    ag_recv,
    rs_send,
    rs_recv,
    c_send,
    c_recv,
):
    g, s, t = lax.axis_index("grp"), lax.axis_index("sp"), lax.axis_index("tp")
    low, high_bit = t % 2, t // 2
    p = t + 1 - 2 * low
    q = t + 2 - 4 * high_bit
    far = 3 - t
    other = 1 - g
    rows, chans = u.shape
    groups, flat = decay.shape[0], st_real.shape[1]
    own, depth = residual.shape
    k_loc, ff = gate_h.shape
    d_loc = down_h.shape[1]
    n_tp = acts.shape[0]
    k_half, f_half = k_loc // 2, ff // 2
    k_piece, d_half = k_half // PIECES, d_loc // HALVES
    f_piece = f_half * HALVES // PIECES

    barrier = pltpu.get_barrier_semaphore()
    pl.semaphore_signal(barrier, inc=1, device_id={"tp": p})
    pl.semaphore_signal(barrier, inc=1, device_id={"tp": q})
    pl.semaphore_signal(barrier, inc=1, device_id={"grp": other})

    @pl.loop(1, n_sp)
    def _(d):
        pl.semaphore_signal(barrier, inc=1, device_id={"sp": (s + d) % n_sp})

    place = pl.ds(pl.multiple_of(s * k_loc, k_loc), k_loc)
    pairs_of = (
        (gate_h, w_gate.at[place, :]),
        (decay_h, decay),
        (freq_h, freq),
        (step_h, log_step),
        (drive_re_h, drive_re),
        (drive_im_h, drive_im),
        (u_h, u),
        (read_re_h, read_re),
        (read_im_h, read_im),
        (skip_h, skip),
        (up_h, w_up.at[place, :]),
        (down_h, w_down.at[s]),
        (value_h, value_w),
        (glu_h, glu_w),
        (gate_in_h, gate_in),
        (mix_h, mix_w),
        (residual_h, residual),
        (gain_h, gain),
    )
    loads = [
        pltpu.make_async_copy(a, b, load_sem.at[i]) for i, (a, b) in enumerate(pairs_of)
    ]
    for load in loads:
        load.start()
    pl.semaphore_wait(barrier, 3 + n_sp - 1)

    bufs = (w_gate, w_up, w_down)
    behind = (s, n_sp - 1 - s)
    n_early, n_late = 2 * PIECES, PIECES

    def await_bytes(sem, ref):
        pltpu.make_async_copy(ref, ref, sem).wait()

    def mine(c, i, origin, half):
        if c < 2:
            row = pl.multiple_of(origin * k_loc + half * k_half + i * k_piece, k_piece)
            return bufs[c].at[pl.ds(row, k_piece), :]
        row = pl.multiple_of(half * f_half + (i % PER) * f_piece, f_piece)
        return bufs[c].at[origin, pl.ds(row, f_piece), pl.ds((i // PER) * d_half, d_half)]

    def z_copy(side, c, i, origin):
        piece = mine(c, i, origin, g)
        return pltpu.make_async_remote_copy(
            src_ref=piece,
            dst_ref=piece,
            send_sem=z_send.at[side, c],
            recv_sem=z_recv.at[c, i, origin - side],
            device_id={"sp": ahead(side)},
        )

    def y_copy(c, i, origin, half):
        piece = mine(c, i, origin, half)
        return pltpu.make_async_remote_copy(
            src_ref=piece,
            dst_ref=piece,
            send_sem=y_send.at[c // 2],
            recv_sem=y_recv.at[0] if c < 2 else y_late.at[origin, i // (PER)],
            device_id={"grp": other},
        )

    def more_copy(side, c, i):
        piece = mine(c, i, s, other)
        return pltpu.make_async_remote_copy(
            src_ref=piece,
            dst_ref=piece,
            send_sem=z_send.at[side, c],
            recv_sem=z_more.at[0 if c < 2 else 1 + i // PER],
            device_id={"sp": ahead(side)},
        )

    def ahead(side):
        return (s + 1) % n_sp if side == 0 else (s + n_sp - 1) % n_sp

    def source(side, k):
        return (s + n_sp - k) % n_sp if side == 0 else (s + k) % n_sp

    def own_sends(side, c, pieces):
        for i in pieces:
            z_copy(side, c, i, s).start()

    def end_sends(side):
        for c in range(3):
            if c == 2:
                own_sends(side, 2, range(PIECES))
            else:
                for i in range(PIECES):
                    more_copy(side, c, i).start()

    inner_one = jnp.logical_or(behind[0] == 1, behind[1] == 1)
    end_one = jnp.logical_not(inner_one)
    mate = s + 1 - 2 * (s % 2)
    taken = (1 - s // (n_sp // 2)) * (n_sp - 1)
    e_rows = own // 2

    def guest_copy(h):
        rows_of = pl.ds(h * e_rows, e_rows)
        return pltpu.make_async_remote_copy(
            src_ref=normed.at[t, rows_of, :],
            dst_ref=guest.at[t, rows_of, :],
            send_sem=g_send.at[0],
            recv_sem=g_recv.at[0, h],
            device_id={"sp": mate},
        )

    def guest_tp(h, slot, kind, target):
        piece = guest.at[slot, pl.ds(h * e_rows, e_rows), :]
        return pltpu.make_async_remote_copy(
            src_ref=piece,
            dst_ref=piece,
            send_sem=g_send.at[(2, 0, 1)[kind]],
            recv_sem=g_recv.at[1 + kind, h],
            device_id={"tp": target},
        )

    guest_cross = pltpu.make_async_remote_copy(
        src_ref=normed.at[q, pl.ds(e_rows, e_rows), :],
        dst_ref=guest.at[q, pl.ds(e_rows, e_rows), :],
        send_sem=g_send.at[2],
        recv_sem=g_recv.at[1, 1],
        device_id={"sp": mate},
    )

    def guest_take(h):
        guest_copy(h).wait_recv()
        if h == 0:
            guest_tp(h, t, 0, q).start()
        guest_tp(h, t, 1, p).start()

    def guest_relay(h):
        guest_tp(h, q, 0, q).wait_recv()
        guest_tp(h, q, 2, p).start()

    def own_early(c, pieces):
        for side in range(2):
            pl.when(behind[side] < n_sp - 1)(functools.partial(own_sends, side, c, pieces))

    def shared(side, k):
        return behind[side] > 1 if k == 1 else behind[side] >= k

    def onward(side, k, c, i, last):
        @pl.when(behind[side] < n_sp - 1)
        def _():
            z_copy(side, c, i, source(side, k)).start()

        if last:

            @pl.when(jnp.logical_and(behind[side] == k, k < n_sp - 1))
            def _():
                own_sends(side, 2, range(PIECES))

    def pass_on(side, k, c, i, last, hold):
        origin = source(side, k)
        z_copy(side, c, i, origin).wait_recv()
        if not hold:
            onward(side, k, c, i, last)

        @pl.when(shared(side, k))
        def _():
            y_copy(c, i, origin, g).start()

    def advance(*slots, hold=False):
        for n in slots:
            for side in range(2):
                if n < n_early * (n_sp - 1):
                    k, c, i = n // n_early + 1, n % n_early // PIECES, n % PIECES
                    last = n % n_early == n_early - 1
                    work = functools.partial(pass_on, side, k, c, i, last, hold)
                    pl.when(behind[side] >= k)(work)
                for b in range(1, n_sp):
                    m = n - n_early * max(b, 2)
                    k = m // n_late + 1
                    if 0 <= m and k <= min(b, n_sp - 2):
                        stop = k == b == n_sp - 2
                        work = functools.partial(pass_on, side, k, 2, m % n_late, False, stop)
                        pl.when(behind[side] == b)(work)

    loads[0].wait()
    own_early(0, range(PIECES))

    for load in loads[1:4]:
        load.wait()
    eye = lax.broadcasted_iota(jnp.int32, (groups, groups), 0) == lax.broadcasted_iota(
        jnp.int32, (groups, groups), 1
    )
    step = jnp.exp(jnp.sum(jnp.where(eye, log_step[...], 0.0), axis=1, keepdims=True))
    rate, turn = decay[...], freq[...]
    magnitude = jnp.exp(rate * step)
    bar_re = magnitude * jnp.cos(turn * step)
    bar_im = magnitude * jnp.sin(turn * step)
    modulus = rate * rate + turn * turn
    ratio_re = ((bar_re - 1.0) * rate + bar_im * turn) / modulus
    ratio_im = (bar_im * rate - (bar_re - 1.0) * turn) / modulus
    tiles = max(1, 128 // states)
    lanes = tiles * states
    part_of = lax.broadcasted_iota(jnp.int32, (1, lanes), 1) // states

    def spread(target, row, value):
        doubled = jnp.concatenate([value] * tiles, axis=1)
        for tile in range(groups // tiles):
            line = doubled[tile * tiles : tile * tiles + 1, :]
            for j in range(1, tiles):
                line = jnp.where(part_of == j, doubled[tile * tiles + j : tile * tiles + j + 1, :], line)
            target[row : row + 1, tile * lanes : (tile + 1) * lanes] = line

    spread(ratio, 0, ratio_re)
    spread(ratio, 1, ratio_im)
    up_re, up_im = bar_re, bar_im
    for n in range(ROWS8):
        spread(pow_real, n, up_re)
        spread(pow_imag, n, up_im)
        up_re, up_im = up_re * bar_re - up_im * bar_im, up_re * bar_im + up_im * bar_re

    for load in loads[4:9]:
        load.wait()
    row_group = lax.broadcasted_iota(jnp.int32, (chans, lanes), 0) // width
    lane = lax.broadcasted_iota(jnp.int32, (chans, lanes), 1)
    for i, ref in enumerate((drive_re, drive_im, read_re, read_im)):
        value = jnp.concatenate([ref[...]] * tiles, axis=1)
        for tile in range(flat // lanes):
            kept = jnp.where(row_group == (lane + tile * lanes) // states, value, 0.0)
            at = slice(tile * lanes, (tile + 1) * lanes)
            for j, piece in enumerate(split(kept)):
                wide[2 * i + j, :, at] = piece

    @pl.loop(0, rows // own)
    def _(b):
        at = pl.ds(pl.multiple_of(b * own, own), own)
        x = u[at, :]
        push_re = mm(x, wide[0]) + mm(x, wide[1])
        push_im = mm(x, wide[2]) + mm(x, wide[3])
        st_real[at, :] = ratio[0:1, :] * push_re - ratio[1:2, :] * push_im
        st_imag[at, :] = ratio[0:1, :] * push_im + ratio[1:2, :] * push_re

    sub = lax.broadcasted_iota(jnp.int32, (ROWS8, flat), 0)
    for i, reach in enumerate((1, 2, 4)):
        masked[2 * i] = jnp.where(sub >= reach, pow_real[reach - 1 : reach, :], 0.0)
        masked[2 * i + 1] = jnp.where(sub >= reach, pow_imag[reach - 1 : reach, :], 0.0)

    def scan_step(b, carry):
        c_re, c_im = carry
        at = pl.ds(pl.multiple_of(b * ROWS8, ROWS8), ROWS8)
        x_re, x_im = st_real[at, :], st_imag[at, :]
        for i, reach in enumerate((1, 2, 4)):
            m_re, m_im = pltpu.roll(x_re, reach, 0), pltpu.roll(x_im, reach, 0)
            a_re, a_im = masked[2 * i], masked[2 * i + 1]
            x_re, x_im = x_re + a_re * m_re - a_im * m_im, x_im + a_re * m_im + a_im * m_re
        p_re, p_im = pow_real[...], pow_imag[...]
        x_re, x_im = x_re + p_re * c_re - p_im * c_im, x_im + p_re * c_im + p_im * c_re
        st_real[at, :] = x_re
        st_imag[at, :] = x_im
        return x_re[ROWS8 - 1 :, :], x_im[ROWS8 - 1 :, :]

    zero = jnp.zeros((1, flat), F32)
    blocks = rows // ROWS8
    tip = lax.fori_loop(0, blocks // 2, scan_step, (zero, zero))
    advance(0, hold=True)
    end_re, end_im = lax.fori_loop(blocks // 2, blocks, scan_step, tip)
    ends[s, :, :flat] = end_re
    ends[s, :, flat:] = end_im

    def end_copy(target, origin):
        return pltpu.make_async_remote_copy(
            src_ref=ends.at[origin],
            dst_ref=ends.at[origin],
            send_sem=end_send.at[target],
            recv_sem=end_recv.at[origin],
            device_id={"sp": target},
        )

    @pl.loop(s + 1, n_sp)
    def _(later):
        end_copy(later, s).start()

    for load in loads[10:12]:
        load.wait()
    own_early(1, range(PIECES))
    for side in range(2):
        pl.when(behind[side] == 0)(functools.partial(end_sends, side))
        pl.when(behind[side] >= 1)(functools.partial(onward, side, 1, 0, 0, False))
    advance(1)
    last_re, last_im = pow_real[ROWS8 - 1 :, :], pow_imag[ROWS8 - 1 :, :]
    long_re, long_im = last_re, last_im
    reach = ROWS8
    while reach < rows:
        long_re, long_im = long_re * long_re - long_im * long_im, 2.0 * long_re * long_im
        reach *= 2

    advance(2, 3, 4)

    @pl.loop(0, s)
    def _(earlier):
        end_copy((s + 1) % n_sp, earlier).wait_recv()

    def carry_step(j, carry):
        c_re, c_im = carry
        e_re, e_im = ends[j, :, :flat], ends[j, :, flat:]
        n_re = long_re * c_re - long_im * c_im + e_re
        n_im = long_re * c_im + long_im * c_re + e_im
        return jnp.where(j < s, n_re, c_re), jnp.where(j < s, n_im, c_im)

    carry = lax.fori_loop(0, n_sp - 1, carry_step, (zero, zero))

    def lift(b, carry):
        c_re, c_im = carry
        at = pl.ds(pl.multiple_of(b * ROWS8, ROWS8), ROWS8)
        p_re, p_im = pow_real[...], pow_imag[...]
        st_real[at, :] = st_real[at, :] + p_re * c_re - p_im * c_im
        st_imag[at, :] = st_imag[at, :] + p_re * c_im + p_im * c_re
        return last_re * c_re - last_im * c_im, last_re * c_im + last_im * c_re

    carry = lax.fori_loop(0, blocks // 2, lift, carry)
    advance(5)
    lax.fori_loop(blocks // 2, blocks, lift, carry)
    loads[9].wait()

    def read_block(b):
        at = pl.ds(pl.multiple_of(b * own, own), own)
        high, small = split(st_real[at, :])
        y = mm_t(high, wide[4]) + mm_t(small, wide[4]) + mm_t(high, wide[5])
        high, small = split(st_imag[at, :])
        y = y - (mm_t(high, wide[6]) + mm_t(small, wide[6]) + mm_t(high, wide[7]))
        y = y + skip[...] * u[at, :].astype(F32)
        acts[t, at, :] = jax.nn.gelu(y).astype(BF)

    half_rows = rows // own // 2
    pl.loop(0, half_rows)(read_block)
    advance(6)
    pl.loop(half_rows, rows // own)(read_block)
    advance(7)

    def gather_tp(buf, lane_no, between, later):
        def copy(slot, kind, target):
            return pltpu.make_async_remote_copy(
                src_ref=buf.at[slot],
                dst_ref=buf.at[slot],
                send_sem=ag_send.at[lane_no, kind],
                recv_sem=ag_recv.at[lane_no, kind],
                device_id={"tp": target},
            )

        sent = [copy(t, 0, q), copy(t, 1, p)]
        for item in sent:
            item.start()
        copy(p, 1, p).wait_recv()
        between()
        copy(q, 0, q).wait_recv()
        relayed = copy(q, 2, p)
        relayed.start()
        later()
        copy(far, 2, p).wait_recv()
        return sent + [relayed]

    def rs_pair(index):
        return pltpu.make_async_remote_copy(
            src_ref=part.at[(far, p)[index]],
            dst_ref=rx_pair.at[index],
            send_sem=rs_send.at[index],
            recv_sem=rs_recv.at[index],
            device_id={"tp": p},
        )

    across = pltpu.make_async_remote_copy(
        src_ref=relay,
        dst_ref=rx_far,
        send_sem=rs_send.at[2],
        recv_sem=rs_recv.at[2],
        device_id={"tp": q},
    )

    pending = gather_tp(acts, 0, lambda: advance(8, 9), lambda: advance(10))
    for load in loads[12:]:
        load.wait()

    near_half = high_bit
    duo = n_tp // 2

    def mix_half(b):
        at = pl.ds(pl.multiple_of(b * duo * own, own), duo * own)
        value = jnp.zeros((duo * own, value_w.shape[1]), F32)
        gated = value
        for j in range(n_tp):
            a = acts[j, at, :]
            value = value + mm(a, value_w[j * chans : (j + 1) * chans, :])
            gated = gated + mm(a, glu_w[j * chans : (j + 1) * chans, :])
        mixed = jax.nn.sigmoid(gate_in[at, :].astype(F32)) * value * jax.nn.sigmoid(gated)
        product = mm(mixed.astype(BF), mix_w[...]).astype(BF)
        part[pl.ds(b * duo, duo)] = product.reshape(duo, own, depth)

    mix_half(1 - near_half)
    rs_pair(0).start()
    advance(11, 12)
    rs_pair(0).wait_recv()
    relay[...] = (part[q].astype(F32) + rx_pair[0].astype(F32)).astype(BF)
    across.start()
    mix_half(near_half)
    rs_pair(1).start()
    advance(13, 14, 15, 16, 17)
    rs_pair(1).wait_recv()
    across.wait_recv()
    pending += [rs_pair(0), rs_pair(1), across]
    near = part[t].astype(F32) + rx_pair[1].astype(F32)
    x = residual[...].astype(F32) + (near + rx_far[...].astype(F32))
    inner[...] = x
    scale = lax.rsqrt(jnp.mean(x * x, axis=-1, keepdims=True) + EPSILON)
    normed[t] = (x * scale * gain[...]).astype(BF)


    @pl.when(end_one)
    def _():
        for h in range(2):
            guest_copy(h).start()

    def gated_half(rows_in, rows_out, b):
        x = rows_in[pl.ds(b * duo, duo)].reshape(duo * own, depth)
        both = (jax.nn.silu(mm(x, w_gate[...])) * mm(x, w_up[...])).astype(BF)
        rows_out[pl.ds(b * duo, duo)] = both.reshape(duo, own, ff)

    def inner_first():
        await_bytes(z_more.at[0], w_gate.at[:k_loc, :])
        await_bytes(y_recv.at[0], w_gate.at[: (n_sp - 2) * k_loc, :])
        gated_half(normed, hidden, near_half)

    def while_gathering():
        advance(18, 19)
        pl.when(inner_one)(inner_first)
        advance(20, 21, 22)
        pl.when(inner_one)(lambda: guest_take(0))
        advance(23)

    pending += gather_tp(normed, 1, while_gathering, lambda: None)

    advance(24)

    @pl.when(end_one)
    def _():
        guest_cross.start()
        for side in range(2):

            @pl.when(behind[side] == 0)
            def _():
                for i in range(PIECES):
                    more_copy(side, 2, i).start()

    @pl.when(inner_one)
    def _():
        guest_take(1)
        gated_half(normed, hidden, 1 - near_half)

    advance(25)

    @pl.when(end_one)
    def _():
        await_bytes(y_recv.at[0], w_gate.at[: (n_sp - 1) * k_loc, :])

    advance(26)
    pl.when(end_one)(lambda: gated_half(normed, hidden, near_half))
    advance(27)
    pl.when(end_one)(lambda: gated_half(normed, hidden, 1 - near_half))
    advance(28)

    def col_pair(o, h, index):
        return pltpu.make_async_remote_copy(
            src_ref=c_part.at[o, h, (far, p)[index]],
            dst_ref=c_in.at[o, h, index],
            send_sem=c_send.at[0],
            recv_sem=c_recv.at[o, h if index == 0 else HALVES],
            device_id={"tp": p},
        )

    def col_far(o, h):
        return pltpu.make_async_remote_copy(
            src_ref=c_relay.at[o, h],
            dst_ref=c_in.at[o, h, 2],
            send_sem=c_send.at[0],
            recv_sem=c_recv.at[o, HALVES],
            device_id={"tp": q},
        )

    def column(o, h, rows_in=hidden, slot=None):
        slot = o if slot is None else slot
        weight = w_down.at[o, :, h * d_half : (h + 1) * d_half]
        product = mm(rows_in[...].reshape(n_tp * own, ff), weight[...]).astype(BF)
        c_part[slot, h] = product.reshape(n_tp, own, d_half)
        for index in range(2):
            col_pair(slot, h, index).start()

    def relay_on(o, h):
        col_pair(o, h, 0).wait_recv()
        both = c_part[o, h, q].astype(F32) + c_in[o, h, 0].astype(F32)
        c_relay[o, h] = both.astype(BF)
        col_far(o, h).start()

    def total(o, h):
        near = c_part[o, h, t].astype(F32) + c_in[o, h, 1].astype(F32)
        return near + c_in[o, h, 2].astype(F32)

    def put(o, h, value):
        at = pl.ds(pl.multiple_of(o * d_loc + h * d_half, d_half), d_half)
        out[:, at] = (inner[:, at] + 0.5 * value).astype(BF)

    def back_copy(h):
        return pltpu.make_async_remote_copy(
            src_ref=g_out.at[h],
            dst_ref=g_in.at[h],
            send_sem=b_send.at[0],
            recv_sem=b_recv.at[h],
            device_id={"sp": mate},
        )

    def settle(o):
        await_bytes(c_recv.at[o, HALVES], c_in.at[o, :, 1:3])
        for h in range(HALVES):
            put(o, h, total(o, h))

    def both_sides(k, work):
        for side in range(2):
            pl.when(behind[side] >= k)(functools.partial(work, side, k))

    def land(h, side, k):
        origin = source(side, k)
        row = pl.multiple_of(other * f_half, f_half)
        came = w_down.at[origin, pl.ds(row, f_half), h * d_half : (h + 1) * d_half]

        @pl.when(shared(side, k))
        def _():
            await_bytes(y_late.at[origin, h], came)

        if k == 1:

            @pl.when(behind[side] == 1)
            def _():
                await_bytes(z_more.at[1 + h], came)

    def next_column(h, side, k):
        land(h, side, k)
        column(source(side, k), h)

    def next_settle(side, k):
        settle(source(side, k))

    def next_relay(h, side, k):
        relay_on(source(side, k), h)

    def columns(k, *parts):
        for h in parts:
            both_sides(k, functools.partial(next_column, h))

    def relays(k, *parts):
        for h in parts:
            both_sides(k, functools.partial(next_relay, h))

    def far_side(work):
        for h in range(HALVES):
            for side in range(2):
                pl.when(behind[side] > 1)(functools.partial(work, h, side, 1))

    def end_side(work):
        for h in range(HALVES):
            for side in range(2):
                pl.when(behind[side] == 1)(functools.partial(work, h, side, 1))

    def sends_done():
        for item in pending:
            item.wait_send()

        @pl.loop(s + 1, n_sp)
        def _(later):
            end_copy(later, s).wait_send()

        def sent(side, b):
            for c, count in ((0, max(2, b + 1)), (1, max(2, b + 1)), (2, max(2, min(b + 1, n_sp - 2)))):
                await_bytes(z_send.at[side, c], w_gate.at[: count * k_half, :])

        for side in range(2):
            for b in range(n_sp - 1):
                pl.when(behind[side] == b)(functools.partial(sent, side, b))
        await_bytes(y_send.at[1], w_gate.at[: (n_sp - 2) * k_half, :])
        await_bytes(g_send.at[0], normed.at[0])
        await_bytes(g_send.at[2], normed.at[0, :e_rows, :])

    @pl.when(end_one)
    def _():
        for h in range(HALVES):
            column(s, h)
        for h in range(HALVES):
            relay_on(s, h)
        advance(29)
        columns(1, 0)
        relays(1, 0)
        advance(30)
        columns(1, 1)
        relays(1, 1)
        advance(31)
        settle(s)
        columns(2, 0)
        relays(2, 0)
        both_sides(1, next_settle)
        sends_done()
        await_bytes(y_send.at[0], w_gate.at[: (n_sp - 1) * k_loc, :])
        columns(2, 1)
        relays(2, 1)
        both_sides(2, next_settle)
        for h in range(HALVES):
            back_copy(h).wait_recv()
            put(taken, h, g_in[h].astype(F32))
        await_bytes(c_send.at[0], c_in.at[: n_sp - 1])

    @pl.when(inner_one)
    def _():
        guest_relay(0)
        for h in range(HALVES):
            column(s, h)
        far_side(next_column)
        for h in range(HALVES):
            relay_on(s, h)
        far_side(next_relay)
        for h in range(2):
            guest_tp(h, p, 1, p).wait_recv()
        gated_half(guest, g_hidden, near_half)
        guest_relay(1)
        for h in range(2):
            guest_tp(h, far, 2, p).wait_recv()
        gated_half(guest, g_hidden, 1 - near_half)
        for h in range(HALVES):
            both_sides(2, functools.partial(land, h))
        for h in range(HALVES):
            column(taken, h, g_hidden, n_sp)
        for h in range(HALVES):
            relay_on(n_sp, h)
        end_side(next_column)
        end_side(next_relay)
        await_bytes(c_recv.at[n_sp, HALVES], c_in.at[n_sp, :, 1:3])
        for h in range(HALVES):
            g_out[h] = total(n_sp, h).astype(BF)
            back_copy(h).start()
        for h in range(HALVES):
            column(taken, h)
        for h in range(HALVES):
            relay_on(taken, h)
        settle(s)
        both_sides(1, next_settle)
        sends_done()
        await_bytes(y_send.at[0], w_gate.at[: (n_sp - 2) * k_loc, :])
        await_bytes(g_send.at[1], normed.at[0])
        both_sides(2, next_settle)
        await_bytes(b_send.at[0], g_out)
        await_bytes(c_send.at[0], c_in)


def quick(
    residual,
    state_input,
    gate_input,
    decay_real,
    frequency,
    log_step,
    drive_real,
    drive_imag,
    read_real,
    read_imag,
    skip_gain,
    value_weight,
    glu_weight,
    mix_weight,
    norm_gain,
    mlp_gate,
    mlp_up,
    mlp_down,
):
    n_sp, n_tp = lax.axis_size("sp"), lax.axis_size("tp")
    groups, states, width = drive_real.shape
    flat, chans = groups * states, groups * width
    rows = state_input.shape[0]
    own, depth = residual.shape
    k_loc, ff = mlp_gate.shape
    d_loc = mlp_down.shape[1]
    d_half = d_loc // HALVES
    hbm = pl.BlockSpec(memory_space=pltpu.HBM)
    dma = pltpu.SemaphoreType.DMA
    operands = (
        residual,
        state_input,
        gate_input,
        decay_real,
        frequency,
        log_step[None, :],
        drive_real.transpose(0, 2, 1).reshape(chans, states),
        drive_imag.transpose(0, 2, 1).reshape(chans, states),
        read_real.reshape(chans, states),
        read_imag.reshape(chans, states),
        skip_gain[None, :],
        value_weight,
        glu_weight,
        mix_weight,
        norm_gain[None, :],
        mlp_gate,
        mlp_up,
        mlp_down,
    )
    return pl.pallas_call(
        functools.partial(quick_kernel, n_sp, width, states),
        out_shape=pltpu.VMEM((own, depth), BF),
        in_specs=[hbm] * len(operands),
        out_specs=pl.BlockSpec(memory_space=pltpu.VMEM),
        scratch_shapes=[pltpu.VMEM(x.shape, x.dtype) for x in operands[:15]]
        + [
            pltpu.VMEM((n_sp * k_loc, ff), BF),
            pltpu.VMEM((n_sp * k_loc, ff), BF),
            pltpu.VMEM((n_sp, ff, d_loc), BF),
            pltpu.VMEM((8, chans, flat), BF),
            pltpu.VMEM((ROWS8, flat), F32),
            pltpu.VMEM((ROWS8, flat), F32),
            pltpu.VMEM((2, flat), F32),
            pltpu.VMEM((rows, flat), F32),
            pltpu.VMEM((rows, flat), F32),
            pltpu.VMEM((6, ROWS8, flat), F32),
            pltpu.VMEM((n_sp, 1, 2 * flat), F32),
            pltpu.VMEM((n_tp, rows, chans), BF),
            pltpu.VMEM((n_tp, own, depth), BF),
            pltpu.VMEM((2, own, depth), BF),
            pltpu.VMEM((own, depth), BF),
            pltpu.VMEM((own, depth), BF),
            pltpu.VMEM((own, depth), F32),
            pltpu.VMEM((n_tp, own, depth), BF),
            pltpu.VMEM((n_tp, own, ff), BF),
            pltpu.VMEM((n_sp + 1, HALVES, n_tp, own, d_half), BF),
            pltpu.VMEM((n_sp + 1, HALVES, 3, own, d_half), BF),
            pltpu.VMEM((n_sp + 1, HALVES, own, d_half), BF),
            pltpu.VMEM((n_tp, own, depth), BF),
            pltpu.VMEM((n_tp, own, ff), BF),
            pltpu.VMEM((HALVES, own, d_half), BF),
            pltpu.VMEM((HALVES, own, d_half), BF),
            dma((len(operands),)),
            dma((n_sp,)),
            dma((n_sp,)),
            dma((2, 3)),
            dma((3, PIECES, n_sp - 1)),
            dma((2,)),
            dma((1,)),
            dma((n_sp, HALVES)),
            dma((1 + HALVES,)),
            dma((3,)),
            dma((4, 2)),
            dma((1,)),
            dma((HALVES,)),
            dma((2, 3)),
            dma((2, 3)),
            dma((3,)),
            dma((3,)),
            dma((1,)),
            dma((n_sp + 1, HALVES + 1)),
        ],
        compiler_params=pltpu.CompilerParams(
            collective_id=0, has_side_effects=True, vmem_limit_bytes=60 * 1024 * 1024
        ),
    )(*operands)


def solution(mesh):
    placed = (
        P(("grp", "sp", "tp"), None),
        P(("grp", "sp"), "tp"),
        P(("grp", "sp"), "tp"),
        P("tp", None),
        P("tp", None),
        P("tp"),
        P("tp", None, None),
        P("tp", None, None),
        P("tp", None, None),
        P("tp", None, None),
        P("tp"),
        P(None, "tp"),
        P(None, "tp"),
        P("tp", None),
        P(),
        P("sp", "tp"),
        P("sp", "tp"),
        P("tp", "sp"),
    )
    body = shards
    if (mesh.shape["tp"], mesh.shape["grp"]) == (4, 2):
        body = quick if mesh.shape["sp"] == 4 else fused
    return jax.shard_map(
        body, mesh=mesh, in_specs=placed, out_specs=P(("grp", "sp", "tp"), None), check_vma=False
    )
```

```python
import functools
import jax
import jax.numpy as jnp
from jax import lax
from jax.experimental import pallas as pl
from jax.experimental.pallas import tpu as pltpu
from jax.sharding import PartitionSpec as P

BF = jnp.bfloat16
F32 = jnp.float32
ROWS8 = 8
PIECES = 4
HALVES = 2
PER = PIECES // HALVES

HIGH = lax.Precision.HIGHEST
EPSILON = 1e-06


def carried_in(value, axis, join, neutral):
    count, mine = (lax.axis_size(axis), lax.axis_index(axis))
    pieces = jax.tree.map(lambda part: lax.all_gather(part, axis), value)
    subtotal = jax.tree.map(
        lambda part, zero: jnp.full_like(part, 0) + jnp.asarray(zero, part.dtype), value, neutral
    )

    def step(position, subtotal):
        longer = join(subtotal, jax.tree.map(lambda part: part[position], pieces))
        return jax.tree.map(lambda new, old: jnp.where(position < mine, new, old), longer, subtotal)

    return lax.fori_loop(0, count - 1, step, subtotal)


def discretize(decay_real, frequency, log_step, drive_real, drive_imag):
    step = jnp.exp(log_step)[:, None]
    magnitude = jnp.exp(decay_real * step)
    turned = frequency * step
    bar_real = magnitude * jnp.cos(turned)
    bar_imag = magnitude * jnp.sin(turned)
    modulus = decay_real * decay_real + frequency * frequency
    ratio_real = ((bar_real - 1.0) * decay_real + bar_imag * frequency) / modulus
    ratio_imag = (bar_imag * decay_real - (bar_real - 1.0) * frequency) / modulus
    in_real = ratio_real[..., None] * drive_real - ratio_imag[..., None] * drive_imag
    in_imag = ratio_real[..., None] * drive_imag + ratio_imag[..., None] * drive_real
    return (bar_real, bar_imag, in_real, in_imag)


def combine(earlier, later):
    real_one, imag_one, state_real_one, state_imag_one = earlier
    real_two, imag_two, state_real_two, state_imag_two = later
    return (
        real_one * real_two - imag_one * imag_two,
        real_one * imag_two + imag_one * real_two,
        real_two * state_real_one - imag_two * state_imag_one + state_real_two,
        real_two * state_imag_one + imag_two * state_real_one + state_imag_two,
    )


def powers(log_rate, angle_rate, count):
    return (
        jnp.exp(log_rate * count) * jnp.cos(angle_rate * count),
        jnp.exp(log_rate * count) * jnp.sin(angle_rate * count),
    )


def block_states(flat_inputs, decay_real, frequency, log_step, in_real, in_imag):
    rows = flat_inputs.shape[0]
    groups, states, width = in_real.shape
    flat = groups * states
    eye = jnp.eye(groups, dtype=jnp.float32)
    wide_real = jnp.einsum("gph,gk->ghkp", in_real, eye).reshape(groups * width, flat)
    wide_imag = jnp.einsum("gph,gk->ghkp", in_imag, eye).reshape(groups * width, flat)
    state_real = jnp.dot(flat_inputs, wide_real, precision=HIGH)
    state_imag = jnp.dot(flat_inputs, wide_imag, precision=HIGH)
    step = jnp.exp(log_step)[:, None]
    log_rate = (decay_real * step).reshape(1, flat)
    angle_rate = (frequency * step).reshape(1, flat)
    reach = 1
    while reach < rows:
        lift_real, lift_imag = powers(log_rate, angle_rate, float(reach))
        blank = jnp.zeros((reach, flat), jnp.float32)
        moved_real = jnp.concatenate([blank, state_real[: rows - reach]], axis=0)
        moved_imag = jnp.concatenate([blank, state_imag[: rows - reach]], axis=0)
        state_real, state_imag = (
            state_real + lift_real * moved_real - lift_imag * moved_imag,
            state_imag + lift_real * moved_imag + lift_imag * moved_real,
        )
        reach = reach * 2
    counts = (lax.iota(jnp.int32, rows) + 1).astype(jnp.float32)[:, None]
    power_real, power_imag = powers(log_rate, angle_rate, counts)
    return (power_real, power_imag, state_real, state_imag)


def readout(state_real, state_imag, read_real, read_imag, flat_inputs, skip_gain):
    groups, width, states = read_real.shape
    eye = jnp.eye(groups, dtype=jnp.float32)
    wide_real = jnp.einsum("ghp,gk->gpkh", read_real, eye).reshape(groups * states, groups * width)
    wide_imag = jnp.einsum("ghp,gk->gpkh", read_imag, eye).reshape(groups * states, groups * width)
    output = jnp.dot(state_real, wide_real, precision=HIGH) - jnp.dot(
        state_imag, wide_imag, precision=HIGH
    )
    output = output + skip_gain * flat_inputs
    return jax.nn.gelu(output).astype(jnp.bfloat16)


def normalize(inner, norm_gain):
    scale = lax.rsqrt(jnp.mean(inner * inner, axis=-1, keepdims=True) + EPSILON)
    return (inner * scale * norm_gain).astype(jnp.bfloat16)


def shards(
    residual,
    state_input,
    gate_input,
    decay_real,
    frequency,
    log_step,
    drive_real,
    drive_imag,
    read_real,
    read_imag,
    skip_gain,
    value_weight,
    glu_weight,
    mix_weight,
    norm_gain,
    mlp_gate,
    mlp_up,
    mlp_down,
):
    bar_real, bar_imag, in_real, in_imag = discretize(
        decay_real, frequency, log_step, drive_real, drive_imag
    )
    flat_inputs = state_input.astype(jnp.float32)
    power_real, power_imag, local_real, local_imag = block_states(
        flat_inputs, decay_real, frequency, log_step, in_real, in_imag
    )
    ends = (power_real[-1], power_imag[-1], local_real[-1], local_imag[-1])
    ones = jnp.ones_like(ends[0])
    zeros = jnp.zeros_like(ends[0])
    incoming = carried_in(
        (ends[0], ends[1], ends[2], ends[3]), "sp", combine, (ones, zeros, zeros, zeros)
    )
    carry_real = incoming[2]
    carry_imag = incoming[3]
    state_real = local_real + power_real * carry_real - power_imag * carry_imag
    state_imag = local_imag + power_real * carry_imag + power_imag * carry_real
    acts = readout(state_real, state_imag, read_real, read_imag, flat_inputs, skip_gain)
    piece = lax.all_gather(acts, "tp", axis=1, tiled=True)
    value = jnp.dot(piece, value_weight, preferred_element_type=jnp.float32)
    gated = jnp.dot(piece, glu_weight, preferred_element_type=jnp.float32)
    mixed = (jax.nn.sigmoid(gate_input.astype(jnp.float32)) * value * jax.nn.sigmoid(gated)).astype(
        jnp.bfloat16
    )
    branch = lax.psum_scatter(
        jnp.dot(mixed, mix_weight, preferred_element_type=jnp.float32).astype(jnp.bfloat16),
        "tp",
        scatter_dimension=0,
        tiled=True,
    ).astype(jnp.float32)
    inner = residual.astype(jnp.float32) + branch
    normed = lax.all_gather(normalize(inner, norm_gain), "tp", axis=0, tiled=True)
    hidden_gate = jnp.dot(
        normed,
        lax.all_gather(mlp_gate, "sp", axis=0, tiled=True),
        preferred_element_type=jnp.float32,
    )
    hidden_up = jnp.dot(
        normed, lax.all_gather(mlp_up, "sp", axis=0, tiled=True), preferred_element_type=jnp.float32
    )
    hidden = (jax.nn.silu(hidden_gate) * hidden_up).astype(jnp.bfloat16)
    down = jnp.dot(
        hidden,
        lax.all_gather(mlp_down, "sp", axis=1, tiled=True),
        preferred_element_type=jnp.float32,
    )
    down_own = lax.psum_scatter(
        down.astype(jnp.bfloat16), "tp", scatter_dimension=0, tiled=True
    ).astype(jnp.float32)
    return (inner + 0.5 * down_own).astype(jnp.bfloat16)


def mm(a, b):
    return jnp.dot(a, b, preferred_element_type=F32)


def mm_t(a, b):
    return lax.dot_general(a, b, (((1,), (1,)), ((), ())), preferred_element_type=F32)


def split(x):
    high = x.astype(BF)
    return high, (x - high.astype(F32)).astype(BF)


def layer_kernel(
    n_sp,
    width,
    states,
    residual,
    u,
    gate_in,
    pow_real,
    pow_imag,
    in_real,
    in_imag,
    rd_real,
    rd_imag,
    skip,
    value_h,
    glu_h,
    mix_h,
    gain,
    gate_h,
    up_h,
    down_h,
    out,
    value_w,
    glu_w,
    mix_w,
    w_gate,
    w_up,
    w_down,
    wide,
    st_real,
    st_imag,
    masked,
    ends,
    acts,
    part,
    rx_pair,
    relay,
    rx_far,
    inner,
    normed,
    hidden,
    c_part,
    c_pair,
    c_relay,
    c_far,
    load_sem,
    end_send,
    end_recv,
    z_send,
    z_recv,
    y_send,
    y_recv,
    ag_send,
    ag_recv,
    rs_send,
    rs_recv,
    c_send,
    c_recv,
):
    g, s, t = lax.axis_index("grp"), lax.axis_index("sp"), lax.axis_index("tp")
    low, high_bit = t % 2, t // 2
    p = t + 1 - 2 * low
    q = t + 2 - 4 * high_bit
    far = 3 - t
    other = 1 - g
    rows, chans = u.shape
    flat = st_real.shape[1]
    own, depth = residual.shape
    k_loc = gate_h.shape[0]
    ff, d_loc = down_h.shape
    k_half, f_half = k_loc // 2, ff // 2

    barrier = pltpu.get_barrier_semaphore()
    pl.semaphore_signal(barrier, inc=1, device_id={"tp": p})
    pl.semaphore_signal(barrier, inc=1, device_id={"tp": q})
    pl.semaphore_signal(barrier, inc=1, device_id={"grp": other})

    @pl.loop(1, n_sp)
    def _(d):
        pl.semaphore_signal(barrier, inc=1, device_id={"sp": (s + d) % n_sp})

    def mine(ref, c, origin, half):
        if c < 2:
            return ref.at[pl.ds(pl.multiple_of(origin * k_loc + half * k_half, k_half), k_half), :]
        return ref.at[origin, pl.ds(pl.multiple_of(half * f_half, f_half), f_half), :]

    bufs = (w_gate, w_up, w_down)
    place = pl.ds(pl.multiple_of(s * k_loc, k_loc), k_loc)
    loads = [
        pltpu.make_async_copy(gate_h, w_gate.at[place, :], load_sem.at[0]),
        pltpu.make_async_copy(up_h, w_up.at[place, :], load_sem.at[1]),
        pltpu.make_async_copy(down_h, w_down.at[s], load_sem.at[2]),
        pltpu.make_async_copy(value_h, value_w, load_sem.at[3]),
        pltpu.make_async_copy(glu_h, glu_w, load_sem.at[4]),
        pltpu.make_async_copy(mix_h, mix_w, load_sem.at[5]),
    ]
    for load in loads:
        load.start()
    pl.semaphore_wait(barrier, 3 + n_sp - 1)

    def z_copy(side, c, k, origin, target):
        piece = mine(bufs[c], c, origin, g)
        return pltpu.make_async_remote_copy(
            src_ref=piece,
            dst_ref=piece,
            send_sem=z_send.at[side, c, k],
            recv_sem=z_recv.at[side, c, k],
            device_id={"sp": target},
        )

    def y_copy(side, c, k, origin, half):
        piece = mine(bufs[c], c, origin, half)
        return pltpu.make_async_remote_copy(
            src_ref=piece,
            dst_ref=piece,
            send_sem=y_send.at[side, c, k],
            recv_sem=y_recv.at[side, c, k],
            device_id={"grp": other},
        )

    right, left = (s + 1) % n_sp, (s + n_sp - 1) % n_sp
    has_right, has_left = s < n_sp - 1, s > 0

    for c in range(3):
        loads[c].wait()

        @pl.when(has_right)
        def _():
            z_copy(0, c, 1, s, right).start()

        @pl.when(has_left)
        def _():
            z_copy(1, c, 1, s, left).start()

    def onward(c, k):
        @pl.when(s >= k)
        def _():
            origin = (s + n_sp - k) % n_sp
            z_copy(0, c, k, origin, right).wait_recv()

            @pl.when(has_right)
            def _():
                z_copy(0, c, k + 1, origin, right).start()

            y_copy(0, c, k, origin, g).start()

        @pl.when(s + k < n_sp)
        def _():
            origin = (s + k) % n_sp
            z_copy(1, c, k, origin, left).wait_recv()

            @pl.when(has_left)
            def _():
                z_copy(1, c, k + 1, origin, left).start()

            y_copy(1, c, k, origin, g).start()

    def arrived(c):
        @pl.loop(1, n_sp)
        def _(k):
            @pl.when(s >= k)
            def _():
                y_copy(0, c, k, (s + n_sp - k) % n_sp, other).wait_recv()

            @pl.when(s + k < n_sp)
            def _():
                y_copy(1, c, k, (s + k) % n_sp, other).wait_recv()

    lanes = in_real.shape[1]
    row_group = lax.broadcasted_iota(jnp.int32, (chans, lanes), 0) // width
    lane = lax.broadcasted_iota(jnp.int32, (chans, lanes), 1)
    for i, ref in enumerate((in_real, in_imag, rd_real, rd_imag)):
        value = ref[...]
        for tile in range(flat // lanes):
            kept = jnp.where(row_group == (lane + tile * lanes) // states, value, 0.0)
            big, small = split(kept)
            at = slice(tile * lanes, (tile + 1) * lanes)
            wide[2 * i, :, at] = big
            wide[2 * i + 1, :, at] = small

    @pl.loop(0, rows // own)
    def _(b):
        at = pl.ds(pl.multiple_of(b * own, own), own)
        x = u[at, :]
        st_real[at, :] = mm(x, wide[0]) + mm(x, wide[1])
        st_imag[at, :] = mm(x, wide[2]) + mm(x, wide[3])

    sub = lax.broadcasted_iota(jnp.int32, (ROWS8, flat), 0)
    for i, reach in enumerate((1, 2, 4)):
        masked[2 * i] = jnp.where(sub >= reach, pow_real[reach - 1 : reach, :], 0.0)
        masked[2 * i + 1] = jnp.where(sub >= reach, pow_imag[reach - 1 : reach, :], 0.0)

    def scan_step(b, carry):
        c_re, c_im = carry
        at = pl.ds(pl.multiple_of(b * ROWS8, ROWS8), ROWS8)
        x_re, x_im = st_real[at, :], st_imag[at, :]
        for i, reach in enumerate((1, 2, 4)):
            m_re, m_im = pltpu.roll(x_re, reach, 0), pltpu.roll(x_im, reach, 0)
            a_re, a_im = masked[2 * i], masked[2 * i + 1]
            x_re, x_im = x_re + a_re * m_re - a_im * m_im, x_im + a_re * m_im + a_im * m_re
        p_re, p_im = pow_real[...], pow_imag[...]
        x_re, x_im = x_re + p_re * c_re - p_im * c_im, x_im + p_re * c_im + p_im * c_re
        st_real[at, :] = x_re
        st_imag[at, :] = x_im
        return x_re[ROWS8 - 1 :, :], x_im[ROWS8 - 1 :, :]

    zero = jnp.zeros((1, flat), F32)
    end_re, end_im = lax.fori_loop(0, rows // ROWS8, scan_step, (zero, zero))
    ends[s, 0:1, :] = end_re
    ends[s, 1:2, :] = end_im

    def end_copy(target, origin):
        return pltpu.make_async_remote_copy(
            src_ref=ends.at[origin],
            dst_ref=ends.at[origin],
            send_sem=end_send.at[target],
            recv_sem=end_recv.at[origin],
            device_id={"sp": target},
        )

    @pl.loop(1, n_sp)
    def _(d):
        end_copy((s + d) % n_sp, s).start()

    onward(0, 1)
    last_re, last_im = pow_real[ROWS8 - 1 :, :], pow_imag[ROWS8 - 1 :, :]
    long_re, long_im = last_re, last_im
    reach = ROWS8
    while reach < rows:
        long_re, long_im = long_re * long_re - long_im * long_im, 2.0 * long_re * long_im
        reach *= 2

    @pl.loop(1, n_sp)
    def _(d):
        end_copy((s + d) % n_sp, (s + d) % n_sp).wait_recv()

    def carry_step(j, carry):
        c_re, c_im = carry
        e_re, e_im = ends[j, 0:1, :], ends[j, 1:2, :]
        n_re = long_re * c_re - long_im * c_im + e_re
        n_im = long_re * c_im + long_im * c_re + e_im
        return jnp.where(j < s, n_re, c_re), jnp.where(j < s, n_im, c_im)

    carry = lax.fori_loop(0, n_sp - 1, carry_step, (zero, zero))

    def lift(b, carry):
        c_re, c_im = carry
        at = pl.ds(pl.multiple_of(b * ROWS8, ROWS8), ROWS8)
        p_re, p_im = pow_real[...], pow_imag[...]
        st_real[at, :] = st_real[at, :] + p_re * c_re - p_im * c_im
        st_imag[at, :] = st_imag[at, :] + p_re * c_im + p_im * c_re
        return last_re * c_re - last_im * c_im, last_re * c_im + last_im * c_re

    lax.fori_loop(0, rows // ROWS8, lift, carry)

    @pl.loop(0, rows // own)
    def _(b):
        at = pl.ds(pl.multiple_of(b * own, own), own)
        high, small = split(st_real[at, :])
        y = mm_t(high, wide[4]) + mm_t(small, wide[4]) + mm_t(high, wide[5])
        high, small = split(st_imag[at, :])
        y = y - (mm_t(high, wide[6]) + mm_t(small, wide[6]) + mm_t(high, wide[7]))
        y = y + skip[...] * u[at, :].astype(F32)
        acts[t, at, :] = jax.nn.gelu(y).astype(BF)

    def gather_tp(buf, lane_no, between):
        def copy(slot, kind, target):
            return pltpu.make_async_remote_copy(
                src_ref=buf.at[slot],
                dst_ref=buf.at[slot],
                send_sem=ag_send.at[lane_no, kind],
                recv_sem=ag_recv.at[lane_no, kind],
                device_id={"tp": target},
            )

        sent = [copy(t, 0, q), copy(t, 1, p)]
        for item in sent:
            item.start()
        between()
        copy(q, 0, q).wait_recv()
        relayed = copy(q, 2, p)
        relayed.start()
        copy(p, 1, p).wait_recv()
        copy(far, 2, p).wait_recv()
        return sent + [relayed]

    def scatter_tp(lane_no, block, middle, between):
        def pair(index):
            return pltpu.make_async_remote_copy(
                src_ref=part.at[lane_no, (far, p)[index]],
                dst_ref=rx_pair.at[lane_no, index],
                send_sem=rs_send.at[lane_no, index],
                recv_sem=rs_recv.at[lane_no, index],
                device_id={"tp": p},
            )

        across = pltpu.make_async_remote_copy(
            src_ref=relay.at[lane_no],
            dst_ref=rx_far.at[lane_no],
            send_sem=rs_send.at[lane_no, 2],
            recv_sem=rs_recv.at[lane_no, 2],
            device_id={"tp": q},
        )
        pairs = [pair(0), pair(1)]
        block(far)
        pairs[0].start()
        block(p)
        pairs[1].start()
        block(q)
        middle()
        pairs[0].wait_recv()
        relay[lane_no] = (part[lane_no, q].astype(F32) + rx_pair[lane_no, 0].astype(F32)).astype(BF)
        across.start()
        block(t)
        between()
        pairs[1].wait_recv()
        across.wait_recv()
        return pairs + [across]

    def total(lane_no):
        near = part[lane_no, t].astype(F32) + rx_pair[lane_no, 1].astype(F32)
        return near + rx_far[lane_no].astype(F32)

    def first_forward():
        onward(1, 1)

    pending = gather_tp(acts, 0, first_forward)
    for load in loads[3:]:
        load.wait()
    n_tp = acts.shape[0]

    def mix_block(r):
        at = pl.ds(pl.multiple_of(r * own, own), own)
        value = jnp.zeros((own, value_w.shape[1]), F32)
        gated = value
        for j in range(n_tp):
            a = acts[j, at, :]
            value = value + mm(a, value_w[j * chans : (j + 1) * chans, :])
            gated = gated + mm(a, glu_w[j * chans : (j + 1) * chans, :])
        mixed = jax.nn.sigmoid(gate_in[at, :].astype(F32)) * value * jax.nn.sigmoid(gated)
        part[0, r] = mm(mixed.astype(BF), mix_w[...]).astype(BF)

    def third_forward():
        if n_sp > 2:
            onward(0, 2)

    pending += scatter_tp(0, mix_block, lambda: onward(2, 1), third_forward)
    inner[...] = residual[...].astype(F32) + total(0)
    x = inner[...]
    scale = lax.rsqrt(jnp.mean(x * x, axis=-1, keepdims=True) + EPSILON)
    normed[t] = (x * scale * gain[...]).astype(BF)

    def second_forward():
        if n_sp > 2:
            onward(1, 2)

    pending += gather_tp(normed, 1, second_forward)
    if n_sp > 2:
        onward(2, 2)

    @pl.loop(3, n_sp)
    def _(k):
        onward(0, k)
        onward(1, k)
        onward(2, k)

    arrived(0)
    arrived(1)

    @pl.loop(0, n_tp)
    def _(r):
        x = normed[r]
        hidden[r] = (jax.nn.silu(mm(x, w_gate[...])) * mm(x, w_up[...])).astype(BF)

    def col_pair(o, index):
        return pltpu.make_async_remote_copy(
            src_ref=c_part.at[o, (far, p)[index]],
            dst_ref=c_pair.at[o, index],
            send_sem=c_send.at[o, index],
            recv_sem=c_recv.at[o, index],
            device_id={"tp": p},
        )

    def col_far(o):
        return pltpu.make_async_remote_copy(
            src_ref=c_relay.at[o],
            dst_ref=c_far.at[o],
            send_sem=c_send.at[o, 2],
            recv_sem=c_recv.at[o, 2],
            device_id={"tp": q},
        )

    def column(o):
        weight = w_down.at[o]
        c_part[o, far] = mm(hidden[far], weight[...]).astype(BF)
        col_pair(o, 0).start()
        c_part[o, q] = mm(hidden[q], weight[...]).astype(BF)
        c_part[o, p] = mm(hidden[p], weight[...]).astype(BF)
        col_pair(o, 1).start()
        col_pair(o, 0).wait_recv()
        c_relay[o] = (c_part[o, q].astype(F32) + c_pair[o, 0].astype(F32)).astype(BF)
        col_far(o).start()
        c_part[o, t] = mm(hidden[t], weight[...]).astype(BF)

    column(s)

    @pl.loop(1, n_sp)
    def _(k):
        @pl.when(s >= k)
        def _():
            origin = (s + n_sp - k) % n_sp
            y_copy(0, 2, k, origin, other).wait_recv()
            column(origin)

        @pl.when(s + k < n_sp)
        def _():
            origin = (s + k) % n_sp
            y_copy(1, 2, k, origin, other).wait_recv()
            column(origin)

    for o in range(n_sp):
        col_pair(o, 1).wait_recv()
        col_far(o).wait_recv()
        near = c_part[o, t].astype(F32) + c_pair[o, 1].astype(F32)
        at = slice(o * d_loc, (o + 1) * d_loc)
        out[:, at] = (inner[:, at] + 0.5 * (near + c_far[o].astype(F32))).astype(BF)

    @pl.loop(0, n_sp)
    def _(o):
        col_pair(o, 0).wait_send()
        col_pair(o, 1).wait_send()
        col_far(o).wait_send()

    for item in pending:
        item.wait_send()

    @pl.loop(1, n_sp)
    def _(d):
        end_copy((s + d) % n_sp, s).wait_send()

    @pl.loop(1, n_sp)
    def _(k):
        for c in range(3):

            @pl.when(jnp.logical_and(has_right, s >= k - 1))
            def _():
                z_copy(0, c, k, (s + n_sp + 1 - k) % n_sp, right).wait_send()

            @pl.when(jnp.logical_and(has_left, s + k - 1 < n_sp))
            def _():
                z_copy(1, c, k, (s + k - 1) % n_sp, left).wait_send()

            @pl.when(s >= k)
            def _():
                y_copy(0, c, k, (s + n_sp - k) % n_sp, g).wait_send()

            @pl.when(s + k < n_sp)
            def _():
                y_copy(1, c, k, (s + k) % n_sp, g).wait_send()


def fused(
    residual,
    state_input,
    gate_input,
    decay_real,
    frequency,
    log_step,
    drive_real,
    drive_imag,
    read_real,
    read_imag,
    skip_gain,
    value_weight,
    glu_weight,
    mix_weight,
    norm_gain,
    mlp_gate,
    mlp_up,
    mlp_down,
):
    n_sp, n_tp = lax.axis_size("sp"), lax.axis_size("tp")
    groups, states, width = drive_real.shape
    flat, chans = groups * states, groups * width
    rows = state_input.shape[0]
    own, depth = residual.shape
    ff, d_loc = mlp_down.shape
    cols = value_weight.shape[1]
    _, _, in_real, in_imag = discretize(decay_real, frequency, log_step, drive_real, drive_imag)
    times = max(1, 128 // states)

    def tiled(x):
        return jnp.concatenate([x.reshape(chans, states)] * times, axis=1)

    step = jnp.exp(log_step)[:, None]
    counts = (lax.iota(jnp.int32, ROWS8) + 1).astype(F32)[:, None]
    pow_real, pow_imag = powers(
        (decay_real * step).reshape(1, flat), (frequency * step).reshape(1, flat), counts
    )
    vmem = pl.BlockSpec(memory_space=pltpu.VMEM)
    hbm = pl.BlockSpec(memory_space=pl.ANY)
    dma = pltpu.SemaphoreType.DMA
    return pl.pallas_call(
        functools.partial(layer_kernel, n_sp, width, states),
        out_shape=jax.ShapeDtypeStruct((own, depth), BF),
        in_specs=[vmem] * 10 + [hbm] * 3 + [vmem] + [hbm] * 3,
        out_specs=vmem,
        scratch_shapes=[
            pltpu.VMEM(value_weight.shape, BF),
            pltpu.VMEM(glu_weight.shape, BF),
            pltpu.VMEM(mix_weight.shape, BF),
            pltpu.VMEM((n_sp * mlp_gate.shape[0], ff), BF),
            pltpu.VMEM((n_sp * mlp_gate.shape[0], ff), BF),
            pltpu.VMEM((n_sp, ff, d_loc), BF),
            pltpu.VMEM((8, chans, flat), BF),
            pltpu.VMEM((rows, flat), F32),
            pltpu.VMEM((rows, flat), F32),
            pltpu.VMEM((6, ROWS8, flat), F32),
            pltpu.VMEM((n_sp, ROWS8, flat), F32),
            pltpu.VMEM((n_tp, rows, chans), BF),
            pltpu.VMEM((1, n_tp, own, depth), BF),
            pltpu.VMEM((1, 2, own, depth), BF),
            pltpu.VMEM((1, own, depth), BF),
            pltpu.VMEM((1, own, depth), BF),
            pltpu.VMEM((own, depth), F32),
            pltpu.VMEM((n_tp, own, depth), BF),
            pltpu.VMEM((n_tp, own, ff), BF),
            pltpu.VMEM((n_sp, n_tp, own, d_loc), BF),
            pltpu.VMEM((n_sp, 2, own, d_loc), BF),
            pltpu.VMEM((n_sp, own, d_loc), BF),
            pltpu.VMEM((n_sp, own, d_loc), BF),
            dma((6,)),
            dma((n_sp,)),
            dma((n_sp,)),
            dma((2, 3, n_sp)),
            dma((2, 3, n_sp)),
            dma((2, 3, n_sp)),
            dma((2, 3, n_sp)),
            dma((2, 3)),
            dma((2, 3)),
            dma((1, 3)),
            dma((1, 3)),
            dma((n_sp, 3)),
            dma((n_sp, 3)),
        ],
        compiler_params=pltpu.CompilerParams(
            collective_id=0, has_side_effects=True, vmem_limit_bytes=60 * 1024 * 1024
        ),
    )(
        residual,
        state_input,
        gate_input,
        pow_real,
        pow_imag,
        tiled(in_real.transpose(0, 2, 1)),
        tiled(in_imag.transpose(0, 2, 1)),
        tiled(read_real),
        tiled(read_imag),
        skip_gain[None, :],
        value_weight,
        glu_weight,
        mix_weight,
        norm_gain[None, :],
        mlp_gate,
        mlp_up,
        mlp_down,
    )


def quick_kernel(
    n_sp,
    width,
    states,
    residual_h,
    u_h,
    gate_in_h,
    decay_h,
    freq_h,
    step_h,
    drive_re_h,
    drive_im_h,
    read_re_h,
    read_im_h,
    skip_h,
    value_h,
    glu_h,
    mix_h,
    gain_h,
    gate_h,
    up_h,
    down_h,
    out,
    residual,
    u,
    gate_in,
    decay,
    freq,
    log_step,
    drive_re,
    drive_im,
    read_re,
    read_im,
    skip,
    value_w,
    glu_w,
    mix_w,
    gain,
    w_gate,
    w_up,
    w_down,
    wide,
    pow_real,
    pow_imag,
    ratio,
    st_real,
    st_imag,
    masked,
    ends,
    acts,
    part,
    rx_pair,
    relay,
    rx_far,
    inner,
    normed,
    hidden,
    c_part,
    c_in,
    c_relay,
    guest,
    g_hidden,
    g_out,
    g_in,
    load_sem,
    end_send,
    end_recv,
    z_send,
    z_recv,
    y_send,
    y_recv,
    y_late,
    z_more,
    z_last,
    g_send,
    g_recv,
    b_send,
    b_recv,
    ag_send,
    ag_recv,
    rs_send,
    rs_recv,
    c_send,
    c_recv,
):
    g, s, t = lax.axis_index("grp"), lax.axis_index("sp"), lax.axis_index("tp")
    low, high_bit = t % 2, t // 2
    p = t + 1 - 2 * low
    q = t + 2 - 4 * high_bit
    far = 3 - t
    other = 1 - g
    rows, chans = u.shape
    groups, flat = decay.shape[0], st_real.shape[1]
    own, depth = residual.shape
    k_loc, ff = gate_h.shape
    d_loc = down_h.shape[1]
    n_tp = acts.shape[0]
    k_half, f_half = k_loc // 2, ff // 2
    k_piece, d_half = k_half // PIECES, d_loc // HALVES
    f_cuts = [f_half * n // PER for n in range(PER + 1)]

    barrier = pltpu.get_barrier_semaphore()
    pl.semaphore_signal(barrier, inc=1, device_id={"tp": p})
    pl.semaphore_signal(barrier, inc=1, device_id={"tp": q})
    pl.semaphore_signal(barrier, inc=1, device_id={"grp": other})

    @pl.loop(1, n_sp)
    def _(d):
        pl.semaphore_signal(barrier, inc=1, device_id={"sp": (s + d) % n_sp})

    place = pl.ds(pl.multiple_of(s * k_loc, k_loc), k_loc)
    pairs_of = (
        (gate_h, w_gate.at[place, :]),
        (decay_h, decay),
        (freq_h, freq),
        (step_h, log_step),
        (drive_re_h, drive_re),
        (drive_im_h, drive_im),
        (u_h, u),
        (read_re_h, read_re),
        (read_im_h, read_im),
        (skip_h, skip),
        (up_h, w_up.at[place, :]),
        (down_h, w_down.at[s]),
        (value_h, value_w),
        (glu_h, glu_w),
        (gate_in_h, gate_in),
        (mix_h, mix_w),
        (residual_h, residual),
        (gain_h, gain),
    )
    loads = [
        pltpu.make_async_copy(a, b, load_sem.at[i]) for i, (a, b) in enumerate(pairs_of)
    ]
    for load in loads:
        load.start()
    pl.semaphore_wait(barrier, 3 + n_sp - 1)

    bufs = (w_gate, w_up, w_down)
    behind = (s, n_sp - 1 - s)
    n_early, n_late = 2 * PIECES, PIECES

    def await_bytes(sem, ref):
        pltpu.make_async_copy(ref, ref, sem).wait()

    def mine(c, i, origin, half):
        if c < 2:
            row = pl.multiple_of(origin * k_loc + half * k_half + i * k_piece, k_piece)
            return bufs[c].at[pl.ds(row, k_piece), :]
        start, stop = f_cuts[i % PER], f_cuts[i % PER + 1]
        row = pl.multiple_of(half * f_half + start, 16)
        return bufs[c].at[origin, pl.ds(row, stop - start), pl.ds((i // PER) * d_half, d_half)]

    def z_copy(side, c, i, origin):
        piece = mine(c, i, origin, g)
        return pltpu.make_async_remote_copy(
            src_ref=piece,
            dst_ref=piece,
            send_sem=z_send.at[side, c],
            recv_sem=z_recv.at[c, i, origin - side],
            device_id={"sp": ahead(side)},
        )

    def y_copy(c, i, origin, half):
        piece = mine(c, i, origin, half)
        return pltpu.make_async_remote_copy(
            src_ref=piece,
            dst_ref=piece,
            send_sem=y_send.at[c // 2],
            recv_sem=y_recv.at[0] if c < 2 else y_late.at[origin, i // (PER)],
            device_id={"grp": other},
        )

    def more_copy(side, c, i):
        piece = mine(c, i, s, other)
        return pltpu.make_async_remote_copy(
            src_ref=piece,
            dst_ref=piece,
            send_sem=z_send.at[side, c],
            recv_sem=z_more.at[0 if c < 2 else 1 + i // PER],
            device_id={"sp": ahead(side)},
        )

    def last_copy(side, k):
        piece = mine(2, PIECES - 1, source(side, k), other)
        return pltpu.make_async_remote_copy(
            src_ref=piece,
            dst_ref=piece,
            send_sem=z_send.at[side, 2],
            recv_sem=z_last.at[0],
            device_id={"sp": ahead(side)},
        )

    def last_on(side, b):
        if b > 1:
            last_copy(side, b - 1).wait_recv()
        if b < n_sp - 1:
            last_copy(side, b - 1).start()

    def last_advance(b):
        for side in range(2):
            pl.when(behind[side] == b)(functools.partial(last_on, side, b))

    def ahead(side):
        return (s + 1) % n_sp if side == 0 else (s + n_sp - 1) % n_sp

    def source(side, k):
        return (s + n_sp - k) % n_sp if side == 0 else (s + k) % n_sp

    def own_sends(side, c, pieces):
        for i in pieces:
            z_copy(side, c, i, s).start()

    def end_sends(side):
        for c in range(3):
            if c == 2:
                own_sends(side, 2, range(PIECES))
            else:
                for i in range(PIECES):
                    more_copy(side, c, i).start()

    inner_one = jnp.logical_or(behind[0] == 1, behind[1] == 1)
    end_one = jnp.logical_not(inner_one)
    mate = s + 1 - 2 * (s % 2)
    taken = (1 - s // (n_sp // 2)) * (n_sp - 1)
    e_rows = own // 2

    def guest_copy(h):
        rows_of = pl.ds(h * e_rows, e_rows)
        return pltpu.make_async_remote_copy(
            src_ref=normed.at[t, rows_of, :],
            dst_ref=guest.at[t, rows_of, :],
            send_sem=g_send.at[0],
            recv_sem=g_recv.at[0, h],
            device_id={"sp": mate},
        )

    def guest_tp(h, slot, kind, target):
        piece = guest.at[slot, pl.ds(h * e_rows, e_rows), :]
        return pltpu.make_async_remote_copy(
            src_ref=piece,
            dst_ref=piece,
            send_sem=g_send.at[(2, 0, 1)[kind]],
            recv_sem=g_recv.at[1 + kind, h],
            device_id={"tp": target},
        )

    guest_cross = pltpu.make_async_remote_copy(
        src_ref=normed.at[q, pl.ds(e_rows, e_rows), :],
        dst_ref=guest.at[q, pl.ds(e_rows, e_rows), :],
        send_sem=g_send.at[2],
        recv_sem=g_recv.at[1, 1],
        device_id={"sp": mate},
    )

    def guest_take(h):
        guest_copy(h).wait_recv()
        if h == 0:
            guest_tp(h, t, 0, q).start()
        guest_tp(h, t, 1, p).start()

    def guest_relay(h):
        guest_tp(h, q, 0, q).wait_recv()
        guest_tp(h, q, 2, p).start()

    def own_early(c, pieces):
        for side in range(2):
            pl.when(behind[side] < n_sp - 1)(functools.partial(own_sends, side, c, pieces))

    def shared(side, k):
        return behind[side] > 1 if k == 1 else behind[side] >= k

    def onward(side, k, c, i, last):
        @pl.when(behind[side] < n_sp - 1)
        def _():
            z_copy(side, c, i, source(side, k)).start()

        if last:

            @pl.when(jnp.logical_and(behind[side] == k, k < n_sp - 1))
            def _():
                own_sends(side, 2, range(PIECES))

    def pass_on(side, k, c, i, last, hold):
        origin = source(side, k)
        z_copy(side, c, i, origin).wait_recv()
        if not hold:
            onward(side, k, c, i, last)

        trade = shared(side, k)
        if c == 2 and i == PIECES - 1:
            trade = jnp.logical_and(trade, behind[side] != k + 1)

        @pl.when(trade)
        def _():
            y_copy(c, i, origin, g).start()

    def advance(*slots, hold=False):
        for n in slots:
            for side in range(2):
                if n < n_early * (n_sp - 1):
                    k, c, i = n // n_early + 1, n % n_early // PIECES, n % PIECES
                    last = n % n_early == n_early - 1
                    work = functools.partial(pass_on, side, k, c, i, last, hold)
                    pl.when(behind[side] >= k)(work)
                for b in range(1, n_sp):
                    m = n - n_early * max(b, 2)
                    k = m // n_late + 1
                    if 0 <= m and k <= min(b, n_sp - 2):
                        stop = k == b == n_sp - 2
                        work = functools.partial(pass_on, side, k, 2, m % n_late, False, stop)
                        pl.when(behind[side] == b)(work)

    loads[0].wait()
    own_early(0, range(PIECES))

    for load in loads[1:4]:
        load.wait()
    eye = lax.broadcasted_iota(jnp.int32, (groups, groups), 0) == lax.broadcasted_iota(
        jnp.int32, (groups, groups), 1
    )
    step = jnp.exp(jnp.sum(jnp.where(eye, log_step[...], 0.0), axis=1, keepdims=True))
    rate, turn = decay[...], freq[...]
    magnitude = jnp.exp(rate * step)
    bar_re = magnitude * jnp.cos(turn * step)
    bar_im = magnitude * jnp.sin(turn * step)
    modulus = rate * rate + turn * turn
    ratio_re = ((bar_re - 1.0) * rate + bar_im * turn) / modulus
    ratio_im = (bar_im * rate - (bar_re - 1.0) * turn) / modulus
    tiles = max(1, 128 // states)
    lanes = tiles * states
    part_of = lax.broadcasted_iota(jnp.int32, (1, lanes), 1) // states

    def spread(target, row, value):
        doubled = jnp.concatenate([value] * tiles, axis=1)
        for tile in range(groups // tiles):
            line = doubled[tile * tiles : tile * tiles + 1, :]
            for j in range(1, tiles):
                line = jnp.where(part_of == j, doubled[tile * tiles + j : tile * tiles + j + 1, :], line)
            target[row : row + 1, tile * lanes : (tile + 1) * lanes] = line

    spread(ratio, 0, ratio_re)
    spread(ratio, 1, ratio_im)
    up_re, up_im = bar_re, bar_im
    for n in range(ROWS8):
        spread(pow_real, n, up_re)
        spread(pow_imag, n, up_im)
        up_re, up_im = up_re * bar_re - up_im * bar_im, up_re * bar_im + up_im * bar_re

    for load in loads[4:9]:
        load.wait()
    row_group = lax.broadcasted_iota(jnp.int32, (chans, lanes), 0) // width
    lane = lax.broadcasted_iota(jnp.int32, (chans, lanes), 1)
    for i, ref in enumerate((drive_re, drive_im, read_re, read_im)):
        value = jnp.concatenate([ref[...]] * tiles, axis=1)
        for tile in range(flat // lanes):
            kept = jnp.where(row_group == (lane + tile * lanes) // states, value, 0.0)
            at = slice(tile * lanes, (tile + 1) * lanes)
            for j, piece in enumerate(split(kept)):
                wide[2 * i + j, :, at] = piece

    @pl.loop(0, rows // own)
    def _(b):
        at = pl.ds(pl.multiple_of(b * own, own), own)
        x = u[at, :]
        push_re = mm(x, wide[0]) + mm(x, wide[1])
        push_im = mm(x, wide[2]) + mm(x, wide[3])
        st_real[at, :] = ratio[0:1, :] * push_re - ratio[1:2, :] * push_im
        st_imag[at, :] = ratio[0:1, :] * push_im + ratio[1:2, :] * push_re

    sub = lax.broadcasted_iota(jnp.int32, (ROWS8, flat), 0)
    for i, reach in enumerate((1, 2, 4)):
        masked[2 * i] = jnp.where(sub >= reach, pow_real[reach - 1 : reach, :], 0.0)
        masked[2 * i + 1] = jnp.where(sub >= reach, pow_imag[reach - 1 : reach, :], 0.0)

    def scan_step(b, carry):
        c_re, c_im = carry
        at = pl.ds(pl.multiple_of(b * ROWS8, ROWS8), ROWS8)
        x_re, x_im = st_real[at, :], st_imag[at, :]
        for i, reach in enumerate((1, 2, 4)):
            m_re, m_im = pltpu.roll(x_re, reach, 0), pltpu.roll(x_im, reach, 0)
            a_re, a_im = masked[2 * i], masked[2 * i + 1]
            x_re, x_im = x_re + a_re * m_re - a_im * m_im, x_im + a_re * m_im + a_im * m_re
        p_re, p_im = pow_real[...], pow_imag[...]
        x_re, x_im = x_re + p_re * c_re - p_im * c_im, x_im + p_re * c_im + p_im * c_re
        st_real[at, :] = x_re
        st_imag[at, :] = x_im
        return x_re[ROWS8 - 1 :, :], x_im[ROWS8 - 1 :, :]

    zero = jnp.zeros((1, flat), F32)
    blocks = rows // ROWS8
    tip = lax.fori_loop(0, blocks // 2, scan_step, (zero, zero))
    advance(0, hold=True)
    end_re, end_im = lax.fori_loop(blocks // 2, blocks, scan_step, tip)
    ends[s, :, :flat] = end_re
    ends[s, :, flat:] = end_im

    def end_copy(target, origin):
        return pltpu.make_async_remote_copy(
            src_ref=ends.at[origin],
            dst_ref=ends.at[origin],
            send_sem=end_send.at[target],
            recv_sem=end_recv.at[origin],
            device_id={"sp": target},
        )

    @pl.loop(s + 1, n_sp)
    def _(later):
        end_copy(later, s).start()

    for load in loads[10:12]:
        load.wait()
    own_early(1, range(PIECES))
    for side in range(2):
        pl.when(behind[side] == 0)(functools.partial(end_sends, side))
        pl.when(behind[side] >= 1)(functools.partial(onward, side, 1, 0, 0, False))
    advance(1)
    last_re, last_im = pow_real[ROWS8 - 1 :, :], pow_imag[ROWS8 - 1 :, :]
    long_re, long_im = last_re, last_im
    reach = ROWS8
    while reach < rows:
        long_re, long_im = long_re * long_re - long_im * long_im, 2.0 * long_re * long_im
        reach *= 2

    advance(2, 3, 4)

    @pl.loop(0, s)
    def _(earlier):
        end_copy((s + 1) % n_sp, earlier).wait_recv()

    def carry_step(j, carry):
        c_re, c_im = carry
        e_re, e_im = ends[j, :, :flat], ends[j, :, flat:]
        n_re = long_re * c_re - long_im * c_im + e_re
        n_im = long_re * c_im + long_im * c_re + e_im
        return jnp.where(j < s, n_re, c_re), jnp.where(j < s, n_im, c_im)

    carry = lax.fori_loop(0, n_sp - 1, carry_step, (zero, zero))

    def lift(b, carry):
        c_re, c_im = carry
        at = pl.ds(pl.multiple_of(b * ROWS8, ROWS8), ROWS8)
        p_re, p_im = pow_real[...], pow_imag[...]
        st_real[at, :] = st_real[at, :] + p_re * c_re - p_im * c_im
        st_imag[at, :] = st_imag[at, :] + p_re * c_im + p_im * c_re
        return last_re * c_re - last_im * c_im, last_re * c_im + last_im * c_re

    carry = lax.fori_loop(0, blocks // 2, lift, carry)
    advance(5)
    lax.fori_loop(blocks // 2, blocks, lift, carry)
    loads[9].wait()

    def read_block(b):
        at = pl.ds(pl.multiple_of(b * 2 * own, own), 2 * own)
        high, small = split(st_real[at, :])
        y = mm_t(high, wide[4]) + mm_t(small, wide[4]) + mm_t(high, wide[5])
        high, small = split(st_imag[at, :])
        y = y - (mm_t(high, wide[6]) + mm_t(small, wide[6]) + mm_t(high, wide[7]))
        y = y + skip[...] * u[at, :].astype(F32)
        acts[t, at, :] = jax.nn.gelu(y).astype(BF)

    half_rows = rows // own // 4
    pl.loop(0, half_rows)(read_block)
    advance(6)
    pl.loop(half_rows, rows // own // 2)(read_block)
    advance(7)

    def gather_tp(buf, lane_no, between, later):
        def copy(slot, kind, target):
            return pltpu.make_async_remote_copy(
                src_ref=buf.at[slot],
                dst_ref=buf.at[slot],
                send_sem=ag_send.at[lane_no, kind],
                recv_sem=ag_recv.at[lane_no, kind],
                device_id={"tp": target},
            )

        sent = [copy(t, 0, q), copy(t, 1, p)]
        for item in sent:
            item.start()
        copy(p, 1, p).wait_recv()
        between()
        copy(q, 0, q).wait_recv()
        relayed = copy(q, 2, p)
        relayed.start()
        later()
        copy(far, 2, p).wait_recv()
        return sent + [relayed]

    def rs_pair(index):
        return pltpu.make_async_remote_copy(
            src_ref=part.at[(far, p)[index]],
            dst_ref=rx_pair.at[index],
            send_sem=rs_send.at[index],
            recv_sem=rs_recv.at[index],
            device_id={"tp": p},
        )

    across = pltpu.make_async_remote_copy(
        src_ref=relay,
        dst_ref=rx_far,
        send_sem=rs_send.at[2],
        recv_sem=rs_recv.at[2],
        device_id={"tp": q},
    )

    pending = gather_tp(acts, 0, lambda: advance(8, 9), lambda: advance(10))
    for load in loads[12:]:
        load.wait()

    near_half = high_bit
    duo = n_tp // 2

    def mix_half(b):
        at = pl.ds(pl.multiple_of(b * duo * own, own), duo * own)
        value = jnp.zeros((duo * own, value_w.shape[1]), F32)
        gated = value
        for j in range(n_tp):
            a = acts[j, at, :]
            value = value + mm(a, value_w[j * chans : (j + 1) * chans, :])
            gated = gated + mm(a, glu_w[j * chans : (j + 1) * chans, :])
        mixed = jax.nn.sigmoid(gate_in[at, :].astype(F32)) * value * jax.nn.sigmoid(gated)
        product = mm(mixed.astype(BF), mix_w[...]).astype(BF)
        part[pl.ds(b * duo, duo)] = product.reshape(duo, own, depth)

    mix_half(1 - near_half)
    rs_pair(0).start()
    advance(11, 12)
    rs_pair(0).wait_recv()
    relay[...] = (part[q].astype(F32) + rx_pair[0].astype(F32)).astype(BF)
    across.start()
    mix_half(near_half)
    rs_pair(1).start()
    advance(13, 14, 15, 16, 17)
    rs_pair(1).wait_recv()
    across.wait_recv()
    pending += [rs_pair(0), rs_pair(1), across]
    near = part[t].astype(F32) + rx_pair[1].astype(F32)
    x = residual[...].astype(F32) + (near + rx_far[...].astype(F32))
    inner[...] = x
    scale = lax.rsqrt(jnp.mean(x * x, axis=-1, keepdims=True) + EPSILON)
    normed[t] = (x * scale * gain[...]).astype(BF)


    @pl.when(end_one)
    def _():
        for h in range(2):
            guest_copy(h).start()

    def gated_half(rows_in, rows_out, b):
        x = rows_in[pl.ds(b * duo, duo)].reshape(duo * own, depth)
        both = (jax.nn.silu(mm(x, w_gate[...])) * mm(x, w_up[...])).astype(BF)
        rows_out[pl.ds(b * duo, duo)] = both.reshape(duo, own, ff)

    def inner_first():
        await_bytes(z_more.at[0], w_gate.at[:k_loc, :])
        await_bytes(y_recv.at[0], w_gate.at[: (n_sp - 2) * k_loc, :])
        gated_half(normed, hidden, near_half)

    def while_gathering():
        advance(18, 19)
        last_advance(1)
        pl.when(inner_one)(inner_first)
        advance(20, 21, 22)
        pl.when(inner_one)(lambda: guest_take(0))
        advance(23)

    pending += gather_tp(normed, 1, while_gathering, lambda: None)

    advance(24)

    @pl.when(end_one)
    def _():
        guest_cross.start()
        for side in range(2):

            @pl.when(behind[side] == 0)
            def _():
                for i in range(PIECES):
                    more_copy(side, 2, i).start()

    last_advance(2)

    @pl.when(inner_one)
    def _():
        guest_take(1)
        gated_half(normed, hidden, 1 - near_half)

    advance(25)

    @pl.when(end_one)
    def _():
        await_bytes(y_recv.at[0], w_gate.at[: (n_sp - 1) * k_loc, :])

    advance(26)
    pl.when(end_one)(lambda: gated_half(normed, hidden, near_half))
    advance(27)
    pl.when(end_one)(lambda: gated_half(normed, hidden, 1 - near_half))
    advance(28)

    def col_pair(o, h, index):
        return pltpu.make_async_remote_copy(
            src_ref=c_part.at[o, h, (far, p)[index]],
            dst_ref=c_in.at[o, h, index],
            send_sem=c_send.at[0],
            recv_sem=c_recv.at[o, h if index == 0 else HALVES],
            device_id={"tp": p},
        )

    def col_far(o, h):
        return pltpu.make_async_remote_copy(
            src_ref=c_relay.at[o, h],
            dst_ref=c_in.at[o, h, 2],
            send_sem=c_send.at[0],
            recv_sem=c_recv.at[o, HALVES],
            device_id={"tp": q},
        )

    def column(o, h, rows_in=hidden, slot=None):
        slot = o if slot is None else slot
        weight = w_down.at[o, :, h * d_half : (h + 1) * d_half]
        for index, b in enumerate((1 - near_half, near_half)):
            some = pl.ds(b * duo, duo)
            product = mm(rows_in[some].reshape(duo * own, ff), weight[...]).astype(BF)
            c_part[slot, h, some] = product.reshape(duo, own, d_half)
            col_pair(slot, h, index).start()

    def relay_on(o, h):
        col_pair(o, h, 0).wait_recv()
        both = c_part[o, h, q].astype(F32) + c_in[o, h, 0].astype(F32)
        c_relay[o, h] = both.astype(BF)
        col_far(o, h).start()

    def total(o, h):
        near = c_part[o, h, t].astype(F32) + c_in[o, h, 1].astype(F32)
        return near + c_in[o, h, 2].astype(F32)

    def put(o, h, value):
        at = pl.ds(pl.multiple_of(o * d_loc + h * d_half, d_half), d_half)
        out[:, at] = (inner[:, at] + 0.5 * value).astype(BF)

    def back_copy(h):
        return pltpu.make_async_remote_copy(
            src_ref=g_out.at[h],
            dst_ref=g_in.at[h],
            send_sem=b_send.at[0],
            recv_sem=b_recv.at[h],
            device_id={"sp": mate},
        )

    def settle(o):
        await_bytes(c_recv.at[o, HALVES], c_in.at[o, :, 1:3])
        for h in range(HALVES):
            put(o, h, total(o, h))

    def both_sides(k, work):
        for side in range(2):
            pl.when(behind[side] >= k)(functools.partial(work, side, k))

    def land(h, side, k):
        origin = source(side, k)
        row = pl.multiple_of(other * f_half, f_half)
        came = w_down.at[origin, pl.ds(row, f_half), h * d_half : (h + 1) * d_half]

        whole = shared(side, k)
        if h == HALVES - 1:
            whole = jnp.logical_and(whole, behind[side] != k + 1)

            @pl.when(behind[side] == k + 1)
            def _():
                await_bytes(y_late.at[origin, h], mine(2, h * PER, origin, other))

        @pl.when(whole)
        def _():
            await_bytes(y_late.at[origin, h], came)

        if k == 1:

            @pl.when(behind[side] == 1)
            def _():
                await_bytes(z_more.at[1 + h], came)

    def next_column(h, side, k):
        land(h, side, k)
        column(source(side, k), h)

    def next_settle(side, k):
        settle(source(side, k))

    def next_relay(h, side, k):
        relay_on(source(side, k), h)

    def columns(k, *parts):
        for h in parts:
            both_sides(k, functools.partial(next_column, h))

    def relays(k, *parts):
        for h in parts:
            both_sides(k, functools.partial(next_relay, h))

    def far_side(work):
        for h in range(HALVES):
            for side in range(2):
                pl.when(behind[side] > 1)(functools.partial(work, h, side, 1))

    def end_side(work):
        for h in range(HALVES):
            for side in range(2):
                pl.when(behind[side] == 1)(functools.partial(work, h, side, 1))

    def sends_done():
        for item in pending:
            item.wait_send()

        @pl.loop(s + 1, n_sp)
        def _(later):
            end_copy(later, s).wait_send()

        def sent(side, b):
            early, late = max(2, b + 1), max(2, min(b + 1, n_sp - 2))
            tail = k_piece if b > 0 else 0
            for c, size in enumerate((early * k_half, early * k_half, late * k_half + tail)):
                await_bytes(z_send.at[side, c], w_gate.at[:size, :])

        for side in range(2):
            for b in range(n_sp - 1):
                pl.when(behind[side] == b)(functools.partial(sent, side, b))
        await_bytes(y_send.at[1], w_gate.at[: (n_sp - 2) * k_half - k_piece, :])
        await_bytes(g_send.at[0], normed.at[0])
        await_bytes(g_send.at[2], normed.at[0, :e_rows, :])

    @pl.when(end_one)
    def _():
        for h in range(HALVES):
            column(s, h)
        for h in range(HALVES):
            relay_on(s, h)
        advance(29)
        columns(1, 0)
        relays(1, 0)
        advance(30)
        columns(1, 1)
        relays(1, 1)
        advance(31)
        settle(s)
        columns(2, 0)
        relays(2, 0)
        both_sides(1, next_settle)
        sends_done()
        await_bytes(y_send.at[0], w_gate.at[: (n_sp - 1) * k_loc, :])
        last_advance(n_sp - 1)
        columns(2, 1)
        relays(2, 1)
        both_sides(2, next_settle)
        for h in range(HALVES):
            back_copy(h).wait_recv()
            put(taken, h, g_in[h].astype(F32))
        await_bytes(c_send.at[0], c_in.at[: n_sp - 1])

    @pl.when(inner_one)
    def _():
        for h in range(HALVES):
            column(s, h)
        far_side(next_column)
        for h in range(HALVES):
            relay_on(s, h)
        far_side(next_relay)
        guest_relay(0)
        for h in range(2):
            guest_tp(h, p, 1, p).wait_recv()
        gated_half(guest, g_hidden, near_half)
        guest_relay(1)
        for h in range(2):
            guest_tp(h, far, 2, p).wait_recv()
        gated_half(guest, g_hidden, 1 - near_half)
        for h in range(HALVES):
            both_sides(2, functools.partial(land, h))
        for h in range(HALVES):
            column(taken, h, g_hidden, n_sp)
        for h in range(HALVES):
            relay_on(n_sp, h)
        end_side(next_column)
        for h in range(HALVES):
            column(taken, h)
        end_side(next_relay)
        for h in range(HALVES):
            relay_on(taken, h)
        await_bytes(c_recv.at[n_sp, HALVES], c_in.at[n_sp, :, 1:3])
        for h in range(HALVES):
            g_out[h] = total(n_sp, h).astype(BF)
            back_copy(h).start()
        settle(s)
        both_sides(1, next_settle)
        sends_done()
        await_bytes(y_send.at[0], w_gate.at[: (n_sp - 2) * k_loc, :])
        await_bytes(g_send.at[1], normed.at[0])
        both_sides(2, next_settle)
        await_bytes(b_send.at[0], g_out)
        await_bytes(c_send.at[0], c_in)


def quick(
    residual,
    state_input,
    gate_input,
    decay_real,
    frequency,
    log_step,
    drive_real,
    drive_imag,
    read_real,
    read_imag,
    skip_gain,
    value_weight,
    glu_weight,
    mix_weight,
    norm_gain,
    mlp_gate,
    mlp_up,
    mlp_down,
):
    n_sp, n_tp = lax.axis_size("sp"), lax.axis_size("tp")
    groups, states, width = drive_real.shape
    flat, chans = groups * states, groups * width
    rows = state_input.shape[0]
    own, depth = residual.shape
    k_loc, ff = mlp_gate.shape
    d_loc = mlp_down.shape[1]
    d_half = d_loc // HALVES
    hbm = pl.BlockSpec(memory_space=pltpu.HBM)
    dma = pltpu.SemaphoreType.DMA
    operands = (
        residual,
        state_input,
        gate_input,
        decay_real,
        frequency,
        log_step[None, :],
        drive_real.transpose(0, 2, 1).reshape(chans, states),
        drive_imag.transpose(0, 2, 1).reshape(chans, states),
        read_real.reshape(chans, states),
        read_imag.reshape(chans, states),
        skip_gain[None, :],
        value_weight,
        glu_weight,
        mix_weight,
        norm_gain[None, :],
        mlp_gate,
        mlp_up,
        mlp_down,
    )
    return pl.pallas_call(
        functools.partial(quick_kernel, n_sp, width, states),
        out_shape=pltpu.VMEM((own, depth), BF),
        in_specs=[hbm] * len(operands),
        out_specs=pl.BlockSpec(memory_space=pltpu.VMEM),
        scratch_shapes=[pltpu.VMEM(x.shape, x.dtype) for x in operands[:15]]
        + [
            pltpu.VMEM((n_sp * k_loc, ff), BF),
            pltpu.VMEM((n_sp * k_loc, ff), BF),
            pltpu.VMEM((n_sp, ff, d_loc), BF),
            pltpu.VMEM((8, chans, flat), BF),
            pltpu.VMEM((ROWS8, flat), F32),
            pltpu.VMEM((ROWS8, flat), F32),
            pltpu.VMEM((2, flat), F32),
            pltpu.VMEM((rows, flat), F32),
            pltpu.VMEM((rows, flat), F32),
            pltpu.VMEM((6, ROWS8, flat), F32),
            pltpu.VMEM((n_sp, 1, 2 * flat), F32),
            pltpu.VMEM((n_tp, rows, chans), BF),
            pltpu.VMEM((n_tp, own, depth), BF),
            pltpu.VMEM((2, own, depth), BF),
            pltpu.VMEM((own, depth), BF),
            pltpu.VMEM((own, depth), BF),
            pltpu.VMEM((own, depth), F32),
            pltpu.VMEM((n_tp, own, depth), BF),
            pltpu.VMEM((n_tp, own, ff), BF),
            pltpu.VMEM((n_sp + 1, HALVES, n_tp, own, d_half), BF),
            pltpu.VMEM((n_sp + 1, HALVES, 3, own, d_half), BF),
            pltpu.VMEM((n_sp + 1, HALVES, own, d_half), BF),
            pltpu.VMEM((n_tp, own, depth), BF),
            pltpu.VMEM((n_tp, own, ff), BF),
            pltpu.VMEM((HALVES, own, d_half), BF),
            pltpu.VMEM((HALVES, own, d_half), BF),
            dma((len(operands),)),
            dma((n_sp,)),
            dma((n_sp,)),
            dma((2, 3)),
            dma((3, PIECES, n_sp - 1)),
            dma((2,)),
            dma((1,)),
            dma((n_sp, HALVES)),
            dma((1 + HALVES,)),
            dma((1,)),
            dma((3,)),
            dma((4, 2)),
            dma((1,)),
            dma((HALVES,)),
            dma((2, 3)),
            dma((2, 3)),
            dma((3,)),
            dma((3,)),
            dma((1,)),
            dma((n_sp + 1, HALVES + 1)),
        ],
        compiler_params=pltpu.CompilerParams(
            collective_id=0, has_side_effects=True, vmem_limit_bytes=60 * 1024 * 1024
        ),
    )(*operands)


def solution(mesh):
    placed = (
        P(("grp", "sp", "tp"), None),
        P(("grp", "sp"), "tp"),
        P(("grp", "sp"), "tp"),
        P("tp", None),
        P("tp", None),
        P("tp"),
        P("tp", None, None),
        P("tp", None, None),
        P("tp", None, None),
        P("tp", None, None),
        P("tp"),
        P(None, "tp"),
        P(None, "tp"),
        P("tp", None),
        P(),
        P("sp", "tp"),
        P("sp", "tp"),
        P("tp", "sp"),
    )
    body = shards
    if (mesh.shape["tp"], mesh.shape["grp"]) == (4, 2):
        body = quick if mesh.shape["sp"] == 4 else fused
    return jax.shard_map(
        body, mesh=mesh, in_specs=placed, out_specs=P(("grp", "sp", "tp"), None), check_vma=False
    )
```

```python
import functools
import jax
import jax.numpy as jnp
from jax import lax
from jax.experimental import pallas as pl
from jax.experimental.pallas import tpu as pltpu
from jax.sharding import PartitionSpec as P

BF = jnp.bfloat16
F32 = jnp.float32
ROWS8 = 8
PIECES = 4
HALVES = 2
PER = PIECES // HALVES

HIGH = lax.Precision.HIGHEST
EPSILON = 1e-06


def carried_in(value, axis, join, neutral):
    count, mine = (lax.axis_size(axis), lax.axis_index(axis))
    pieces = jax.tree.map(lambda part: lax.all_gather(part, axis), value)
    subtotal = jax.tree.map(
        lambda part, zero: jnp.full_like(part, 0) + jnp.asarray(zero, part.dtype), value, neutral
    )

    def step(position, subtotal):
        longer = join(subtotal, jax.tree.map(lambda part: part[position], pieces))
        return jax.tree.map(lambda new, old: jnp.where(position < mine, new, old), longer, subtotal)

    return lax.fori_loop(0, count - 1, step, subtotal)


def discretize(decay_real, frequency, log_step, drive_real, drive_imag):
    step = jnp.exp(log_step)[:, None]
    magnitude = jnp.exp(decay_real * step)
    turned = frequency * step
    bar_real = magnitude * jnp.cos(turned)
    bar_imag = magnitude * jnp.sin(turned)
    modulus = decay_real * decay_real + frequency * frequency
    ratio_real = ((bar_real - 1.0) * decay_real + bar_imag * frequency) / modulus
    ratio_imag = (bar_imag * decay_real - (bar_real - 1.0) * frequency) / modulus
    in_real = ratio_real[..., None] * drive_real - ratio_imag[..., None] * drive_imag
    in_imag = ratio_real[..., None] * drive_imag + ratio_imag[..., None] * drive_real
    return (bar_real, bar_imag, in_real, in_imag)


def combine(earlier, later):
    real_one, imag_one, state_real_one, state_imag_one = earlier
    real_two, imag_two, state_real_two, state_imag_two = later
    return (
        real_one * real_two - imag_one * imag_two,
        real_one * imag_two + imag_one * real_two,
        real_two * state_real_one - imag_two * state_imag_one + state_real_two,
        real_two * state_imag_one + imag_two * state_real_one + state_imag_two,
    )


def powers(log_rate, angle_rate, count):
    return (
        jnp.exp(log_rate * count) * jnp.cos(angle_rate * count),
        jnp.exp(log_rate * count) * jnp.sin(angle_rate * count),
    )


def block_states(flat_inputs, decay_real, frequency, log_step, in_real, in_imag):
    rows = flat_inputs.shape[0]
    groups, states, width = in_real.shape
    flat = groups * states
    eye = jnp.eye(groups, dtype=jnp.float32)
    wide_real = jnp.einsum("gph,gk->ghkp", in_real, eye).reshape(groups * width, flat)
    wide_imag = jnp.einsum("gph,gk->ghkp", in_imag, eye).reshape(groups * width, flat)
    state_real = jnp.dot(flat_inputs, wide_real, precision=HIGH)
    state_imag = jnp.dot(flat_inputs, wide_imag, precision=HIGH)
    step = jnp.exp(log_step)[:, None]
    log_rate = (decay_real * step).reshape(1, flat)
    angle_rate = (frequency * step).reshape(1, flat)
    reach = 1
    while reach < rows:
        lift_real, lift_imag = powers(log_rate, angle_rate, float(reach))
        blank = jnp.zeros((reach, flat), jnp.float32)
        moved_real = jnp.concatenate([blank, state_real[: rows - reach]], axis=0)
        moved_imag = jnp.concatenate([blank, state_imag[: rows - reach]], axis=0)
        state_real, state_imag = (
            state_real + lift_real * moved_real - lift_imag * moved_imag,
            state_imag + lift_real * moved_imag + lift_imag * moved_real,
        )
        reach = reach * 2
    counts = (lax.iota(jnp.int32, rows) + 1).astype(jnp.float32)[:, None]
    power_real, power_imag = powers(log_rate, angle_rate, counts)
    return (power_real, power_imag, state_real, state_imag)


def readout(state_real, state_imag, read_real, read_imag, flat_inputs, skip_gain):
    groups, width, states = read_real.shape
    eye = jnp.eye(groups, dtype=jnp.float32)
    wide_real = jnp.einsum("ghp,gk->gpkh", read_real, eye).reshape(groups * states, groups * width)
    wide_imag = jnp.einsum("ghp,gk->gpkh", read_imag, eye).reshape(groups * states, groups * width)
    output = jnp.dot(state_real, wide_real, precision=HIGH) - jnp.dot(
        state_imag, wide_imag, precision=HIGH
    )
    output = output + skip_gain * flat_inputs
    return jax.nn.gelu(output).astype(jnp.bfloat16)


def normalize(inner, norm_gain):
    scale = lax.rsqrt(jnp.mean(inner * inner, axis=-1, keepdims=True) + EPSILON)
    return (inner * scale * norm_gain).astype(jnp.bfloat16)


def shards(
    residual,
    state_input,
    gate_input,
    decay_real,
    frequency,
    log_step,
    drive_real,
    drive_imag,
    read_real,
    read_imag,
    skip_gain,
    value_weight,
    glu_weight,
    mix_weight,
    norm_gain,
    mlp_gate,
    mlp_up,
    mlp_down,
):
    bar_real, bar_imag, in_real, in_imag = discretize(
        decay_real, frequency, log_step, drive_real, drive_imag
    )
    flat_inputs = state_input.astype(jnp.float32)
    power_real, power_imag, local_real, local_imag = block_states(
        flat_inputs, decay_real, frequency, log_step, in_real, in_imag
    )
    ends = (power_real[-1], power_imag[-1], local_real[-1], local_imag[-1])
    ones = jnp.ones_like(ends[0])
    zeros = jnp.zeros_like(ends[0])
    incoming = carried_in(
        (ends[0], ends[1], ends[2], ends[3]), "sp", combine, (ones, zeros, zeros, zeros)
    )
    carry_real = incoming[2]
    carry_imag = incoming[3]
    state_real = local_real + power_real * carry_real - power_imag * carry_imag
    state_imag = local_imag + power_real * carry_imag + power_imag * carry_real
    acts = readout(state_real, state_imag, read_real, read_imag, flat_inputs, skip_gain)
    piece = lax.all_gather(acts, "tp", axis=1, tiled=True)
    value = jnp.dot(piece, value_weight, preferred_element_type=jnp.float32)
    gated = jnp.dot(piece, glu_weight, preferred_element_type=jnp.float32)
    mixed = (jax.nn.sigmoid(gate_input.astype(jnp.float32)) * value * jax.nn.sigmoid(gated)).astype(
        jnp.bfloat16
    )
    branch = lax.psum_scatter(
        jnp.dot(mixed, mix_weight, preferred_element_type=jnp.float32).astype(jnp.bfloat16),
        "tp",
        scatter_dimension=0,
        tiled=True,
    ).astype(jnp.float32)
    inner = residual.astype(jnp.float32) + branch
    normed = lax.all_gather(normalize(inner, norm_gain), "tp", axis=0, tiled=True)
    hidden_gate = jnp.dot(
        normed,
        lax.all_gather(mlp_gate, "sp", axis=0, tiled=True),
        preferred_element_type=jnp.float32,
    )
    hidden_up = jnp.dot(
        normed, lax.all_gather(mlp_up, "sp", axis=0, tiled=True), preferred_element_type=jnp.float32
    )
    hidden = (jax.nn.silu(hidden_gate) * hidden_up).astype(jnp.bfloat16)
    down = jnp.dot(
        hidden,
        lax.all_gather(mlp_down, "sp", axis=1, tiled=True),
        preferred_element_type=jnp.float32,
    )
    down_own = lax.psum_scatter(
        down.astype(jnp.bfloat16), "tp", scatter_dimension=0, tiled=True
    ).astype(jnp.float32)
    return (inner + 0.5 * down_own).astype(jnp.bfloat16)


def mm(a, b):
    return jnp.dot(a, b, preferred_element_type=F32)


def mm_t(a, b):
    return lax.dot_general(a, b, (((1,), (1,)), ((), ())), preferred_element_type=F32)


def split(x):
    high = x.astype(BF)
    return high, (x - high.astype(F32)).astype(BF)


def layer_kernel(
    n_sp,
    width,
    states,
    residual,
    u,
    gate_in,
    pow_real,
    pow_imag,
    in_real,
    in_imag,
    rd_real,
    rd_imag,
    skip,
    value_h,
    glu_h,
    mix_h,
    gain,
    gate_h,
    up_h,
    down_h,
    out,
    value_w,
    glu_w,
    mix_w,
    w_gate,
    w_up,
    w_down,
    wide,
    st_real,
    st_imag,
    masked,
    ends,
    acts,
    part,
    rx_pair,
    relay,
    rx_far,
    inner,
    normed,
    hidden,
    c_part,
    c_pair,
    c_relay,
    c_far,
    load_sem,
    end_send,
    end_recv,
    z_send,
    z_recv,
    y_send,
    y_recv,
    ag_send,
    ag_recv,
    rs_send,
    rs_recv,
    c_send,
    c_recv,
):
    g, s, t = lax.axis_index("grp"), lax.axis_index("sp"), lax.axis_index("tp")
    low, high_bit = t % 2, t // 2
    p = t + 1 - 2 * low
    q = t + 2 - 4 * high_bit
    far = 3 - t
    other = 1 - g
    rows, chans = u.shape
    flat = st_real.shape[1]
    own, depth = residual.shape
    k_loc = gate_h.shape[0]
    ff, d_loc = down_h.shape
    k_half, f_half = k_loc // 2, ff // 2

    barrier = pltpu.get_barrier_semaphore()
    pl.semaphore_signal(barrier, inc=1, device_id={"tp": p})
    pl.semaphore_signal(barrier, inc=1, device_id={"tp": q})
    pl.semaphore_signal(barrier, inc=1, device_id={"grp": other})

    @pl.loop(1, n_sp)
    def _(d):
        pl.semaphore_signal(barrier, inc=1, device_id={"sp": (s + d) % n_sp})

    def mine(ref, c, origin, half):
        if c < 2:
            return ref.at[pl.ds(pl.multiple_of(origin * k_loc + half * k_half, k_half), k_half), :]
        return ref.at[origin, pl.ds(pl.multiple_of(half * f_half, f_half), f_half), :]

    bufs = (w_gate, w_up, w_down)
    place = pl.ds(pl.multiple_of(s * k_loc, k_loc), k_loc)
    loads = [
        pltpu.make_async_copy(gate_h, w_gate.at[place, :], load_sem.at[0]),
        pltpu.make_async_copy(up_h, w_up.at[place, :], load_sem.at[1]),
        pltpu.make_async_copy(down_h, w_down.at[s], load_sem.at[2]),
        pltpu.make_async_copy(value_h, value_w, load_sem.at[3]),
        pltpu.make_async_copy(glu_h, glu_w, load_sem.at[4]),
        pltpu.make_async_copy(mix_h, mix_w, load_sem.at[5]),
    ]
    for load in loads:
        load.start()
    pl.semaphore_wait(barrier, 3 + n_sp - 1)

    def z_copy(side, c, k, origin, target):
        piece = mine(bufs[c], c, origin, g)
        return pltpu.make_async_remote_copy(
            src_ref=piece,
            dst_ref=piece,
            send_sem=z_send.at[side, c, k],
            recv_sem=z_recv.at[side, c, k],
            device_id={"sp": target},
        )

    def y_copy(side, c, k, origin, half):
        piece = mine(bufs[c], c, origin, half)
        return pltpu.make_async_remote_copy(
            src_ref=piece,
            dst_ref=piece,
            send_sem=y_send.at[side, c, k],
            recv_sem=y_recv.at[side, c, k],
            device_id={"grp": other},
        )

    right, left = (s + 1) % n_sp, (s + n_sp - 1) % n_sp
    has_right, has_left = s < n_sp - 1, s > 0

    for c in range(3):
        loads[c].wait()

        @pl.when(has_right)
        def _():
            z_copy(0, c, 1, s, right).start()

        @pl.when(has_left)
        def _():
            z_copy(1, c, 1, s, left).start()

    def onward(c, k):
        @pl.when(s >= k)
        def _():
            origin = (s + n_sp - k) % n_sp
            z_copy(0, c, k, origin, right).wait_recv()

            @pl.when(has_right)
            def _():
                z_copy(0, c, k + 1, origin, right).start()

            y_copy(0, c, k, origin, g).start()

        @pl.when(s + k < n_sp)
        def _():
            origin = (s + k) % n_sp
            z_copy(1, c, k, origin, left).wait_recv()

            @pl.when(has_left)
            def _():
                z_copy(1, c, k + 1, origin, left).start()

            y_copy(1, c, k, origin, g).start()

    def arrived(c):
        @pl.loop(1, n_sp)
        def _(k):
            @pl.when(s >= k)
            def _():
                y_copy(0, c, k, (s + n_sp - k) % n_sp, other).wait_recv()

            @pl.when(s + k < n_sp)
            def _():
                y_copy(1, c, k, (s + k) % n_sp, other).wait_recv()

    lanes = in_real.shape[1]
    row_group = lax.broadcasted_iota(jnp.int32, (chans, lanes), 0) // width
    lane = lax.broadcasted_iota(jnp.int32, (chans, lanes), 1)
    for i, ref in enumerate((in_real, in_imag, rd_real, rd_imag)):
        value = ref[...]
        for tile in range(flat // lanes):
            kept = jnp.where(row_group == (lane + tile * lanes) // states, value, 0.0)
            big, small = split(kept)
            at = slice(tile * lanes, (tile + 1) * lanes)
            wide[2 * i, :, at] = big
            wide[2 * i + 1, :, at] = small

    @pl.loop(0, rows // own)
    def _(b):
        at = pl.ds(pl.multiple_of(b * own, own), own)
        x = u[at, :]
        st_real[at, :] = mm(x, wide[0]) + mm(x, wide[1])
        st_imag[at, :] = mm(x, wide[2]) + mm(x, wide[3])

    sub = lax.broadcasted_iota(jnp.int32, (ROWS8, flat), 0)
    for i, reach in enumerate((1, 2, 4)):
        masked[2 * i] = jnp.where(sub >= reach, pow_real[reach - 1 : reach, :], 0.0)
        masked[2 * i + 1] = jnp.where(sub >= reach, pow_imag[reach - 1 : reach, :], 0.0)

    def scan_step(b, carry):
        c_re, c_im = carry
        at = pl.ds(pl.multiple_of(b * ROWS8, ROWS8), ROWS8)
        x_re, x_im = st_real[at, :], st_imag[at, :]
        for i, reach in enumerate((1, 2, 4)):
            m_re, m_im = pltpu.roll(x_re, reach, 0), pltpu.roll(x_im, reach, 0)
            a_re, a_im = masked[2 * i], masked[2 * i + 1]
            x_re, x_im = x_re + a_re * m_re - a_im * m_im, x_im + a_re * m_im + a_im * m_re
        p_re, p_im = pow_real[...], pow_imag[...]
        x_re, x_im = x_re + p_re * c_re - p_im * c_im, x_im + p_re * c_im + p_im * c_re
        st_real[at, :] = x_re
        st_imag[at, :] = x_im
        return x_re[ROWS8 - 1 :, :], x_im[ROWS8 - 1 :, :]

    zero = jnp.zeros((1, flat), F32)
    end_re, end_im = lax.fori_loop(0, rows // ROWS8, scan_step, (zero, zero))
    ends[s, 0:1, :] = end_re
    ends[s, 1:2, :] = end_im

    def end_copy(target, origin):
        return pltpu.make_async_remote_copy(
            src_ref=ends.at[origin],
            dst_ref=ends.at[origin],
            send_sem=end_send.at[target],
            recv_sem=end_recv.at[origin],
            device_id={"sp": target},
        )

    @pl.loop(1, n_sp)
    def _(d):
        end_copy((s + d) % n_sp, s).start()

    onward(0, 1)
    last_re, last_im = pow_real[ROWS8 - 1 :, :], pow_imag[ROWS8 - 1 :, :]
    long_re, long_im = last_re, last_im
    reach = ROWS8
    while reach < rows:
        long_re, long_im = long_re * long_re - long_im * long_im, 2.0 * long_re * long_im
        reach *= 2

    @pl.loop(1, n_sp)
    def _(d):
        end_copy((s + d) % n_sp, (s + d) % n_sp).wait_recv()

    def carry_step(j, carry):
        c_re, c_im = carry
        e_re, e_im = ends[j, 0:1, :], ends[j, 1:2, :]
        n_re = long_re * c_re - long_im * c_im + e_re
        n_im = long_re * c_im + long_im * c_re + e_im
        return jnp.where(j < s, n_re, c_re), jnp.where(j < s, n_im, c_im)

    carry = lax.fori_loop(0, n_sp - 1, carry_step, (zero, zero))

    def lift(b, carry):
        c_re, c_im = carry
        at = pl.ds(pl.multiple_of(b * ROWS8, ROWS8), ROWS8)
        p_re, p_im = pow_real[...], pow_imag[...]
        st_real[at, :] = st_real[at, :] + p_re * c_re - p_im * c_im
        st_imag[at, :] = st_imag[at, :] + p_re * c_im + p_im * c_re
        return last_re * c_re - last_im * c_im, last_re * c_im + last_im * c_re

    lax.fori_loop(0, rows // ROWS8, lift, carry)

    @pl.loop(0, rows // own)
    def _(b):
        at = pl.ds(pl.multiple_of(b * own, own), own)
        high, small = split(st_real[at, :])
        y = mm_t(high, wide[4]) + mm_t(small, wide[4]) + mm_t(high, wide[5])
        high, small = split(st_imag[at, :])
        y = y - (mm_t(high, wide[6]) + mm_t(small, wide[6]) + mm_t(high, wide[7]))
        y = y + skip[...] * u[at, :].astype(F32)
        acts[t, at, :] = jax.nn.gelu(y).astype(BF)

    def gather_tp(buf, lane_no, between):
        def copy(slot, kind, target):
            return pltpu.make_async_remote_copy(
                src_ref=buf.at[slot],
                dst_ref=buf.at[slot],
                send_sem=ag_send.at[lane_no, kind],
                recv_sem=ag_recv.at[lane_no, kind],
                device_id={"tp": target},
            )

        sent = [copy(t, 0, q), copy(t, 1, p)]
        for item in sent:
            item.start()
        between()
        copy(q, 0, q).wait_recv()
        relayed = copy(q, 2, p)
        relayed.start()
        copy(p, 1, p).wait_recv()
        copy(far, 2, p).wait_recv()
        return sent + [relayed]

    def scatter_tp(lane_no, block, middle, between):
        def pair(index):
            return pltpu.make_async_remote_copy(
                src_ref=part.at[lane_no, (far, p)[index]],
                dst_ref=rx_pair.at[lane_no, index],
                send_sem=rs_send.at[lane_no, index],
                recv_sem=rs_recv.at[lane_no, index],
                device_id={"tp": p},
            )

        across = pltpu.make_async_remote_copy(
            src_ref=relay.at[lane_no],
            dst_ref=rx_far.at[lane_no],
            send_sem=rs_send.at[lane_no, 2],
            recv_sem=rs_recv.at[lane_no, 2],
            device_id={"tp": q},
        )
        pairs = [pair(0), pair(1)]
        block(far)
        pairs[0].start()
        block(p)
        pairs[1].start()
        block(q)
        middle()
        pairs[0].wait_recv()
        relay[lane_no] = (part[lane_no, q].astype(F32) + rx_pair[lane_no, 0].astype(F32)).astype(BF)
        across.start()
        block(t)
        between()
        pairs[1].wait_recv()
        across.wait_recv()
        return pairs + [across]

    def total(lane_no):
        near = part[lane_no, t].astype(F32) + rx_pair[lane_no, 1].astype(F32)
        return near + rx_far[lane_no].astype(F32)

    def first_forward():
        onward(1, 1)

    pending = gather_tp(acts, 0, first_forward)
    for load in loads[3:]:
        load.wait()
    n_tp = acts.shape[0]

    def mix_block(r):
        at = pl.ds(pl.multiple_of(r * own, own), own)
        value = jnp.zeros((own, value_w.shape[1]), F32)
        gated = value
        for j in range(n_tp):
            a = acts[j, at, :]
            value = value + mm(a, value_w[j * chans : (j + 1) * chans, :])
            gated = gated + mm(a, glu_w[j * chans : (j + 1) * chans, :])
        mixed = jax.nn.sigmoid(gate_in[at, :].astype(F32)) * value * jax.nn.sigmoid(gated)
        part[0, r] = mm(mixed.astype(BF), mix_w[...]).astype(BF)

    def third_forward():
        if n_sp > 2:
            onward(0, 2)

    pending += scatter_tp(0, mix_block, lambda: onward(2, 1), third_forward)
    inner[...] = residual[...].astype(F32) + total(0)
    x = inner[...]
    scale = lax.rsqrt(jnp.mean(x * x, axis=-1, keepdims=True) + EPSILON)
    normed[t] = (x * scale * gain[...]).astype(BF)

    def second_forward():
        if n_sp > 2:
            onward(1, 2)

    pending += gather_tp(normed, 1, second_forward)
    if n_sp > 2:
        onward(2, 2)

    @pl.loop(3, n_sp)
    def _(k):
        onward(0, k)
        onward(1, k)
        onward(2, k)

    arrived(0)
    arrived(1)

    @pl.loop(0, n_tp)
    def _(r):
        x = normed[r]
        hidden[r] = (jax.nn.silu(mm(x, w_gate[...])) * mm(x, w_up[...])).astype(BF)

    def col_pair(o, index):
        return pltpu.make_async_remote_copy(
            src_ref=c_part.at[o, (far, p)[index]],
            dst_ref=c_pair.at[o, index],
            send_sem=c_send.at[o, index],
            recv_sem=c_recv.at[o, index],
            device_id={"tp": p},
        )

    def col_far(o):
        return pltpu.make_async_remote_copy(
            src_ref=c_relay.at[o],
            dst_ref=c_far.at[o],
            send_sem=c_send.at[o, 2],
            recv_sem=c_recv.at[o, 2],
            device_id={"tp": q},
        )

    def column(o):
        weight = w_down.at[o]
        c_part[o, far] = mm(hidden[far], weight[...]).astype(BF)
        col_pair(o, 0).start()
        c_part[o, q] = mm(hidden[q], weight[...]).astype(BF)
        c_part[o, p] = mm(hidden[p], weight[...]).astype(BF)
        col_pair(o, 1).start()
        col_pair(o, 0).wait_recv()
        c_relay[o] = (c_part[o, q].astype(F32) + c_pair[o, 0].astype(F32)).astype(BF)
        col_far(o).start()
        c_part[o, t] = mm(hidden[t], weight[...]).astype(BF)

    column(s)

    @pl.loop(1, n_sp)
    def _(k):
        @pl.when(s >= k)
        def _():
            origin = (s + n_sp - k) % n_sp
            y_copy(0, 2, k, origin, other).wait_recv()
            column(origin)

        @pl.when(s + k < n_sp)
        def _():
            origin = (s + k) % n_sp
            y_copy(1, 2, k, origin, other).wait_recv()
            column(origin)

    for o in range(n_sp):
        col_pair(o, 1).wait_recv()
        col_far(o).wait_recv()
        near = c_part[o, t].astype(F32) + c_pair[o, 1].astype(F32)
        at = slice(o * d_loc, (o + 1) * d_loc)
        out[:, at] = (inner[:, at] + 0.5 * (near + c_far[o].astype(F32))).astype(BF)

    @pl.loop(0, n_sp)
    def _(o):
        col_pair(o, 0).wait_send()
        col_pair(o, 1).wait_send()
        col_far(o).wait_send()

    for item in pending:
        item.wait_send()

    @pl.loop(1, n_sp)
    def _(d):
        end_copy((s + d) % n_sp, s).wait_send()

    @pl.loop(1, n_sp)
    def _(k):
        for c in range(3):

            @pl.when(jnp.logical_and(has_right, s >= k - 1))
            def _():
                z_copy(0, c, k, (s + n_sp + 1 - k) % n_sp, right).wait_send()

            @pl.when(jnp.logical_and(has_left, s + k - 1 < n_sp))
            def _():
                z_copy(1, c, k, (s + k - 1) % n_sp, left).wait_send()

            @pl.when(s >= k)
            def _():
                y_copy(0, c, k, (s + n_sp - k) % n_sp, g).wait_send()

            @pl.when(s + k < n_sp)
            def _():
                y_copy(1, c, k, (s + k) % n_sp, g).wait_send()


def fused(
    residual,
    state_input,
    gate_input,
    decay_real,
    frequency,
    log_step,
    drive_real,
    drive_imag,
    read_real,
    read_imag,
    skip_gain,
    value_weight,
    glu_weight,
    mix_weight,
    norm_gain,
    mlp_gate,
    mlp_up,
    mlp_down,
):
    n_sp, n_tp = lax.axis_size("sp"), lax.axis_size("tp")
    groups, states, width = drive_real.shape
    flat, chans = groups * states, groups * width
    rows = state_input.shape[0]
    own, depth = residual.shape
    ff, d_loc = mlp_down.shape
    cols = value_weight.shape[1]
    _, _, in_real, in_imag = discretize(decay_real, frequency, log_step, drive_real, drive_imag)
    times = max(1, 128 // states)

    def tiled(x):
        return jnp.concatenate([x.reshape(chans, states)] * times, axis=1)

    step = jnp.exp(log_step)[:, None]
    counts = (lax.iota(jnp.int32, ROWS8) + 1).astype(F32)[:, None]
    pow_real, pow_imag = powers(
        (decay_real * step).reshape(1, flat), (frequency * step).reshape(1, flat), counts
    )
    vmem = pl.BlockSpec(memory_space=pltpu.VMEM)
    hbm = pl.BlockSpec(memory_space=pl.ANY)
    dma = pltpu.SemaphoreType.DMA
    return pl.pallas_call(
        functools.partial(layer_kernel, n_sp, width, states),
        out_shape=jax.ShapeDtypeStruct((own, depth), BF),
        in_specs=[vmem] * 10 + [hbm] * 3 + [vmem] + [hbm] * 3,
        out_specs=vmem,
        scratch_shapes=[
            pltpu.VMEM(value_weight.shape, BF),
            pltpu.VMEM(glu_weight.shape, BF),
            pltpu.VMEM(mix_weight.shape, BF),
            pltpu.VMEM((n_sp * mlp_gate.shape[0], ff), BF),
            pltpu.VMEM((n_sp * mlp_gate.shape[0], ff), BF),
            pltpu.VMEM((n_sp, ff, d_loc), BF),
            pltpu.VMEM((8, chans, flat), BF),
            pltpu.VMEM((rows, flat), F32),
            pltpu.VMEM((rows, flat), F32),
            pltpu.VMEM((6, ROWS8, flat), F32),
            pltpu.VMEM((n_sp, ROWS8, flat), F32),
            pltpu.VMEM((n_tp, rows, chans), BF),
            pltpu.VMEM((1, n_tp, own, depth), BF),
            pltpu.VMEM((1, 2, own, depth), BF),
            pltpu.VMEM((1, own, depth), BF),
            pltpu.VMEM((1, own, depth), BF),
            pltpu.VMEM((own, depth), F32),
            pltpu.VMEM((n_tp, own, depth), BF),
            pltpu.VMEM((n_tp, own, ff), BF),
            pltpu.VMEM((n_sp, n_tp, own, d_loc), BF),
            pltpu.VMEM((n_sp, 2, own, d_loc), BF),
            pltpu.VMEM((n_sp, own, d_loc), BF),
            pltpu.VMEM((n_sp, own, d_loc), BF),
            dma((6,)),
            dma((n_sp,)),
            dma((n_sp,)),
            dma((2, 3, n_sp)),
            dma((2, 3, n_sp)),
            dma((2, 3, n_sp)),
            dma((2, 3, n_sp)),
            dma((2, 3)),
            dma((2, 3)),
            dma((1, 3)),
            dma((1, 3)),
            dma((n_sp, 3)),
            dma((n_sp, 3)),
        ],
        compiler_params=pltpu.CompilerParams(
            collective_id=0, has_side_effects=True, vmem_limit_bytes=60 * 1024 * 1024
        ),
    )(
        residual,
        state_input,
        gate_input,
        pow_real,
        pow_imag,
        tiled(in_real.transpose(0, 2, 1)),
        tiled(in_imag.transpose(0, 2, 1)),
        tiled(read_real),
        tiled(read_imag),
        skip_gain[None, :],
        value_weight,
        glu_weight,
        mix_weight,
        norm_gain[None, :],
        mlp_gate,
        mlp_up,
        mlp_down,
    )


def quick_kernel(
    n_sp,
    width,
    states,
    residual_h,
    u_h,
    gate_in_h,
    decay_h,
    freq_h,
    step_h,
    drive_re_h,
    drive_im_h,
    read_re_h,
    read_im_h,
    skip_h,
    value_h,
    glu_h,
    mix_h,
    gain_h,
    gate_h,
    up_h,
    down_h,
    out,
    residual,
    u,
    gate_in,
    decay,
    freq,
    log_step,
    drive_re,
    drive_im,
    read_re,
    read_im,
    skip,
    value_w,
    glu_w,
    mix_w,
    gain,
    w_gate,
    w_up,
    w_down,
    wide,
    pow_real,
    pow_imag,
    ratio,
    st_real,
    st_imag,
    masked,
    ends,
    acts,
    part,
    rx_pair,
    relay,
    rx_far,
    inner,
    normed,
    hidden,
    c_part,
    c_in,
    c_relay,
    guest,
    g_hidden,
    g_out,
    g_in,
    load_sem,
    end_send,
    end_recv,
    z_send,
    z_recv,
    y_send,
    y_recv,
    y_late,
    z_more,
    z_last,
    g_send,
    g_recv,
    b_send,
    b_recv,
    ag_send,
    ag_recv,
    rs_send,
    rs_recv,
    c_send,
    c_recv,
):
    g, s, t = lax.axis_index("grp"), lax.axis_index("sp"), lax.axis_index("tp")
    low, high_bit = t % 2, t // 2
    p = t + 1 - 2 * low
    q = t + 2 - 4 * high_bit
    far = 3 - t
    other = 1 - g
    rows, chans = u.shape
    groups, flat = decay.shape[0], st_real.shape[1]
    own, depth = residual.shape
    k_loc, ff = gate_h.shape
    d_loc = down_h.shape[1]
    n_tp = acts.shape[0]
    k_half, f_half = k_loc // 2, ff // 2
    k_piece, d_half = k_half // PIECES, d_loc // HALVES
    f_cuts = [f_half * n // PER for n in range(PER + 1)]

    barrier = pltpu.get_barrier_semaphore()
    pl.semaphore_signal(barrier, inc=1, device_id={"tp": p})
    pl.semaphore_signal(barrier, inc=1, device_id={"tp": q})
    pl.semaphore_signal(barrier, inc=1, device_id={"grp": other})

    @pl.loop(1, n_sp)
    def _(d):
        pl.semaphore_signal(barrier, inc=1, device_id={"sp": (s + d) % n_sp})

    place = pl.ds(pl.multiple_of(s * k_loc, k_loc), k_loc)
    pairs_of = (
        (gate_h, w_gate.at[place, :]),
        (decay_h, decay),
        (freq_h, freq),
        (step_h, log_step),
        (drive_re_h, drive_re),
        (drive_im_h, drive_im),
        (u_h, u),
        (read_re_h, read_re),
        (read_im_h, read_im),
        (skip_h, skip),
        (up_h, w_up.at[place, :]),
        (down_h, w_down.at[s]),
        (value_h, value_w),
        (glu_h, glu_w),
        (gate_in_h, gate_in),
        (mix_h, mix_w),
        (residual_h, residual),
        (gain_h, gain),
    )
    loads = [
        pltpu.make_async_copy(a, b, load_sem.at[i]) for i, (a, b) in enumerate(pairs_of)
    ]
    for load in loads:
        load.start()
    pl.semaphore_wait(barrier, 3 + n_sp - 1)

    bufs = (w_gate, w_up, w_down)
    behind = (s, n_sp - 1 - s)
    n_early, n_late = 2 * PIECES, PIECES

    def await_bytes(sem, ref):
        pltpu.make_async_copy(ref, ref, sem).wait()

    def mine(c, i, origin, half):
        if c < 2:
            row = pl.multiple_of(origin * k_loc + half * k_half + i * k_piece, k_piece)
            return bufs[c].at[pl.ds(row, k_piece), :]
        start, stop = f_cuts[i % PER], f_cuts[i % PER + 1]
        row = pl.multiple_of(half * f_half + start, 16)
        return bufs[c].at[origin, pl.ds(row, stop - start), pl.ds((i // PER) * d_half, d_half)]

    def z_copy(side, c, i, origin):
        piece = mine(c, i, origin, g)
        return pltpu.make_async_remote_copy(
            src_ref=piece,
            dst_ref=piece,
            send_sem=z_send.at[side, c],
            recv_sem=z_recv.at[c, i, origin - side],
            device_id={"sp": ahead(side)},
        )

    def y_copy(c, i, origin, half):
        piece = mine(c, i, origin, half)
        return pltpu.make_async_remote_copy(
            src_ref=piece,
            dst_ref=piece,
            send_sem=y_send.at[c // 2],
            recv_sem=y_recv.at[0] if c < 2 else y_late.at[origin, i // (PER)],
            device_id={"grp": other},
        )

    def more_copy(side, c, i):
        piece = mine(c, i, s, other)
        return pltpu.make_async_remote_copy(
            src_ref=piece,
            dst_ref=piece,
            send_sem=z_send.at[side, c],
            recv_sem=z_more.at[0 if c < 2 else 1 + i // PER],
            device_id={"sp": ahead(side)},
        )

    def last_copy(side, k):
        piece = mine(2, PIECES - 1, source(side, k), other)
        return pltpu.make_async_remote_copy(
            src_ref=piece,
            dst_ref=piece,
            send_sem=z_send.at[side, 2],
            recv_sem=z_last.at[0],
            device_id={"sp": ahead(side)},
        )

    def last_on(side, b):
        if b > 1:
            last_copy(side, b - 1).wait_recv()
        if b < n_sp - 1:
            last_copy(side, b - 1).start()

    def last_advance(b):
        for side in range(2):
            pl.when(behind[side] == b)(functools.partial(last_on, side, b))

    def ahead(side):
        return (s + 1) % n_sp if side == 0 else (s + n_sp - 1) % n_sp

    def source(side, k):
        return (s + n_sp - k) % n_sp if side == 0 else (s + k) % n_sp

    def own_sends(side, c, pieces):
        for i in pieces:
            z_copy(side, c, i, s).start()

    def end_sends(side):
        for c in range(3):
            if c == 2:
                own_sends(side, 2, range(PIECES))
            else:
                for i in range(PIECES):
                    more_copy(side, c, i).start()

    inner_one = jnp.logical_or(behind[0] == 1, behind[1] == 1)
    end_one = jnp.logical_not(inner_one)
    mate = s + 1 - 2 * (s % 2)
    taken = (1 - s // (n_sp // 2)) * (n_sp - 1)
    e_rows = own // 2

    def guest_copy(h):
        rows_of = pl.ds(h * e_rows, e_rows)
        return pltpu.make_async_remote_copy(
            src_ref=normed.at[t, rows_of, :],
            dst_ref=guest.at[t, rows_of, :],
            send_sem=g_send.at[0],
            recv_sem=g_recv.at[0, h],
            device_id={"sp": mate},
        )

    def guest_tp(h, slot, kind, target):
        piece = guest.at[slot, pl.ds(h * e_rows, e_rows), :]
        return pltpu.make_async_remote_copy(
            src_ref=piece,
            dst_ref=piece,
            send_sem=g_send.at[(2, 0, 1)[kind]],
            recv_sem=g_recv.at[1 + kind, h],
            device_id={"tp": target},
        )

    guest_cross = pltpu.make_async_remote_copy(
        src_ref=normed.at[q, pl.ds(e_rows, e_rows), :],
        dst_ref=guest.at[q, pl.ds(e_rows, e_rows), :],
        send_sem=g_send.at[2],
        recv_sem=g_recv.at[1, 1],
        device_id={"sp": mate},
    )

    def guest_take(h):
        guest_copy(h).wait_recv()
        if h == 0:
            guest_tp(h, t, 0, q).start()
        guest_tp(h, t, 1, p).start()

    def guest_relay(h):
        guest_tp(h, q, 0, q).wait_recv()
        guest_tp(h, q, 2, p).start()

    def own_early(c, pieces):
        for side in range(2):
            pl.when(behind[side] < n_sp - 1)(functools.partial(own_sends, side, c, pieces))

    def shared(side, k):
        return behind[side] > 1 if k == 1 else behind[side] >= k

    def onward(side, k, c, i, last):
        @pl.when(behind[side] < n_sp - 1)
        def _():
            z_copy(side, c, i, source(side, k)).start()

        if last:

            @pl.when(jnp.logical_and(behind[side] == k, k < n_sp - 1))
            def _():
                own_sends(side, 2, range(PIECES))

    def pass_on(side, k, c, i, last, hold):
        origin = source(side, k)
        z_copy(side, c, i, origin).wait_recv()
        if not hold:
            onward(side, k, c, i, last)

        trade = shared(side, k)
        if c == 2 and i == PIECES - 1:
            trade = jnp.logical_and(trade, behind[side] != k + 1)

        @pl.when(trade)
        def _():
            y_copy(c, i, origin, g).start()

    def advance(*slots, hold=False):
        for n in slots:
            for side in range(2):
                if n < n_early * (n_sp - 1):
                    k, c, i = n // n_early + 1, n % n_early // PIECES, n % PIECES
                    last = n % n_early == n_early - 1
                    work = functools.partial(pass_on, side, k, c, i, last, hold)
                    pl.when(behind[side] >= k)(work)
                for b in range(1, n_sp):
                    m = n - n_early * max(b, 2)
                    k = m // n_late + 1
                    if 0 <= m and k <= min(b, n_sp - 2):
                        stop = k == b == n_sp - 2
                        work = functools.partial(pass_on, side, k, 2, m % n_late, False, stop)
                        pl.when(behind[side] == b)(work)

    loads[0].wait()
    own_early(0, range(PIECES))

    for load in loads[1:4]:
        load.wait()
    eye = lax.broadcasted_iota(jnp.int32, (groups, groups), 0) == lax.broadcasted_iota(
        jnp.int32, (groups, groups), 1
    )
    step = jnp.exp(jnp.sum(jnp.where(eye, log_step[...], 0.0), axis=1, keepdims=True))
    rate, turn = decay[...], freq[...]
    magnitude = jnp.exp(rate * step)
    bar_re = magnitude * jnp.cos(turn * step)
    bar_im = magnitude * jnp.sin(turn * step)
    modulus = rate * rate + turn * turn
    ratio_re = ((bar_re - 1.0) * rate + bar_im * turn) / modulus
    ratio_im = (bar_im * rate - (bar_re - 1.0) * turn) / modulus
    tiles = max(1, 128 // states)
    lanes = tiles * states
    part_of = lax.broadcasted_iota(jnp.int32, (1, lanes), 1) // states

    def spread(target, row, value):
        doubled = jnp.concatenate([value] * tiles, axis=1)
        for tile in range(groups // tiles):
            line = doubled[tile * tiles : tile * tiles + 1, :]
            for j in range(1, tiles):
                line = jnp.where(part_of == j, doubled[tile * tiles + j : tile * tiles + j + 1, :], line)
            target[row : row + 1, tile * lanes : (tile + 1) * lanes] = line

    spread(ratio, 0, ratio_re)
    spread(ratio, 1, ratio_im)
    up_re, up_im = bar_re, bar_im
    for n in range(ROWS8):
        spread(pow_real, n, up_re)
        spread(pow_imag, n, up_im)
        up_re, up_im = up_re * bar_re - up_im * bar_im, up_re * bar_im + up_im * bar_re

    for load in loads[4:9]:
        load.wait()
    row_group = lax.broadcasted_iota(jnp.int32, (chans, lanes), 0) // width
    lane = lax.broadcasted_iota(jnp.int32, (chans, lanes), 1)
    for i, ref in enumerate((drive_re, drive_im, read_re, read_im)):
        value = jnp.concatenate([ref[...]] * tiles, axis=1)
        for tile in range(flat // lanes):
            kept = jnp.where(row_group == (lane + tile * lanes) // states, value, 0.0)
            at = slice(tile * lanes, (tile + 1) * lanes)
            for j, piece in enumerate(split(kept)):
                wide[2 * i + j, :, at] = piece

    @pl.loop(0, rows // own // 2)
    def _(b):
        at = pl.ds(pl.multiple_of(b * 2 * own, own), 2 * own)
        x = u[at, :]
        push_re = mm(x, wide[0]) + mm(x, wide[1])
        push_im = mm(x, wide[2]) + mm(x, wide[3])
        st_real[at, :] = ratio[0:1, :] * push_re - ratio[1:2, :] * push_im
        st_imag[at, :] = ratio[0:1, :] * push_im + ratio[1:2, :] * push_re

    sub = lax.broadcasted_iota(jnp.int32, (ROWS8, flat), 0)
    for i, reach in enumerate((1, 2, 4)):
        masked[2 * i] = jnp.where(sub >= reach, pow_real[reach - 1 : reach, :], 0.0)
        masked[2 * i + 1] = jnp.where(sub >= reach, pow_imag[reach - 1 : reach, :], 0.0)

    def scan_step(b, carry):
        c_re, c_im = carry
        at = pl.ds(pl.multiple_of(b * ROWS8, ROWS8), ROWS8)
        x_re, x_im = st_real[at, :], st_imag[at, :]
        for i, reach in enumerate((1, 2, 4)):
            m_re, m_im = pltpu.roll(x_re, reach, 0), pltpu.roll(x_im, reach, 0)
            a_re, a_im = masked[2 * i], masked[2 * i + 1]
            x_re, x_im = x_re + a_re * m_re - a_im * m_im, x_im + a_re * m_im + a_im * m_re
        p_re, p_im = pow_real[...], pow_imag[...]
        x_re, x_im = x_re + p_re * c_re - p_im * c_im, x_im + p_re * c_im + p_im * c_re
        st_real[at, :] = x_re
        st_imag[at, :] = x_im
        return x_re[ROWS8 - 1 :, :], x_im[ROWS8 - 1 :, :]

    zero = jnp.zeros((1, flat), F32)
    blocks = rows // ROWS8
    tip = lax.fori_loop(0, blocks // 2, scan_step, (zero, zero))
    advance(0, hold=True)
    end_re, end_im = lax.fori_loop(blocks // 2, blocks, scan_step, tip)
    ends[s, :, :flat] = end_re
    ends[s, :, flat:] = end_im

    def end_copy(target, origin):
        return pltpu.make_async_remote_copy(
            src_ref=ends.at[origin],
            dst_ref=ends.at[origin],
            send_sem=end_send.at[target],
            recv_sem=end_recv.at[origin],
            device_id={"sp": target},
        )

    @pl.loop(s + 1, n_sp)
    def _(later):
        end_copy(later, s).start()

    for load in loads[10:12]:
        load.wait()
    own_early(1, range(PIECES))
    for side in range(2):
        pl.when(behind[side] == 0)(functools.partial(end_sends, side))
        pl.when(behind[side] >= 1)(functools.partial(onward, side, 1, 0, 0, False))
    advance(1)
    last_re, last_im = pow_real[ROWS8 - 1 :, :], pow_imag[ROWS8 - 1 :, :]
    long_re, long_im = last_re, last_im
    reach = ROWS8
    while reach < rows:
        long_re, long_im = long_re * long_re - long_im * long_im, 2.0 * long_re * long_im
        reach *= 2

    advance(2, 3, 4)

    @pl.loop(0, s)
    def _(earlier):
        end_copy((s + 1) % n_sp, earlier).wait_recv()

    def carry_step(j, carry):
        c_re, c_im = carry
        e_re, e_im = ends[j, :, :flat], ends[j, :, flat:]
        n_re = long_re * c_re - long_im * c_im + e_re
        n_im = long_re * c_im + long_im * c_re + e_im
        return jnp.where(j < s, n_re, c_re), jnp.where(j < s, n_im, c_im)

    carry = lax.fori_loop(0, n_sp - 1, carry_step, (zero, zero))

    def lift(b, carry):
        c_re, c_im = carry
        at = pl.ds(pl.multiple_of(b * ROWS8, ROWS8), ROWS8)
        p_re, p_im = pow_real[...], pow_imag[...]
        st_real[at, :] = st_real[at, :] + p_re * c_re - p_im * c_im
        st_imag[at, :] = st_imag[at, :] + p_re * c_im + p_im * c_re
        return last_re * c_re - last_im * c_im, last_re * c_im + last_im * c_re

    carry = lax.fori_loop(0, blocks // 2, lift, carry)
    advance(5)
    lax.fori_loop(blocks // 2, blocks, lift, carry)
    loads[9].wait()

    def read_block(b):
        at = pl.ds(pl.multiple_of(b * 2 * own, own), 2 * own)
        high, small = split(st_real[at, :])
        y = mm_t(high, wide[4]) + mm_t(small, wide[4]) + mm_t(high, wide[5])
        high, small = split(st_imag[at, :])
        y = y - (mm_t(high, wide[6]) + mm_t(small, wide[6]) + mm_t(high, wide[7]))
        y = y + skip[...] * u[at, :].astype(F32)
        acts[t, at, :] = jax.nn.gelu(y).astype(BF)

    half_rows = rows // own // 4
    pl.loop(0, half_rows)(read_block)
    advance(6)
    pl.loop(half_rows, rows // own // 2)(read_block)
    advance(7)

    def gather_tp(buf, lane_no, between, later):
        def copy(slot, kind, target):
            return pltpu.make_async_remote_copy(
                src_ref=buf.at[slot],
                dst_ref=buf.at[slot],
                send_sem=ag_send.at[lane_no, kind],
                recv_sem=ag_recv.at[lane_no, kind],
                device_id={"tp": target},
            )

        sent = [copy(t, 0, q), copy(t, 1, p)]
        for item in sent:
            item.start()
        copy(p, 1, p).wait_recv()
        between()
        copy(q, 0, q).wait_recv()
        relayed = copy(q, 2, p)
        relayed.start()
        later()
        copy(far, 2, p).wait_recv()
        return sent + [relayed]

    def rs_pair(index):
        return pltpu.make_async_remote_copy(
            src_ref=part.at[(far, p)[index]],
            dst_ref=rx_pair.at[index],
            send_sem=rs_send.at[index],
            recv_sem=rs_recv.at[index],
            device_id={"tp": p},
        )

    across = pltpu.make_async_remote_copy(
        src_ref=relay,
        dst_ref=rx_far,
        send_sem=rs_send.at[2],
        recv_sem=rs_recv.at[2],
        device_id={"tp": q},
    )

    pending = gather_tp(acts, 0, lambda: advance(8, 9), lambda: advance(10))
    for load in loads[12:]:
        load.wait()

    near_half = high_bit
    duo = n_tp // 2

    def mix_half(b):
        at = pl.ds(pl.multiple_of(b * duo * own, own), duo * own)
        value = jnp.zeros((duo * own, value_w.shape[1]), F32)
        gated = value
        for j in range(n_tp):
            a = acts[j, at, :]
            value = value + mm(a, value_w[j * chans : (j + 1) * chans, :])
            gated = gated + mm(a, glu_w[j * chans : (j + 1) * chans, :])
        mixed = jax.nn.sigmoid(gate_in[at, :].astype(F32)) * value * jax.nn.sigmoid(gated)
        product = mm(mixed.astype(BF), mix_w[...]).astype(BF)
        part[pl.ds(b * duo, duo)] = product.reshape(duo, own, depth)

    mix_half(1 - near_half)
    rs_pair(0).start()
    advance(11, 12)
    rs_pair(0).wait_recv()
    relay[...] = (part[q].astype(F32) + rx_pair[0].astype(F32)).astype(BF)
    across.start()
    mix_half(near_half)
    rs_pair(1).start()
    advance(13, 14, 15, 16, 17)
    rs_pair(1).wait_recv()
    across.wait_recv()
    pending += [rs_pair(0), rs_pair(1), across]
    near = part[t].astype(F32) + rx_pair[1].astype(F32)
    x = residual[...].astype(F32) + (near + rx_far[...].astype(F32))
    inner[...] = x
    scale = lax.rsqrt(jnp.mean(x * x, axis=-1, keepdims=True) + EPSILON)
    normed[t] = (x * scale * gain[...]).astype(BF)


    @pl.when(end_one)
    def _():
        for h in range(2):
            guest_copy(h).start()

    def gated_half(rows_in, rows_out, b):
        x = rows_in[pl.ds(b * duo, duo)].reshape(duo * own, depth)
        both = (jax.nn.silu(mm(x, w_gate[...])) * mm(x, w_up[...])).astype(BF)
        rows_out[pl.ds(b * duo, duo)] = both.reshape(duo, own, ff)

    def inner_first():
        await_bytes(z_more.at[0], w_gate.at[:k_loc, :])
        await_bytes(y_recv.at[0], w_gate.at[: (n_sp - 2) * k_loc, :])
        gated_half(normed, hidden, near_half)

    def while_gathering():
        advance(18, 19)
        last_advance(1)
        pl.when(inner_one)(inner_first)
        advance(20, 21, 22)
        pl.when(inner_one)(lambda: guest_take(0))
        advance(23)

    pending += gather_tp(normed, 1, while_gathering, lambda: None)

    advance(24)

    @pl.when(end_one)
    def _():
        guest_cross.start()
        for side in range(2):

            @pl.when(behind[side] == 0)
            def _():
                for i in range(PIECES):
                    more_copy(side, 2, i).start()

    last_advance(2)

    @pl.when(inner_one)
    def _():
        guest_take(1)
        gated_half(normed, hidden, 1 - near_half)

    advance(25)

    @pl.when(end_one)
    def _():
        await_bytes(y_recv.at[0], w_gate.at[: (n_sp - 1) * k_loc, :])

    advance(26)
    pl.when(end_one)(lambda: gated_half(normed, hidden, near_half))
    advance(27)
    pl.when(end_one)(lambda: gated_half(normed, hidden, 1 - near_half))
    advance(28)

    def col_pair(o, h, index):
        return pltpu.make_async_remote_copy(
            src_ref=c_part.at[o, h, (far, p)[index]],
            dst_ref=c_in.at[o, h, index],
            send_sem=c_send.at[0],
            recv_sem=c_recv.at[o, h if index == 0 else HALVES],
            device_id={"tp": p},
        )

    def col_far(o, h):
        return pltpu.make_async_remote_copy(
            src_ref=c_relay.at[o, h],
            dst_ref=c_in.at[o, h, 2],
            send_sem=c_send.at[0],
            recv_sem=c_recv.at[o, HALVES],
            device_id={"tp": q},
        )

    def column(o, h, rows_in=hidden, slot=None):
        slot = o if slot is None else slot
        weight = w_down.at[o, :, h * d_half : (h + 1) * d_half]
        for index, b in enumerate((1 - near_half, near_half)):
            some = pl.ds(b * duo, duo)
            product = mm(rows_in[some].reshape(duo * own, ff), weight[...]).astype(BF)
            c_part[slot, h, some] = product.reshape(duo, own, d_half)
            col_pair(slot, h, index).start()

    def relay_on(o, h):
        col_pair(o, h, 0).wait_recv()
        both = c_part[o, h, q].astype(F32) + c_in[o, h, 0].astype(F32)
        c_relay[o, h] = both.astype(BF)
        col_far(o, h).start()

    def total(o, h):
        near = c_part[o, h, t].astype(F32) + c_in[o, h, 1].astype(F32)
        return near + c_in[o, h, 2].astype(F32)

    def put(o, h, value):
        at = pl.ds(pl.multiple_of(o * d_loc + h * d_half, d_half), d_half)
        out[:, at] = (inner[:, at] + 0.5 * value).astype(BF)

    def back_copy(h):
        return pltpu.make_async_remote_copy(
            src_ref=g_out.at[h],
            dst_ref=g_in.at[h],
            send_sem=b_send.at[0],
            recv_sem=b_recv.at[h],
            device_id={"sp": mate},
        )

    def settle(o):
        await_bytes(c_recv.at[o, HALVES], c_in.at[o, :, 1:3])
        for h in range(HALVES):
            put(o, h, total(o, h))

    def both_sides(k, work):
        for side in range(2):
            pl.when(behind[side] >= k)(functools.partial(work, side, k))

    def land(h, side, k):
        origin = source(side, k)
        row = pl.multiple_of(other * f_half, f_half)
        came = w_down.at[origin, pl.ds(row, f_half), h * d_half : (h + 1) * d_half]

        whole = shared(side, k)
        if h == HALVES - 1:
            whole = jnp.logical_and(whole, behind[side] != k + 1)

            @pl.when(behind[side] == k + 1)
            def _():
                await_bytes(y_late.at[origin, h], mine(2, h * PER, origin, other))

        @pl.when(whole)
        def _():
            await_bytes(y_late.at[origin, h], came)

        if k == 1:

            @pl.when(behind[side] == 1)
            def _():
                await_bytes(z_more.at[1 + h], came)

    def next_column(h, side, k):
        land(h, side, k)
        column(source(side, k), h)

    def next_settle(side, k):
        settle(source(side, k))

    def next_relay(h, side, k):
        relay_on(source(side, k), h)

    def columns(k, *parts):
        for h in parts:
            both_sides(k, functools.partial(next_column, h))

    def relays(k, *parts):
        for h in parts:
            both_sides(k, functools.partial(next_relay, h))

    def far_side(work):
        for h in range(HALVES):
            for side in range(2):
                pl.when(behind[side] > 1)(functools.partial(work, h, side, 1))

    def end_side(work):
        for h in range(HALVES):
            for side in range(2):
                pl.when(behind[side] == 1)(functools.partial(work, h, side, 1))

    def sends_done():
        for item in pending:
            item.wait_send()

        @pl.loop(s + 1, n_sp)
        def _(later):
            end_copy(later, s).wait_send()

        def sent(side, b):
            early, late = max(2, b + 1), max(2, min(b + 1, n_sp - 2))
            tail = k_piece if b > 0 else 0
            for c, size in enumerate((early * k_half, early * k_half, late * k_half + tail)):
                await_bytes(z_send.at[side, c], w_gate.at[:size, :])

        for side in range(2):
            for b in range(n_sp - 1):
                pl.when(behind[side] == b)(functools.partial(sent, side, b))
        await_bytes(y_send.at[1], w_gate.at[: (n_sp - 2) * k_half - k_piece, :])
        await_bytes(g_send.at[0], normed.at[0])
        await_bytes(g_send.at[2], normed.at[0, :e_rows, :])

    @pl.when(end_one)
    def _():
        for h in range(HALVES):
            column(s, h)
        for h in range(HALVES):
            relay_on(s, h)
        advance(29)
        columns(1, 0)
        relays(1, 0)
        advance(30)
        columns(1, 1)
        relays(1, 1)
        advance(31)
        settle(s)
        columns(2, 0)
        relays(2, 0)
        both_sides(1, next_settle)
        sends_done()
        await_bytes(y_send.at[0], w_gate.at[: (n_sp - 1) * k_loc, :])
        last_advance(n_sp - 1)
        columns(2, 1)
        relays(2, 1)
        both_sides(2, next_settle)
        for h in range(HALVES):
            back_copy(h).wait_recv()
            put(taken, h, g_in[h].astype(F32))
        await_bytes(c_send.at[0], c_in.at[: n_sp - 1])

    @pl.when(inner_one)
    def _():
        for h in range(HALVES):
            column(s, h)
        far_side(next_column)
        for h in range(HALVES):
            relay_on(s, h)
        far_side(next_relay)
        guest_relay(0)
        for h in range(2):
            guest_tp(h, p, 1, p).wait_recv()
        gated_half(guest, g_hidden, near_half)
        guest_relay(1)
        for h in range(2):
            guest_tp(h, far, 2, p).wait_recv()
        gated_half(guest, g_hidden, 1 - near_half)
        for h in range(HALVES):
            both_sides(2, functools.partial(land, h))
        for h in range(HALVES):
            column(taken, h, g_hidden, n_sp)
        for h in range(HALVES):
            relay_on(n_sp, h)
        end_side(next_column)
        for h in range(HALVES):
            column(taken, h)
        end_side(next_relay)
        for h in range(HALVES):
            relay_on(taken, h)
        await_bytes(c_recv.at[n_sp, HALVES], c_in.at[n_sp, :, 1:3])
        for h in range(HALVES):
            g_out[h] = total(n_sp, h).astype(BF)
            back_copy(h).start()
        settle(s)
        both_sides(1, next_settle)
        sends_done()
        await_bytes(y_send.at[0], w_gate.at[: (n_sp - 2) * k_loc, :])
        await_bytes(g_send.at[1], normed.at[0])
        both_sides(2, next_settle)
        await_bytes(b_send.at[0], g_out)
        await_bytes(c_send.at[0], c_in)


def quick(
    residual,
    state_input,
    gate_input,
    decay_real,
    frequency,
    log_step,
    drive_real,
    drive_imag,
    read_real,
    read_imag,
    skip_gain,
    value_weight,
    glu_weight,
    mix_weight,
    norm_gain,
    mlp_gate,
    mlp_up,
    mlp_down,
):
    n_sp, n_tp = lax.axis_size("sp"), lax.axis_size("tp")
    groups, states, width = drive_real.shape
    flat, chans = groups * states, groups * width
    rows = state_input.shape[0]
    own, depth = residual.shape
    k_loc, ff = mlp_gate.shape
    d_loc = mlp_down.shape[1]
    d_half = d_loc // HALVES
    hbm = pl.BlockSpec(memory_space=pltpu.HBM)
    dma = pltpu.SemaphoreType.DMA
    operands = (
        residual,
        state_input,
        gate_input,
        decay_real,
        frequency,
        log_step[None, :],
        drive_real.transpose(0, 2, 1).reshape(chans, states),
        drive_imag.transpose(0, 2, 1).reshape(chans, states),
        read_real.reshape(chans, states),
        read_imag.reshape(chans, states),
        skip_gain[None, :],
        value_weight,
        glu_weight,
        mix_weight,
        norm_gain[None, :],
        mlp_gate,
        mlp_up,
        mlp_down,
    )
    return pl.pallas_call(
        functools.partial(quick_kernel, n_sp, width, states),
        out_shape=pltpu.VMEM((own, depth), BF),
        in_specs=[hbm] * len(operands),
        out_specs=pl.BlockSpec(memory_space=pltpu.VMEM),
        scratch_shapes=[pltpu.VMEM(x.shape, x.dtype) for x in operands[:15]]
        + [
            pltpu.VMEM((n_sp * k_loc, ff), BF),
            pltpu.VMEM((n_sp * k_loc, ff), BF),
            pltpu.VMEM((n_sp, ff, d_loc), BF),
            pltpu.VMEM((8, chans, flat), BF),
            pltpu.VMEM((ROWS8, flat), F32),
            pltpu.VMEM((ROWS8, flat), F32),
            pltpu.VMEM((2, flat), F32),
            pltpu.VMEM((rows, flat), F32),
            pltpu.VMEM((rows, flat), F32),
            pltpu.VMEM((6, ROWS8, flat), F32),
            pltpu.VMEM((n_sp, 1, 2 * flat), F32),
            pltpu.VMEM((n_tp, rows, chans), BF),
            pltpu.VMEM((n_tp, own, depth), BF),
            pltpu.VMEM((2, own, depth), BF),
            pltpu.VMEM((own, depth), BF),
            pltpu.VMEM((own, depth), BF),
            pltpu.VMEM((own, depth), F32),
            pltpu.VMEM((n_tp, own, depth), BF),
            pltpu.VMEM((n_tp, own, ff), BF),
            pltpu.VMEM((n_sp + 1, HALVES, n_tp, own, d_half), BF),
            pltpu.VMEM((n_sp + 1, HALVES, 3, own, d_half), BF),
            pltpu.VMEM((n_sp + 1, HALVES, own, d_half), BF),
            pltpu.VMEM((n_tp, own, depth), BF),
            pltpu.VMEM((n_tp, own, ff), BF),
            pltpu.VMEM((HALVES, own, d_half), BF),
            pltpu.VMEM((HALVES, own, d_half), BF),
            dma((len(operands),)),
            dma((n_sp,)),
            dma((n_sp,)),
            dma((2, 3)),
            dma((3, PIECES, n_sp - 1)),
            dma((2,)),
            dma((1,)),
            dma((n_sp, HALVES)),
            dma((1 + HALVES,)),
            dma((1,)),
            dma((3,)),
            dma((4, 2)),
            dma((1,)),
            dma((HALVES,)),
            dma((2, 3)),
            dma((2, 3)),
            dma((3,)),
            dma((3,)),
            dma((1,)),
            dma((n_sp + 1, HALVES + 1)),
        ],
        compiler_params=pltpu.CompilerParams(
            collective_id=0, has_side_effects=True, vmem_limit_bytes=60 * 1024 * 1024
        ),
    )(*operands)


def solution(mesh):
    placed = (
        P(("grp", "sp", "tp"), None),
        P(("grp", "sp"), "tp"),
        P(("grp", "sp"), "tp"),
        P("tp", None),
        P("tp", None),
        P("tp"),
        P("tp", None, None),
        P("tp", None, None),
        P("tp", None, None),
        P("tp", None, None),
        P("tp"),
        P(None, "tp"),
        P(None, "tp"),
        P("tp", None),
        P(),
        P("sp", "tp"),
        P("sp", "tp"),
        P("tp", "sp"),
    )
    body = shards
    if (mesh.shape["tp"], mesh.shape["grp"]) == (4, 2):
        body = quick if mesh.shape["sp"] == 4 else fused
    return jax.shard_map(
        body, mesh=mesh, in_specs=placed, out_specs=P(("grp", "sp", "tp"), None), check_vma=False
    )
```
